32 devices in a mesh: sp: 4 (over y, x), tp: 8 (over z, core).
Axes of the slice: x: 2, y: 2, z: 4, core: 2. Of those that a mesh axis runs over, the one named last changes fastest.
Arguments:
- residual_in: bfloat16 [2048, 4096], P('sp', 'tp'), may hold values from -24 to 24
- norm_gain: float32 [2, 4096], replicated, may hold values from 0.1 to 1.9
- gate_proj: bfloat16 [2, 4096, 2048], P(None, 'sp', 'tp'), may hold values from -0.09375 to 0.09375
- filter_proj: bfloat16 [2, 4096, 2048], P(None, 'sp', 'tp'), may hold values from -0.09375 to 0.09375
- signal_proj: bfloat16 [2, 4096, 2048], P(None, 'sp', 'tp'), may hold values from -0.09375 to 0.09375
- conv_taps: float32 [2, 3, 2048], P(None, None, 'tp'), may hold values from -3 to 3
- out_proj: bfloat16 [2, 2048, 4096], P(None, 'tp', 'sp'), may hold values from -0.1875 to 0.1875
- final_gain: float32 [4096], P('tp'), may hold values from 0.1 to 1.9
Outputs:
- final_rows: float32 [2048, 4096], P('sp', 'tp')
The draws below stay inside these ranges and needn't reach their ends.
All inputs are finite; a program needn't handle non-finite values.
Results may differ from the reference program's by a relative error of at most 0.033.
Values may be sent and summed in bfloat16 or wider, within the bound.
A program may use at most 64 MiB of HBM per device.

```python
import math
import jax
import jax.numpy as jnp
from jax import lax

D = 4096
CW = 2048
TAPS = 3
LAYERS = 2
TOKENS = 2048
N_TP = 8


def draw_residual_in(key, part):
    subkeys = jax.random.split(key, 4)
    standard = jax.random.normal(subkeys[0], (TOKENS, D), jnp.float32)
    group_scale = jnp.exp(jax.random.uniform(subkeys[1], (D // 64,), jnp.float32, math.log(0.3), math.log(3.0)))
    column_scale = jnp.repeat(group_scale, 64)
    values = standard * column_scale[None, :]
    return jnp.clip(values, -24.0, 24.0).astype(jnp.bfloat16)


def spiked(values, rng, source, target, shards_of, factor):
    def block_of(position):
        return (jnp.arange(values.shape[position]) // (values.shape[position] // shards_of)).reshape((-1,) + (1,) * (values.ndim - 1 - position))

    near = jax.random.permutation(rng, shards_of)[block_of(target)]
    other_side = (block_of(target) + shards_of // 2) % shards_of
    return jnp.where((block_of(source) == near) | (block_of(source) == other_side), factor * values, values)


def block_levels(key, shape, pieces, least, high):
    def one(dim, blocks):
        heights = jax.random.uniform(jax.random.fold_in(jax.random.fold_in(key, 6), dim), (blocks,), jnp.float32, least / len(pieces), high / len(pieces))
        return jnp.repeat(jnp.exp(heights), shape[dim] // blocks).reshape((-1,) + (1,) * (len(shape) - dim - 1))

    loudness = one(*pieces[0])
    for cut in pieces[1:]:
        loudness = loudness * one(*cut)
    return loudness


def normal_values(own_key, dims, spread, most, cuts=(), held_as=jnp.bfloat16):
    result = jax.random.normal(own_key, dims, jnp.float32) * spread
    if len(cuts) > 0:
        result = block_levels(own_key, dims, cuts, -0.22, 0.18) * result
    return jnp.clip(result, min=-most, max=most).astype(held_as)


def heavy_noise(own_key, extent, scale, reach, shards, heavy, dtype=jnp.bfloat16):
    array = scale * jax.random.normal(own_key, extent, jnp.float32)
    if shards:
        array = array * block_levels(own_key, extent, shards, -0.22, 0.18)
    return jnp.clip(spiked(array, jax.random.fold_in(own_key, 3), *heavy), -reach, reach).astype(dtype)


def setup_inputs(seed: int = 0) -> dict:
    seeds = jax.random.split(jax.random.key(seed), 9)
    return {
        "residual_in": draw_residual_in(jax.random.fold_in(seeds[8], 71), 0),
        "norm_gain": jnp.clip(1.0 + 0.18 * jax.random.normal(seeds[1], (LAYERS, D), jnp.float32), 0.1, 1.9),
        "gate_proj": normal_values(seeds[2], (LAYERS, D, CW), D ** -0.5, 0.09375, ((1, 4), (2, 8))),
        "filter_proj": normal_values(seeds[3], (LAYERS, D, CW), D ** -0.5, 0.09375, ((1, 4), (2, 8))),
        "signal_proj": normal_values(seeds[4], (LAYERS, D, CW), D ** -0.5, 0.09375, ((1, 4), (2, 8))),
        "conv_taps": normal_values(seeds[5], (LAYERS, TAPS, CW), 0.6, 3.0, ((2, 8),), jnp.float32),
        "out_proj": heavy_noise(seeds[6], (LAYERS, CW, D), CW ** -0.5, 0.1875, ((1, 8), (2, 4)), (1, 2, 8, 2.0)),
        "final_gain": jnp.clip(1.0 + 0.18 * jax.random.normal(seeds[7], (D,), jnp.float32), 0.1, 1.9),
    }


norm_floor = 1e-06

def rms_scaled(values, gain_row):
    mean_square = lax.optimization_barrier(jnp.mean(values * values, axis=-1, keepdims=True))
    return values * lax.rsqrt(mean_square + norm_floor) * gain_row

def stored(values):
    return lax.optimization_barrier(values.astype(jnp.bfloat16)).astype(jnp.float32)

def causal_filter(product, taps):
    width_taps = taps.shape[0]
    length = product.shape[0]
    padded = jnp.concatenate([jnp.zeros((width_taps - 1, product.shape[1]), jnp.bfloat16), product], axis=0)
    filtered = jnp.zeros(product.shape, jnp.float32)
    for tap_index in range(width_taps):
        filtered = filtered + taps[tap_index] * padded[tap_index:tap_index + length].astype(jnp.float32)
    return filtered

def reference(residual_in, norm_gain, gate_proj, filter_proj, signal_proj, conv_taps, out_proj, final_gain):
    stream = residual_in
    block_width = CW // N_TP
    for layer_number in range(LAYERS):
        normed = rms_scaled(stream.astype(jnp.float32), norm_gain[layer_number]).astype(jnp.bfloat16)
        gate_rows = stored(jnp.dot(normed, gate_proj[layer_number], preferred_element_type=jnp.float32))
        filter_in = stored(jnp.dot(normed, filter_proj[layer_number], preferred_element_type=jnp.float32))
        signal_rows = stored(jnp.dot(normed, signal_proj[layer_number], preferred_element_type=jnp.float32))
        product = (filter_in * signal_rows).astype(jnp.bfloat16)
        filtered = causal_filter(product, conv_taps[layer_number])
        mixed_rows = (gate_rows * filtered).astype(jnp.bfloat16)
        branch = jnp.zeros((mixed_rows.shape[0], D), jnp.float32)
        for block_number in range(N_TP):
            lower_col = block_number * block_width
            partial_sum = jnp.dot(mixed_rows[:, lower_col:lower_col + block_width], out_proj[layer_number, lower_col:lower_col + block_width], preferred_element_type=jnp.float32)
            branch = branch + stored(partial_sum)
        stream = (stream.astype(jnp.float32) + branch).astype(jnp.bfloat16)
    return rms_scaled(stream.astype(jnp.float32), final_gain)
```

```python
import functools
import heapq

import jax
import jax.numpy as jnp
from jax import lax
from jax.experimental import pallas as pl
from jax.experimental.pallas import tpu as pltpu
from jax.sharding import PartitionSpec as P

MESH = pl.DeviceIdType.MESH
NORM_FLOOR = 1e-06
TILES = 4
CHUNK_US = 11.2
HOP_US = 2.0
f32 = jnp.float32
bf16 = jnp.bfloat16


def grid_width(count):
    height = max(h for h in range(1, count + 1) if count % h == 0 and h * h <= count)
    return count // height


def snake(index, width):
    y, x = index // width, index % width
    return y * width + x + (y % 2) * (width - 1 - 2 * x)


def line_plan(count, tiles, reduce, gather):
    unit = CHUNK_US / tiles
    heap, left, ready = [], {}, {}
    for z in range(count):
        for tile in range(tiles):
            if not reduce:
                heap.append((0.0, tile, 0, z, ("F", tile, z)))
                continue
            left[z, ("F", tile, z)] = (z > 0) + (z < count - 1)
            if left[z, ("F", tile, z)] == 0:
                heap.append((0.0, tile, 0, z, ("F", tile, z)))
            if z == 0:
                for d in range(1, count):
                    order = (tile, count - d) if gather else (count - d, tile)
                    heap.append((0.0, *order, z, ("R", tile, d)))
            if z == count - 1:
                for d in range(count - 1):
                    order = (tile, d) if gather else (d, tile)
                    heap.append((0.0, *order, z, ("L", tile, d)))
    heapq.heapify(heap)
    free = {}
    out = [[] for _ in range(count)]

    def send(now, z, step, event):
        begin = max(now, free.get((z, step), 0.0))
        free[z, step] = begin + unit
        key = (z + step, event)
        ready[key] = max(ready.get(key, 0.0), begin + unit + HOP_US)
        left[key] = left.get(key, 1) - 1
        if left[key] == 0:
            heapq.heappush(heap, (ready[key], event[1], 0, z + step, event))

    while heap:
        now, _, _, z, event = heapq.heappop(heap)
        kind, tile, which = event
        out[z].append((now, event))
        if kind in "RL":
            step = 1 if kind == "R" else -1
            send(now, z, step, ("F", tile, which) if which == z + step else event)
        elif kind == "F" and gather:
            if z + 1 < count:
                send(now, z, 1, ("GR", tile, z))
            if z > 0:
                send(now, z, -1, ("GL", tile, z))
        elif kind == "GR" and z + 1 < count:
            send(now, z, 1, event)
        elif kind == "GL" and z > 0:
            send(now, z, -1, event)
    return out


def kernel(
    sizes,
    residual, gain_in, filter_w, signal_w, gate_w, out_w, taps_in,
    result, scales,
    stream, normed, weights, outs, own_part, pair_send, pair_recv, line_recv,
    filter_rows, signal_rows, product, edge_send, edge_recv, mixed, closing, squares, gain, taps, scale_rows,
    weight_send, weight_recv, gather_send, gather_recv, twin_send, twin_recv,
    reduce_send, reduce_recv, pair_send_sem, pair_recv_sem,
    edge_send_sem, edge_recv_sem, square_send, square_recv, local_sem,
):
    S, T, L, R, F, C, DS, TAPS = sizes
    NZ, TB, RT, H, D = T // 2, T // S, R // TILES, S // 2, T * F
    width = grid_width(S)
    s, t = lax.axis_index("sp"), lax.axis_index("tp")
    z, core = t // 2, t % 2
    partner = (s, t + 1 - 2 * core)
    position = snake(s, width)

    def at_position(p):
        return snake((p + 2 * S) % S, width)

    ring = [(at_position(position + 1), t), (at_position(position - 1), t)]
    last = L - 1

    barrier = pltpu.get_barrier_semaphore()
    for k in range(1, T):
        pl.semaphore_signal(barrier, inc=1, device_id=(s, (t + k) % T), device_id_type=MESH)
    for other in range(1, S):
        pl.semaphore_signal(barrier, inc=1, device_id=((s + other) % S, t), device_id_type=MESH)

    locals_ = []

    def local(src, dst):
        copy = pltpu.make_async_copy(src, dst, local_sem.at[len(locals_)])
        copy.start()
        locals_.append(copy)

    local(residual, stream.at[0, t])
    local(gain_in, gain)
    local(taps_in, taps)
    for l in range(L):
        for k, w in enumerate((filter_w, signal_w, gate_w)):
            local(w.at[l], weights.at[l, k, pl.ds(s * TB, TB)])
        local(out_w.at[l], outs.at[l, s])
    pl.semaphore_wait(barrier, T - 1 + S - 1)

    def weight_ref(i, slot, half):
        l, k = divmod(i, 4)
        if k < 3:
            if half is None:
                return weights.at[l, k, pl.ds(slot * TB, TB)]
            return weights.at[l, k, pl.ds(slot * TB, TB), pl.ds(half * (F // 2), F // 2)]
        if half is None:
            return outs.at[l, slot]
        return outs.at[l, slot, pl.ds(half * (C // 2), C // 2)]

    def weight_source(i, half):
        l, k = divmod(i, 4)
        ref = (filter_w, signal_w, gate_w, out_w)[k]
        if half is None:
            return ref.at[l]
        if k < 3:
            return ref.at[l, pl.ds(0, TB), pl.ds(half * (F // 2), F // 2)]
        return ref.at[l, pl.ds(half * (C // 2), C // 2)]

    def weight_copy(i, direction, hop, receive=False):
        sign = 1 if direction == 0 else -1
        half = direction if hop == H else None
        slot = at_position(position - sign * (hop if receive else hop - 1))
        dst = weight_ref(i, slot, half)
        src = weight_source(i, half) if hop == 1 and not receive else dst
        return pltpu.make_async_remote_copy(
            src_ref=src, dst_ref=dst,
            send_sem=weight_send.at[i, direction, hop - 1],
            recv_sem=weight_recv.at[i, direction, hop - 1],
            device_id=ring[direction], device_id_type=MESH,
        )

    def weight_first(i):
        if i < 4 * L:
            for direction in range(2):
                weight_copy(i, direction, 1).start()

    def weight_forward(i):
        for hop in range(1, H):
            for direction in range(2):
                weight_copy(i, direction, hop, True).wait_recv()
                weight_copy(i, direction, hop + 1).start()
        for step in ((2,), (2,), (), (1, 2))[i % 4]:
            weight_first(i + step)

    def weight_ready(i):
        for direction in range(2):
            weight_copy(i, direction, H, True).wait_recv()

    def rows_of(tile):
        return pl.ds(tile * RT, RT)

    def gather_copy(l, tile, src, direction):
        ref = stream.at[l, 2 * src + core, rows_of(tile)]
        return pltpu.make_async_remote_copy(
            src_ref=ref, dst_ref=ref,
            send_sem=gather_send.at[l, tile, direction, src],
            recv_sem=gather_recv.at[l, tile, direction, src],
            device_id=(s, (t + (2 if direction == 0 else T - 2)) % T), device_id_type=MESH,
        )

    def twin_copy(l, tile, src, receive=False):
        block = 2 * src + (1 - core if receive else core)
        ref = stream.at[l, block, rows_of(tile)]
        return pltpu.make_async_remote_copy(
            src_ref=ref, dst_ref=ref,
            send_sem=twin_send.at[l, tile, src], recv_sem=twin_recv.at[l, tile, src],
            device_id=partner, device_id_type=MESH,
        )

    def reduce_copy(l, tile, d, direction):
        return pltpu.make_async_remote_copy(
            src_ref=own_part.at[l, d, rows_of(tile)],
            dst_ref=line_recv.at[l, direction, d, rows_of(tile)],
            send_sem=reduce_send.at[l, tile, direction, d],
            recv_sem=reduce_recv.at[l, tile, direction, d],
            device_id=(s, (t + (2 if direction == 0 else T - 2)) % T), device_id_type=MESH,
        )

    def pair_copy(l, tile, d):
        return pltpu.make_async_remote_copy(
            src_ref=pair_send.at[l, d, rows_of(tile)], dst_ref=pair_recv.at[l, d, rows_of(tile)],
            send_sem=pair_send_sem.at[l, tile, d], recv_sem=pair_recv_sem.at[l, tile, d],
            device_id=partner, device_id_type=MESH,
        )

    def total_into(l, tile, d, incoming, base, store):
        step = min(RT, 32)

        def body(i, _):
            rows = pl.ds(pl.multiple_of(tile * RT + i * step, step), step)
            value = own_part[l, d, rows].astype(f32) + pair_recv[l, d, rows].astype(f32)
            for direction in incoming:
                value = value + line_recv[l, direction, d, rows].astype(f32)
            if base:
                value = stream[l, t, rows].astype(f32) + value
            store(rows, value.astype(bf16))
            return 0

        lax.fori_loop(0, RT // step, body, 0)

    def square_copy(tile, k, receive=False):
        block = (t + T - k) % T if receive else t
        return pltpu.make_async_remote_copy(
            src_ref=squares.at[tile, block], dst_ref=squares.at[tile, block],
            send_sem=square_send.at[tile, k], recv_sem=square_recv.at[tile, k],
            device_id=(s, (t + k) % T), device_id_type=MESH,
        )

    def close(tile):
        acc = jnp.zeros((RT, 128), f32)
        for b in range(F // 128):
            value = closing[tile * RT:(tile + 1) * RT, b * 128:(b + 1) * 128].astype(f32)
            acc = acc + value * value
        squares[tile, t] = jnp.sum(acc.T, axis=0, keepdims=True)
        for k in range(1, T):
            square_copy(tile, k).start()

    def run_event(zi, l, event, gather_layer):
        kind, tile, which = event
        if kind in "RL":
            direction = 0 if kind == "R" else 1
            pair_copy(l, tile, which).wait_recv()
            incoming = [direction] if (zi > 0 if direction == 0 else zi < NZ - 1) else []
            for d in incoming:
                reduce_copy(l, tile, which, d).wait_recv()

            def store(rows, value):
                own_part[l, which, rows] = value

            total_into(l, tile, which, incoming, False, store)
            reduce_copy(l, tile, which, direction).start()
        elif kind == "F":
            if l is not None:
                pair_copy(l, tile, zi).wait_recv()
                incoming = ([0] if zi > 0 else []) + ([1] if zi < NZ - 1 else [])
                for d in incoming:
                    reduce_copy(l, tile, zi, d).wait_recv()

                def store(rows, value):
                    if l < last:
                        stream[l + 1, t, rows] = value
                    else:
                        closing[rows] = value

                total_into(l, tile, zi, incoming, True, store)
                if l == last:
                    close(tile)
            if gather_layer is not None:
                if zi + 1 < NZ:
                    gather_copy(gather_layer, tile, zi, 0).start()
                if zi > 0:
                    gather_copy(gather_layer, tile, zi, 1).start()
                twin_copy(gather_layer, tile, zi).start()
        else:
            direction = 0 if kind == "GR" else 1
            gather_copy(gather_layer, tile, which, direction).wait_recv()
            if (zi + 1 < NZ) if direction == 0 else (zi > 0):
                gather_copy(gather_layer, tile, which, direction).start()
            twin_copy(gather_layer, tile, which).start()

    def run_phase(l, gather_layer, weight_events):
        plan = line_plan(NZ, TILES, l is not None, gather_layer is not None)
        for zi in range(NZ):
            events = [
                (now, n, e) for n, (now, e) in enumerate(plan[zi])
                if (e[0], zi) not in (("R", 0), ("L", NZ - 1))
            ]
            events += [(now, -1, ("W", i, 0)) for now, i in weight_events if i < 4 * L]
            if gather_layer is not None:
                for tile in range(TILES):
                    arrived = max(now for now, e in plan[zi] if e[1] == tile)
                    events.append((arrived + HOP_US, TILES * T * T, ("N", tile, 0)))
            events.sort(key=lambda e: (e[0], e[1]))

            @pl.when(z == zi)
            def _():
                for _, _, event in events:
                    if event[0] == "W":
                        weight_forward(event[1])
                    elif event[0] == "N":
                        normalize(gather_layer, event[1])
                    else:
                        run_event(zi, l, event, gather_layer)

    def normalize(l, tile):
        for src in range(NZ):
            twin_copy(l, tile, src, True).wait_recv()
        step = min(RT, 16)

        def body(i, _):
            rows = pl.ds(pl.multiple_of(tile * RT + i * step, step), step)
            acc = jnp.zeros((step, F), f32)
            for b in range(T):
                value = stream[l, b, rows].astype(f32)
                acc = acc + value * value
            scale = lax.rsqrt(jnp.sum(acc, axis=1, keepdims=True) / D + NORM_FLOOR)
            for b in range(T):
                value = stream[l, b, rows].astype(f32)
                normed[rows, b * F:(b + 1) * F] = (value * scale * gain[l:l + 1, b * F:(b + 1) * F]).astype(bf16)
            return 0

        lax.fori_loop(0, RT // step, body, 0)

    def project(l, k, into):
        step = min(R, 256)

        def body(i, _):
            rows = pl.ds(pl.multiple_of(i * step, step), step)
            value = jnp.dot(
                normed[rows, :], weights[l, k].reshape(D, C), preferred_element_type=f32
            )
            into[rows, :] = value.astype(bf16)
            return 0

        lax.fori_loop(0, R // step, body, 0)

    def edge_copy(l):
        return pltpu.make_async_remote_copy(
            src_ref=edge_send.at[l], dst_ref=edge_recv.at[l],
            send_sem=edge_send_sem.at[l], recv_sem=edge_recv_sem.at[l],
            device_id=((s + 1) % S, t), device_id_type=MESH,
        )

    def mix(l):
        weight_ready(4 * l)
        project(l, 0, filter_rows)
        weight_ready(4 * l + 1)
        project(l, 1, signal_rows)
        value = (filter_rows[...].astype(f32) * signal_rows[...].astype(f32)).astype(bf16)
        product[8:8 + R, :] = value.astype(f32)
        edge_send[l] = value[R - 16:, :]

        @pl.when(s < S - 1)
        def _():
            edge_copy(l).start()

        if l == 0:
            weight_forward(4 * l + 3)
        weight_ready(4 * l + 2)

        @pl.when(s > 0)
        def _():
            edge_copy(l).wait_recv()
            product[0:8, :] = edge_recv[l].astype(f32)[8:, :]

        @pl.when(s == 0)
        def _():
            product[0:8, :] = jnp.zeros((8, C), f32)

    order = sorted(range(NZ), key=lambda d: (min(d, NZ - 1 - d), -d))

    def partials(l, tile):
        first, rows = tile * RT, slice(tile * RT, (tile + 1) * RT)
        gate = jnp.dot(
            normed[rows, :], weights[l, 2].reshape(D, C), preferred_element_type=f32
        ).astype(bf16)
        filtered = jnp.zeros((RT, C), f32)
        for k in range(TAPS):
            begin = 8 - (TAPS - 1) + k + first
            filtered = filtered + taps[k, l:l + 1, :] * product[begin:begin + RT, :]
        mixed[rows, :] = (gate.astype(f32) * filtered).astype(bf16)
        if tile == 0:
            weight_ready(4 * l + 3)
        for own in (False, True):
            for d in order:
                block = 2 * d + (core if own else 1 - core)
                columns = pl.ds(pl.multiple_of((block % TB) * F, F), F)
                value = jnp.dot(
                    mixed[rows, :], outs[l, block // TB, :, columns], preferred_element_type=f32
                ).astype(bf16)
                if own:
                    own_part[l, d, rows] = value
                else:
                    pair_send[l, d, rows] = value
                    pair_copy(l, tile, d).start()

    def launch(l, tile, near=0, far=NZ):
        @pl.when(z == 0)
        def _():
            for d in range(NZ - 1, 0, -1):
                if near <= d < far:
                    run_event(0, l, ("R", tile, d), None)

        @pl.when(z == NZ - 1)
        def _():
            for d in range(NZ - 1):
                if near <= NZ - 1 - d < far:
                    run_event(NZ - 1, l, ("L", tile, d), None)

    def drain_gather(l):
        for tile in range(TILES):
            for d in range(NZ):
                twin_copy(l, tile, d).wait_send()

                @pl.when((z < NZ - 1) & (d <= z))
                def _():
                    gather_copy(l, tile, d, 0).wait_send()

                @pl.when((z > 0) & (d >= z))
                def _():
                    gather_copy(l, tile, d, 1).wait_send()

    def drain_reduce(l):
        @pl.when(s < S - 1)
        def _():
            edge_copy(l).wait_send()

        for tile in range(TILES):
            for d in range(NZ):
                pair_copy(l, tile, d).wait_send()

                @pl.when((z < NZ - 1) & (d > z))
                def _():
                    reduce_copy(l, tile, d, 0).wait_send()

                @pl.when((z > 0) & (d < z))
                def _():
                    reduce_copy(l, tile, d, 1).wait_send()

    def drain_weights(first, end):
        for i in range(first, end):
            for direction in range(2):
                for hop in range(1, H + 1):
                    weight_copy(i, direction, hop).wait_send()

    weight_first(0)
    weight_first(1)
    for copy in locals_[:3]:
        copy.wait()
    run_phase(None, 0, ((13.0, 0), (24.0, 1)))
    for copy in locals_[3:]:
        copy.wait()
    weight_forward(2)
    for l in range(L):
        mix(l)
        if l == 1:
            drain_gather(0)
        if l > 0:
            drain_gather(l)
            drain_reduce(l - 1)
            drain_weights(4 * l - 4, 4 * l)
        for tile in range(TILES):
            partials(l, tile)
            if tile > 0:
                launch(l, tile - 1, 0 if l < last else NZ - 1)
        launch(l, TILES - 1, 0 if l < last else NZ - 1)
        if l < last:
            run_phase(l, l + 1, ((8.0, 4 * l + 4), (20.0, 4 * l + 5), (36.0, 4 * l + 6), (52.0, 4 * l + 7)))
        else:
            for distance in range(NZ - 2, 0, -1):
                for tile in range(TILES):
                    launch(l, tile, distance, distance + 1)
            run_phase(l, None, ())

    drain_reduce(last)
    drain_weights(4 * last, 4 * L)
    for tile in range(TILES):
        for k in range(1, T):
            square_copy(tile, k, True).wait_recv()
        total = squares[tile, 0]
        for k in range(1, T):
            total = total + squares[tile, k]
        scale = lax.rsqrt(total / D + NORM_FLOOR)
        scale_rows[tile * RT:(tile + 1) * RT, :] = jnp.broadcast_to(scale, (128, RT)).T
    outgoing = [
        pltpu.make_async_copy(closing, result, local_sem.at[0]),
        pltpu.make_async_copy(scale_rows, scales, local_sem.at[1]),
    ]
    for copy in outgoing:
        copy.start()
    for copy in outgoing:
        copy.wait()

    for tile in range(TILES):
        for k in range(1, T):
            square_copy(tile, k).wait_send()


def finish(pieces, closing, scale, gain, result, rows_in, scale_in, gain_in, rows_out, sems, gain_sem):
    R, F = rows_in.shape
    step = R // pieces
    gains = pltpu.make_async_copy(gain, gain_in, gain_sem)
    gains.start()

    def copies(i):
        rows = pl.ds(i * step, step)
        return (
            pltpu.make_async_copy(closing.at[rows], rows_in.at[rows], sems.at[i, 0]),
            pltpu.make_async_copy(scale.at[rows], scale_in.at[rows], sems.at[i, 1]),
            pltpu.make_async_copy(rows_out.at[rows], result.at[rows], sems.at[i, 2]),
        )

    for i in range(pieces):
        copies(i)[0].start()
        copies(i)[1].start()
    gains.wait()
    for i in range(pieces):
        copies(i)[0].wait()
        copies(i)[1].wait()
        rows = slice(i * step, (i + 1) * step)
        for b in range(F // 128):
            columns = slice(b * 128, (b + 1) * 128)
            rows_out[rows, columns] = (
                rows_in[rows, columns].astype(f32) * scale_in[rows, :] * gain_in[:, columns]
            )
        copies(i)[2].start()
    for i in range(pieces):
        copies(i)[2].wait()


def per_device(
    S, T, residual_in, norm_gain, gate_proj, filter_proj, signal_proj, conv_taps, out_proj, final_gain
):
    R, F = residual_in.shape
    L, DS, C = gate_proj.shape
    TAPS = conv_taps.shape[1]
    NZ, TB, H = T // 2, T // S, S // 2
    dma = pltpu.SemaphoreType.DMA
    cut = lambda w: w.reshape(L, TB, F, C)
    any_space = pl.BlockSpec(memory_space=pl.ANY)
    closing, scale = pl.pallas_call(
        functools.partial(kernel, (S, T, L, R, F, C, DS, TAPS)),
        out_shape=(jax.ShapeDtypeStruct((R, F), bf16), jax.ShapeDtypeStruct((R, 128), f32)),
        in_specs=[any_space] * 7,
        out_specs=(any_space, any_space),
        scratch_shapes=[
            pltpu.VMEM((L, T, R, F), bf16),
            pltpu.VMEM((R, T * F), bf16),
            pltpu.VMEM((L, 3, T, F, C), bf16),
            pltpu.VMEM((L, S, C, DS), bf16),
            pltpu.VMEM((L, NZ, R, F), bf16),
            pltpu.VMEM((L, NZ, R, F), bf16),
            pltpu.VMEM((L, NZ, R, F), bf16),
            pltpu.VMEM((L, 2, NZ, R, F), bf16),
            pltpu.VMEM((R, C), bf16),
            pltpu.VMEM((R, C), bf16),
            pltpu.VMEM((R + 8, C), f32),
            pltpu.VMEM((L, 16, C), bf16),
            pltpu.VMEM((L, 16, C), bf16),
            pltpu.VMEM((R, C), bf16),
            pltpu.VMEM((R, F), bf16),
            pltpu.VMEM((TILES, T, 1, R // TILES), f32),
            pltpu.VMEM((L, T * F), f32),
            pltpu.VMEM((TAPS, L, C), f32),
            pltpu.VMEM((R, 128), f32),
            dma((4 * L, 2, H)), dma((4 * L, 2, H)),
            dma((L, TILES, 2, NZ)), dma((L, TILES, 2, NZ)),
            dma((L, TILES, NZ)), dma((L, TILES, NZ)),
            dma((L, TILES, 2, NZ)), dma((L, TILES, 2, NZ)),
            dma((L, TILES, NZ)), dma((L, TILES, NZ)),
            dma((L,)), dma((L,)),
            dma((TILES, T)), dma((TILES, T)),
            dma((4 * L + 3,)),
        ],
        compiler_params=pltpu.CompilerParams(
            collective_id=0, has_side_effects=True, vmem_limit_bytes=60 * 2**20
        ),
        name="mixers",
    )(
        residual_in, norm_gain, cut(filter_proj), cut(signal_proj),
        cut(gate_proj), out_proj, conv_taps.transpose(1, 0, 2),
    )
    return pl.pallas_call(
        functools.partial(finish, 4),
        out_shape=jax.ShapeDtypeStruct((R, F), f32),
        in_specs=[any_space] * 3,
        out_specs=any_space,
        scratch_shapes=[
            pltpu.VMEM((R, F), bf16), pltpu.VMEM((R, 128), f32), pltpu.VMEM((1, F), f32),
            pltpu.VMEM((R, F), f32), dma((4, 3)), dma,
        ],
        name="finish",
    )(closing, scale, final_gain.reshape(1, F))


def solution(mesh):
    return jax.shard_map(
        functools.partial(per_device, mesh.shape["sp"], mesh.shape["tp"]),
        mesh=mesh,
        in_specs=(
            P("sp", "tp"),
            P(),
            P(None, "sp", "tp"),
            P(None, "sp", "tp"),
            P(None, "sp", "tp"),
            P(None, None, "tp"),
            P(None, "tp", "sp"),
            P("tp"),
        ),
        out_specs=P("sp", "tp"),
        check_vma=False,
    )
```

```python
import functools
import heapq

import jax
import jax.numpy as jnp
from jax import lax
from jax.experimental import pallas as pl
from jax.experimental.pallas import tpu as pltpu
from jax.sharding import PartitionSpec as P

MESH = pl.DeviceIdType.MESH
NORM_FLOOR = 1e-06
TILES = 4
CHUNK_US = 11.2
HOP_US = 2.0
f32 = jnp.float32
bf16 = jnp.bfloat16


def grid_width(count):
    height = max(h for h in range(1, count + 1) if count % h == 0 and h * h <= count)
    return count // height


def snake(index, width):
    y, x = index // width, index % width
    return y * width + x + (y % 2) * (width - 1 - 2 * x)


def line_plan(count, tiles, reduce, gather):
    unit = CHUNK_US / tiles
    heap, left, ready = [], {}, {}
    for z in range(count):
        for tile in range(tiles):
            if not reduce:
                heap.append((0.0, tile, 0, z, ("F", tile, z)))
                continue
            left[z, ("F", tile, z)] = (z > 0) + (z < count - 1)
            if left[z, ("F", tile, z)] == 0:
                heap.append((0.0, tile, 0, z, ("F", tile, z)))
            if z == 0:
                for d in range(1, count):
                    order = (tile, count - d) if gather else (count - d, tile)
                    heap.append((0.0, *order, z, ("R", tile, d)))
            if z == count - 1:
                for d in range(count - 1):
                    order = (tile, d) if gather else (d, tile)
                    heap.append((0.0, *order, z, ("L", tile, d)))
    heapq.heapify(heap)
    free = {}
    out = [[] for _ in range(count)]

    def send(now, z, step, event):
        begin = max(now, free.get((z, step), 0.0))
        free[z, step] = begin + unit
        key = (z + step, event)
        ready[key] = max(ready.get(key, 0.0), begin + unit + HOP_US)
        left[key] = left.get(key, 1) - 1
        if left[key] == 0:
            heapq.heappush(heap, (ready[key], event[1], 0, z + step, event))

    while heap:
        now, _, _, z, event = heapq.heappop(heap)
        kind, tile, which = event
        out[z].append((now, event))
        if kind in "RL":
            step = 1 if kind == "R" else -1
            send(now, z, step, ("F", tile, which) if which == z + step else event)
        elif kind == "F" and gather:
            if z + 1 < count:
                send(now, z, 1, ("GR", tile, z))
            if z > 0:
                send(now, z, -1, ("GL", tile, z))
        elif kind == "GR" and z + 1 < count:
            send(now, z, 1, event)
        elif kind == "GL" and z > 0:
            send(now, z, -1, event)
    return out


def kernel(
    sizes,
    residual, gain_in, filter_w, signal_w, gate_w, out_w, taps_in,
    result, scales,
    stream, normed, weights, outs, own_part, pair_send, pair_recv, line_recv,
    filter_rows, signal_rows, product, edge_send, edge_recv, mixed, closing, squares, gain, taps, scale_rows,
    weight_send, weight_recv, gather_send, gather_recv, twin_send, twin_recv,
    reduce_send, reduce_recv, pair_send_sem, pair_recv_sem,
    edge_send_sem, edge_recv_sem, square_send, square_recv, local_sem,
):
    S, T, L, R, F, C, DS, TAPS = sizes
    NZ, TB, RT, H, D = T // 2, T // S, R // TILES, S // 2, T * F
    width = grid_width(S)
    s, t = lax.axis_index("sp"), lax.axis_index("tp")
    z, core = t // 2, t % 2
    partner = (s, t + 1 - 2 * core)
    position = snake(s, width)

    def at_position(p):
        return snake((p + 2 * S) % S, width)

    ring = [(at_position(position + 1), t), (at_position(position - 1), t)]
    last = L - 1

    barrier = pltpu.get_barrier_semaphore()
    for k in range(1, T):
        pl.semaphore_signal(barrier, inc=1, device_id=(s, (t + k) % T), device_id_type=MESH)
    for other in range(1, S):
        pl.semaphore_signal(barrier, inc=1, device_id=((s + other) % S, t), device_id_type=MESH)

    locals_ = []

    def local(src, dst):
        copy = pltpu.make_async_copy(src, dst, local_sem.at[len(locals_)])
        copy.start()
        locals_.append(copy)

    local(residual, stream.at[0, t])
    local(gain_in, gain)
    local(taps_in, taps)
    for l in range(L):
        for k, w in enumerate((filter_w, signal_w, gate_w)):
            local(w.at[l], weights.at[l, k, pl.ds(s * TB, TB)])
        local(out_w.at[l], outs.at[l, s])
    pl.semaphore_wait(barrier, T - 1 + S - 1)

    def weight_ref(i, slot, half):
        l, k = divmod(i, 4)
        if k < 3:
            if half is None:
                return weights.at[l, k, pl.ds(slot * TB, TB)]
            return weights.at[l, k, pl.ds(slot * TB, TB), pl.ds(half * (F // 2), F // 2)]
        if half is None:
            return outs.at[l, slot]
        return outs.at[l, slot, pl.ds(half * (C // 2), C // 2)]

    def weight_source(i, half):
        l, k = divmod(i, 4)
        ref = (filter_w, signal_w, gate_w, out_w)[k]
        if half is None:
            return ref.at[l]
        if k < 3:
            return ref.at[l, pl.ds(0, TB), pl.ds(half * (F // 2), F // 2)]
        return ref.at[l, pl.ds(half * (C // 2), C // 2)]

    def weight_copy(i, direction, hop, receive=False):
        sign = 1 if direction == 0 else -1
        half = direction if hop == H else None
        slot = at_position(position - sign * (hop if receive else hop - 1))
        dst = weight_ref(i, slot, half)
        src = weight_source(i, half) if hop == 1 and not receive else dst
        return pltpu.make_async_remote_copy(
            src_ref=src, dst_ref=dst,
            send_sem=weight_send.at[i, direction, hop - 1],
            recv_sem=weight_recv.at[i, direction, hop - 1],
            device_id=ring[direction], device_id_type=MESH,
        )

    def weight_first(i):
        if i < 4 * L:
            for direction in range(2):
                weight_copy(i, direction, 1).start()

    def weight_forward(i):
        for hop in range(1, H):
            for direction in range(2):
                weight_copy(i, direction, hop, True).wait_recv()
                weight_copy(i, direction, hop + 1).start()
        for step in ((2,), (2,), (), (1, 2))[i % 4]:
            weight_first(i + step)

    def weight_ready(i):
        for direction in range(2):
            weight_copy(i, direction, H, True).wait_recv()

    def rows_of(tile):
        return pl.ds(tile * RT, RT)

    def gather_copy(l, tile, src, direction):
        ref = stream.at[l, 2 * src + core, rows_of(tile)]
        return pltpu.make_async_remote_copy(
            src_ref=ref, dst_ref=ref,
            send_sem=gather_send.at[l, tile, direction, src],
            recv_sem=gather_recv.at[l, tile, direction, src],
            device_id=(s, (t + (2 if direction == 0 else T - 2)) % T), device_id_type=MESH,
        )

    def twin_copy(l, tile, src, receive=False):
        block = 2 * src + (1 - core if receive else core)
        ref = stream.at[l, block, rows_of(tile)]
        return pltpu.make_async_remote_copy(
            src_ref=ref, dst_ref=ref,
            send_sem=twin_send.at[l, tile, src], recv_sem=twin_recv.at[l, tile, src],
            device_id=partner, device_id_type=MESH,
        )

    def reduce_copy(l, tile, d, direction):
        return pltpu.make_async_remote_copy(
            src_ref=own_part.at[l, d, rows_of(tile)],
            dst_ref=line_recv.at[l, direction, d, rows_of(tile)],
            send_sem=reduce_send.at[l, tile, direction, d],
            recv_sem=reduce_recv.at[l, tile, direction, d],
            device_id=(s, (t + (2 if direction == 0 else T - 2)) % T), device_id_type=MESH,
        )

    def pair_copy(l, tile, d):
        return pltpu.make_async_remote_copy(
            src_ref=pair_send.at[l, d, rows_of(tile)], dst_ref=pair_recv.at[l, d, rows_of(tile)],
            send_sem=pair_send_sem.at[l, tile, d], recv_sem=pair_recv_sem.at[l, tile, d],
            device_id=partner, device_id_type=MESH,
        )

    def total_into(l, tile, d, incoming, base, store):
        step = min(RT, 32)

        def body(i, _):
            rows = pl.ds(pl.multiple_of(tile * RT + i * step, step), step)
            value = own_part[l, d, rows].astype(f32) + pair_recv[l, d, rows].astype(f32)
            for direction in incoming:
                value = value + line_recv[l, direction, d, rows].astype(f32)
            if base:
                value = stream[l, t, rows].astype(f32) + value
            store(rows, value.astype(bf16))
            return 0

        lax.fori_loop(0, RT // step, body, 0)

    def square_copy(tile, k, receive=False):
        block = (t + T - k) % T if receive else t
        return pltpu.make_async_remote_copy(
            src_ref=squares.at[tile, block], dst_ref=squares.at[tile, block],
            send_sem=square_send.at[tile, k], recv_sem=square_recv.at[tile, k],
            device_id=(s, (t + k) % T), device_id_type=MESH,
        )

    def close(tile):
        acc = jnp.zeros((RT, 128), f32)
        for b in range(F // 128):
            value = closing[tile * RT:(tile + 1) * RT, b * 128:(b + 1) * 128].astype(f32)
            acc = acc + value * value
        squares[tile, t] = jnp.sum(acc.T, axis=0, keepdims=True)
        for k in range(1, T):
            square_copy(tile, k).start()

    def run_event(zi, l, event, gather_layer):
        kind, tile, which = event
        if kind in "RL":
            direction = 0 if kind == "R" else 1
            pair_copy(l, tile, which).wait_recv()
            incoming = [direction] if (zi > 0 if direction == 0 else zi < NZ - 1) else []
            for d in incoming:
                reduce_copy(l, tile, which, d).wait_recv()

            def store(rows, value):
                own_part[l, which, rows] = value

            total_into(l, tile, which, incoming, False, store)
            reduce_copy(l, tile, which, direction).start()
        elif kind == "F":
            if l is not None:
                pair_copy(l, tile, zi).wait_recv()
                incoming = ([0] if zi > 0 else []) + ([1] if zi < NZ - 1 else [])
                for d in incoming:
                    reduce_copy(l, tile, zi, d).wait_recv()

                def store(rows, value):
                    if l < last:
                        stream[l + 1, t, rows] = value
                    else:
                        closing[rows] = value

                total_into(l, tile, zi, incoming, True, store)
                if l == last:
                    close(tile)
            if gather_layer is not None:
                if zi + 1 < NZ:
                    gather_copy(gather_layer, tile, zi, 0).start()
                if zi > 0:
                    gather_copy(gather_layer, tile, zi, 1).start()
                twin_copy(gather_layer, tile, zi).start()
        else:
            direction = 0 if kind == "GR" else 1
            gather_copy(gather_layer, tile, which, direction).wait_recv()
            if (zi + 1 < NZ) if direction == 0 else (zi > 0):
                gather_copy(gather_layer, tile, which, direction).start()
            twin_copy(gather_layer, tile, which).start()

    def run_phase(l, gather_layer, weight_events):
        plan = line_plan(NZ, TILES, l is not None, gather_layer is not None)
        for zi in range(NZ):
            events = [
                (now, n, e) for n, (now, e) in enumerate(plan[zi])
                if (e[0], zi) not in (("R", 0), ("L", NZ - 1))
            ]
            events += [(now, -1, ("W", i, 0)) for now, i in weight_events if i < 4 * L]
            if gather_layer is not None:
                for tile in range(TILES):
                    arrived = max(now for now, e in plan[zi] if e[1] == tile)
                    events.append((arrived + HOP_US, TILES * T * T, ("N", tile, 0)))
            events.sort(key=lambda e: (e[0], e[1]))

            @pl.when(z == zi)
            def _():
                for _, _, event in events:
                    if event[0] == "W":
                        weight_forward(event[1])
                    elif event[0] == "N":
                        normalize(gather_layer, event[1])
                    else:
                        run_event(zi, l, event, gather_layer)

    def normalize(l, tile):
        for src in range(NZ):
            twin_copy(l, tile, src, True).wait_recv()
        step = min(RT, 16)

        def body(i, _):
            rows = pl.ds(pl.multiple_of(tile * RT + i * step, step), step)
            acc = jnp.zeros((step, F), f32)
            for b in range(T):
                value = stream[l, b, rows].astype(f32)
                acc = acc + value * value
            scale = lax.rsqrt(jnp.sum(acc, axis=1, keepdims=True) / D + NORM_FLOOR)
            for b in range(T):
                value = stream[l, b, rows].astype(f32)
                normed[rows, b * F:(b + 1) * F] = (value * scale * gain[l:l + 1, b * F:(b + 1) * F]).astype(bf16)
            return 0

        lax.fori_loop(0, RT // step, body, 0)

    def project(l, k, into):
        step = min(R, 256)

        def body(i, _):
            rows = pl.ds(pl.multiple_of(i * step, step), step)
            value = jnp.dot(
                normed[rows, :], weights[l, k].reshape(D, C), preferred_element_type=f32
            )
            into[rows, :] = value.astype(bf16)
            return 0

        lax.fori_loop(0, R // step, body, 0)

    def edge_copy(l):
        return pltpu.make_async_remote_copy(
            src_ref=edge_send.at[l], dst_ref=edge_recv.at[l],
            send_sem=edge_send_sem.at[l], recv_sem=edge_recv_sem.at[l],
            device_id=((s + 1) % S, t), device_id_type=MESH,
        )

    def mix(l):
        weight_ready(4 * l)
        project(l, 0, filter_rows)
        weight_ready(4 * l + 1)
        project(l, 1, signal_rows)
        value = (filter_rows[...].astype(f32) * signal_rows[...].astype(f32)).astype(bf16)
        product[8:8 + R, :] = value.astype(f32)
        edge_send[l] = value[R - 16:, :]

        @pl.when(s < S - 1)
        def _():
            edge_copy(l).start()

        if l == 0:
            weight_forward(4 * l + 3)
        weight_ready(4 * l + 2)

        @pl.when(s > 0)
        def _():
            edge_copy(l).wait_recv()
            product[0:8, :] = edge_recv[l].astype(f32)[8:, :]

        @pl.when(s == 0)
        def _():
            product[0:8, :] = jnp.zeros((8, C), f32)

    order = sorted(range(NZ), key=lambda d: (min(d, NZ - 1 - d), -d))

    def partials(l, tile):
        first, rows = tile * RT, slice(tile * RT, (tile + 1) * RT)
        gate = jnp.dot(
            normed[rows, :], weights[l, 2].reshape(D, C), preferred_element_type=f32
        ).astype(bf16)
        filtered = jnp.zeros((RT, C), f32)
        for k in range(TAPS):
            begin = 8 - (TAPS - 1) + k + first
            filtered = filtered + taps[k, l:l + 1, :] * product[begin:begin + RT, :]
        mixed[rows, :] = (gate.astype(f32) * filtered).astype(bf16)
        if tile == 0:
            weight_ready(4 * l + 3)
        for own in (False, True):
            for d in order:
                block = 2 * d + (core if own else 1 - core)
                columns = pl.ds(pl.multiple_of((block % TB) * F, F), F)
                value = jnp.dot(
                    mixed[rows, :], outs[l, block // TB, :, columns], preferred_element_type=f32
                ).astype(bf16)
                if own:
                    own_part[l, d, rows] = value
                else:
                    pair_send[l, d, rows] = value
                    pair_copy(l, tile, d).start()

    def launch(l, tile, near=0, far=NZ):
        @pl.when(z == 0)
        def _():
            for d in range(NZ - 1, 0, -1):
                if near <= d < far:
                    run_event(0, l, ("R", tile, d), None)

        @pl.when(z == NZ - 1)
        def _():
            for d in range(NZ - 1):
                if near <= NZ - 1 - d < far:
                    run_event(NZ - 1, l, ("L", tile, d), None)

    def drain_gather(l):
        for tile in range(TILES):
            for d in range(NZ):
                twin_copy(l, tile, d).wait_send()

                @pl.when((z < NZ - 1) & (d <= z))
                def _():
                    gather_copy(l, tile, d, 0).wait_send()

                @pl.when((z > 0) & (d >= z))
                def _():
                    gather_copy(l, tile, d, 1).wait_send()

    def drain_reduce(l):
        @pl.when(s < S - 1)
        def _():
            edge_copy(l).wait_send()

        for tile in range(TILES):
            for d in range(NZ):
                pair_copy(l, tile, d).wait_send()

                @pl.when((z < NZ - 1) & (d > z))
                def _():
                    reduce_copy(l, tile, d, 0).wait_send()

                @pl.when((z > 0) & (d < z))
                def _():
                    reduce_copy(l, tile, d, 1).wait_send()

    def drain_weights(first, end):
        for i in range(first, end):
            for direction in range(2):
                for hop in range(1, H + 1):
                    weight_copy(i, direction, hop).wait_send()

    weight_first(0)
    weight_first(1)
    for copy in locals_[:3]:
        copy.wait()
    run_phase(None, 0, ((13.0, 0), (24.0, 1)))
    for copy in locals_[3:]:
        copy.wait()
    weight_forward(2)
    for l in range(L):
        mix(l)
        if l == 1:
            drain_gather(0)
        if l > 0:
            drain_gather(l)
            drain_reduce(l - 1)
            drain_weights(4 * l - 4, 4 * l)
        for tile in range(TILES):
            partials(l, tile)
            if tile > 0:
                launch(l, tile - 1, 0 if l < last else NZ - 1)
        launch(l, TILES - 1, 0 if l < last else NZ - 1)
        if l < last:
            run_phase(l, l + 1, ((8.0, 4 * l + 4), (20.0, 4 * l + 5), (36.0, 4 * l + 6), (52.0, 4 * l + 7)))
        else:
            for distance in range(NZ - 2, 0, -1):
                for tile in range(TILES):
                    launch(l, tile, distance, distance + 1)
            run_phase(l, None, ())

    drain_reduce(last)
    drain_weights(4 * last, 4 * L)
    for tile in range(TILES):
        for k in range(1, T):
            square_copy(tile, k, True).wait_recv()
        total = squares[tile, 0]
        for k in range(1, T):
            total = total + squares[tile, k]
        scale = lax.rsqrt(total / D + NORM_FLOOR)
        scale_rows[tile * RT:(tile + 1) * RT, :] = jnp.broadcast_to(scale, (128, RT)).T
    outgoing = [
        pltpu.make_async_copy(closing, result, local_sem.at[0]),
        pltpu.make_async_copy(scale_rows, scales, local_sem.at[1]),
    ]
    for copy in outgoing:
        copy.start()
    for copy in outgoing:
        copy.wait()

    for tile in range(TILES):
        for k in range(1, T):
            square_copy(tile, k).wait_send()


LINK_SENDS = (
    {0: "u", 4: "u", 2: "c"},
    {1: "ud", 0: "u", 4: "u", 2: "dc", 5: "d"},
    {2: "cd", 1: "u", 0: "u", 4: "u"},
    {3: "c"},
)
NEEDED = (0, 1, 4, 5)


def first_plan(tiles):
    unit = CHUNK_US / tiles
    heap, free = [], {}
    out = [[] for _ in range(4)]
    complete = [{tile: 0.0 for tile in range(tiles)} for _ in range(4)]
    for zz in range(4):
        for tile in range(tiles):
            heapq.heappush(heap, (0.0, tile, zz, zz))
    while heap:
        now, tile, zz, kind = heapq.heappop(heap)
        out[zz].append((now, tile, ("S" if kind == zz else "G", tile, kind)))
        if kind in NEEDED:
            complete[zz][tile] = max(complete[zz][tile], now)
        for way in LINK_SENDS[zz].get(kind, ""):
            begin = max(now, free.get((zz, way), 0.0))
            free[zz, way] = begin + unit
            target, there = {"u": (zz + 1, kind), "d": (zz - 1, kind), "c": (3 - zz, 7 - kind)}[way]
            heapq.heappush(heap, (begin + unit + HOP_US, tile, target, there))
    limits = [max(complete[zz][tile] for zz in range(4)) for tile in range(tiles)]
    for zz in range(4):
        out[zz].append((0.0, tiles, ("Q", 0, 0)))
        out[zz].append((16.0 if zz == 1 else 0.0, tiles + 1, ("Y", 0, 0)))
        out[zz].append((30.0, tiles, ("WY", 0, 0)))
        out[zz].sort(key=lambda e: (e[0], e[1]))
    stages = []
    for tile in range(tiles):
        low = limits[tile - 1] if tile > 0 else -1.0
        high = limits[tile] if tile < tiles - 1 else float("inf")
        stages.append([[e for now, _, e in events if low < now <= high] for events in out])
    return stages


def paired_kernel(
    sizes,
    residual, gain_in, filter_w, signal_w, gate_w, out_w, taps_in,
    result, scales,
    acts, stream, normed, first_rows, first_w, weights, outs, own_part, pair_send, pair_recv, line_recv,
    part_send, part_recv, own_sum, product, edge_send, edge_recv, filter_rows, signal_rows,
    mixed, closing, squares, first_squares, row_scale, gain, taps, scale_rows,
    act_recv, line_send, cross_send, act_twin_recv, act_twin_send, first_recv, first_send,
    part_recv_sem, part_send_sem, weight_recv, weight_send,
    gather_recv, gather_send, twin_recv, twin_send, reduce_recv, reduce_send,
    pair_recv_sem, pair_send_sem, edge_recv_sem, edge_send_sem, square_recv, square_send, local_sem,
):
    S, T, L, R, F, C, DS, TAPS = sizes
    NZ, TB, RT, D = T // 2, T // S, R // TILES, T * F
    last = L - 1
    s, t = lax.axis_index("sp"), lax.axis_index("tp")
    z, core = t // 2, t % 2
    y, x = s // 2, s % 2
    zz = z + y * (NZ - 1 - 2 * z)
    local_kind = x + y * (1 - 2 * x)
    partner = (s, t + 1 - 2 * core)
    x_peer, y_peer = (s + 1 - 2 * x, t), (s + 2 - 4 * y, t)
    x_slot, y_slot = s + 1 - 2 * x, s + 2 - 4 * y
    diagonal = S - 1 - s
    own_w = (filter_w, signal_w, gate_w, out_w)

    barrier = pltpu.get_barrier_semaphore()
    for k in range(1, T):
        pl.semaphore_signal(barrier, inc=1, device_id=(s, (t + k) % T), device_id_type=MESH)
    for other in range(1, S):
        pl.semaphore_signal(barrier, inc=1, device_id=((s + other) % S, t), device_id_type=MESH)

    locals_ = []

    def local(src, dst):
        copy = pltpu.make_async_copy(src, dst, local_sem.at[len(locals_)])
        copy.start()
        locals_.append(copy)

    def remote(src, dst, send_sem, recv_sem, device):
        return pltpu.make_async_remote_copy(
            src_ref=src, dst_ref=dst, send_sem=send_sem, recv_sem=recv_sem,
            device_id=device, device_id_type=MESH,
        )

    local(residual, acts.at[zz, core])
    local(gain_in, gain)
    local(taps_in, taps)
    for k in range(3):
        local(own_w[k].at[0], first_w.at[k, pl.ds(local_kind * 2, 2)])
    for l in range(L):
        if l > 0:
            for k in range(3):
                local(own_w[k].at[l], weights.at[l - 1, k, pl.ds(s * TB, TB)])
        local(out_w.at[l], outs.at[l, s])
    pl.semaphore_wait(barrier, T - 1 + S - 1)

    def rows_of(tile):
        return pl.ds(tile * RT, RT)

    def tile_rows(tile):
        return pl.ds(pl.multiple_of(tile * RT, RT), RT)

    def drained(ref, sem, device):
        remote(ref, ref, sem, sem, device).wait_send()


    def first_copy(k):
        block = first_w.at[k, pl.ds(local_kind * 2, 2)]
        return remote(own_w[k].at[0], block, first_send.at[0], first_recv.at[k], x_peer)

    def first_arrival(k):
        block = first_w.at[k, pl.ds(2 - local_kind * 2, 2)]
        return remote(block, block, first_send.at[0], first_recv.at[k], x_peer)

    def act_copy(kind, tile, way):
        ref = acts.at[kind, core, rows_of(tile)]
        if way == "c":
            there = 7 - kind
            return remote(
                ref, acts.at[there, core, rows_of(tile)],
                cross_send.at[0], act_recv.at[there, tile], y_peer,
            )
        step = 2 - 4 * y if way == "u" else 4 * y - 2
        return remote(
            ref, ref, line_send.at["ud".index(way)], act_recv.at[kind, tile], (s, (t + step + T) % T)
        )

    def act_arrival(kind, tile):
        ref = acts.at[kind, core, rows_of(tile)]
        return remote(ref, ref, cross_send.at[0], act_recv.at[kind, tile], y_peer)

    def act_twin(kind, tile, receive=False):
        ref = acts.at[kind, 1 - core if receive else core, rows_of(tile)]
        return remote(ref, ref, act_twin_send.at[0], act_twin_recv.at[kind, tile], partner)

    def part_copy(m, tile, receive=False):
        return remote(
            part_send.at[m, rows_of(tile)], part_recv.at[m, rows_of(tile)],
            part_send_sem.at[0], part_recv_sem.at[m, tile], y_peer,
        )

    def first_square_copy(k):
        return remote(
            first_squares.at[t], first_squares.at[t],
            square_send.at[1], square_recv.at[TILES], (s, (t + k) % T),
        )

    def row_squares(ref, tile):
        acc = jnp.zeros((RT, 128), f32)
        for b in range(F // 128):
            value = ref[tile * RT:(tile + 1) * RT, b * 128:(b + 1) * 128].astype(f32)
            acc = acc + value * value
        return jnp.sum(acc.T, axis=0, keepdims=True)

    def first_event(zi, event):
        what, tile, kind = event
        if what in "SG":
            if what == "G":
                act_arrival(kind, tile).wait_recv()
            for way in LINK_SENDS[zi].get(kind, ""):
                act_copy(kind, tile, way).start()
            if kind in NEEDED:
                act_twin(kind, tile).start()
        elif what == "Q":
            for i in range(TILES):
                first_squares[t, :, i * RT:(i + 1) * RT] = row_squares(acts.at[zi, core], i)
            for k in range(1, T):
                first_square_copy(k).start()
        elif what == "Y":
            weight_copy(3, 1, 0).start()
        else:
            weight_arrival(3, 1, 0).wait_recv()
            weight_copy(3, 0, 1).start()

    def scale_tile(tile):
        step = min(RT, 32)

        def body(i, _):
            rows = pl.ds(pl.multiple_of(tile * RT + i * step, step), step)
            for kind in NEEDED:
                j, below = (kind, RT) if kind < 2 else (kind - 4, 0)
                block = j + y * (NZ - 1 - 2 * j)
                into = pl.ds(pl.multiple_of(below + i * step, step), step)
                for c in range(2):
                    columns = pl.ds(pl.multiple_of((2 * block + c) * F, F), F)
                    value = acts[kind, c, rows].astype(f32) * gain[0:1, columns]
                    begin = (2 * j + c) * F
                    first_rows[tile, into, begin:begin + F] = value.astype(bf16)
            return 0

        lax.fori_loop(0, RT // step, body, 0)

    def first_product(tile, m):
        value = jnp.dot(
            first_rows[tile], first_w[m].reshape(D // 2, C), preferred_element_type=f32
        )
        rows = tile_rows(tile)
        part_send[m, rows] = value[:RT].astype(bf16)
        part_copy(m, tile).start()
        own_sum[m, rows] = value[RT:]

    def first_weight(m):
        locals_[3 + m].wait()
        first_arrival(m).wait_recv()

    def loop(count, body):
        def step(i, _):
            body(i)
            return 0

        lax.fori_loop(0, count, step, 0)

    def joined(m, tile):
        part_copy(m, tile, True).wait_recv()
        rows = tile_rows(tile)
        scale = row_scale[rows, :]
        total = own_sum[m, rows] + part_recv[m, rows].astype(f32)
        return jnp.concatenate(
            [total[:, b * 128:(b + 1) * 128] * scale for b in range(C // 128)], axis=1
        ).astype(bf16)

    def first_scale():
        block = first_squares.at[pl.ds(0, T - 1)]
        remote(block, block, square_send.at[1], square_recv.at[TILES], partner).wait_recv()
        total = first_squares[0]
        for k in range(1, T):
            total = total + first_squares[k]
        scale = lax.rsqrt(total / D + NORM_FLOOR)
        for i in range(TILES):
            row_scale[i * RT:(i + 1) * RT, :] = jnp.broadcast_to(
                scale[:, i * RT:(i + 1) * RT], (128, RT)
            ).T


    def weight_ref(i, slot, half=None):
        l, k = divmod(i, 4)
        if k < 3:
            if half is None:
                return weights.at[l - 1, k, pl.ds(slot * TB, TB)]
            return weights.at[l - 1, k, pl.ds(slot * TB, TB), pl.ds(half * (F // 2), F // 2)]
        if half is None:
            return outs.at[l, slot]
        return outs.at[l, slot, pl.ds(half * (C // 2), C // 2)]

    def weight_copy(i, axis, hop):
        l, k = divmod(i, 4)
        if hop == 0:
            src, dst = own_w[k].at[l], weight_ref(i, s)
        else:
            src = dst = weight_ref(i, (y_slot, x_slot)[axis], axis)
        return remote(
            src, dst, weight_send.at[i - 3], weight_recv.at[i - 3, axis, hop], (x_peer, y_peer)[axis]
        )

    def weight_arrival(i, axis, hop):
        ref = weight_ref(i, (x_slot, y_slot)[axis]) if hop == 0 else weight_ref(i, diagonal, axis)
        return remote(
            ref, ref, weight_send.at[i - 3], weight_recv.at[i - 3, axis, hop], (x_peer, y_peer)[axis]
        )

    def weight_first(i):
        if i < 4 * L:
            for axis in range(2):
                weight_copy(i, axis, 0).start()

    def weight_forward(i):
        for axis in range(2):
            weight_arrival(i, 1 - axis, 0).wait_recv()
            weight_copy(i, axis, 1).start()
        for step in ((2,), (2,), (), (1, 2))[i % 4]:
            weight_first(i + step)

    def weight_ready(i):
        for axis in range(2):
            weight_arrival(i, axis, 1).wait_recv()

    def weight_drain(i):
        l, k = divmod(i, 4)
        ref = weights.at[l - 1, k, pl.ds(0, 3 * TB)] if k < 3 else outs.at[l, pl.ds(0, 3)]
        drained(ref, weight_send.at[i - 3], x_peer)

    def line_peer(direction):
        return (s, (t + (2 if direction == 0 else T - 2)) % T)

    def gather_copy(l, tile, src, direction):
        ref = stream.at[l - 1, 2 * src + core, rows_of(tile)]
        return remote(
            ref, ref, gather_send.at[l - 1, direction], gather_recv.at[l - 1, tile, src],
            line_peer(direction),
        )

    def twin_copy(l, tile, src, receive=False):
        ref = stream.at[l - 1, 2 * src + (1 - core if receive else core), rows_of(tile)]
        return remote(ref, ref, twin_send.at[l - 1], twin_recv.at[l - 1, tile, src], partner)

    def reduce_copy(l, tile, d, direction):
        return remote(
            own_part.at[l, d, rows_of(tile)], line_recv.at[l, direction, d, rows_of(tile)],
            reduce_send.at[l, direction], reduce_recv.at[l, tile, d + 1 - direction],
            line_peer(direction),
        )

    def pair_copy(l, tile, d):
        return remote(
            pair_send.at[l, d, rows_of(tile)], pair_recv.at[l, d, rows_of(tile)],
            pair_send_sem.at[l], pair_recv_sem.at[l, tile, d], partner,
        )

    def total_into(l, tile, d, incoming, base, store):
        step = min(RT, 32)

        def body(i, _):
            rows = pl.ds(pl.multiple_of(tile * RT + i * step, step), step)
            value = own_part[l, d, rows].astype(f32) + pair_recv[l, d, rows].astype(f32)
            for direction in incoming:
                value = value + line_recv[l, direction, d, rows].astype(f32)
            if base:
                before = acts[zz, core, rows] if l == 0 else stream[l - 1, t, rows]
                value = before.astype(f32) + value
            store(rows, value.astype(bf16))
            return 0

        lax.fori_loop(0, RT // step, body, 0)

    def square_copy(tile, k):
        return remote(
            squares.at[tile, t], squares.at[tile, t],
            square_send.at[0], square_recv.at[tile], (s, (t + k) % T),
        )

    def close(tile):
        squares[tile, t] = row_squares(closing, tile)
        for k in range(1, T):
            square_copy(tile, k).start()

    def run_event(zi, l, event, gather_layer):
        kind, tile, which = event
        if kind in "RL":
            direction = 0 if kind == "R" else 1
            pair_copy(l, tile, which).wait_recv()
            incoming = [direction] if (zi > 0 if direction == 0 else zi < NZ - 1) else []
            for d in incoming:
                reduce_copy(l, tile, which, d).wait_recv()

            def store(rows, value):
                own_part[l, which, rows] = value

            total_into(l, tile, which, incoming, False, store)
            reduce_copy(l, tile, which, direction).start()
        elif kind == "F":
            pair_copy(l, tile, zi).wait_recv()
            incoming = ([0] if zi > 0 else []) + ([1] if zi < NZ - 1 else [])
            for d in incoming:
                reduce_copy(l, tile, zi, d).wait_recv()

            def store(rows, value):
                if l < last:
                    stream[l, t, rows] = value
                else:
                    closing[rows] = value

            total_into(l, tile, zi, incoming, True, store)
            if l == last:
                close(tile)
            else:
                if zi + 1 < NZ:
                    gather_copy(gather_layer, tile, zi, 0).start()
                if zi > 0:
                    gather_copy(gather_layer, tile, zi, 1).start()
                twin_copy(gather_layer, tile, zi).start()
        else:
            direction = 0 if kind == "GR" else 1
            gather_copy(gather_layer, tile, which, direction).wait_recv()
            if (zi + 1 < NZ) if direction == 0 else (zi > 0):
                gather_copy(gather_layer, tile, which, direction).start()
            twin_copy(gather_layer, tile, which).start()

    def run_phase(l, gather_layer, weight_events):
        plan = line_plan(NZ, TILES, True, gather_layer is not None)
        for zi in range(NZ):
            events = [
                (now, n, e) for n, (now, e) in enumerate(plan[zi])
                if (e[0], zi) not in (("R", 0), ("L", NZ - 1))
            ]
            events += [(now, -1, ("W", i, 0)) for now, i in weight_events if i < 4 * L]
            if gather_layer is not None:
                for tile in range(TILES):
                    arrived = max(now for now, e in plan[zi] if e[1] == tile)
                    events.append((arrived + HOP_US, TILES * T * T, ("N", tile, 0)))
            events.sort(key=lambda e: (e[0], e[1]))

            @pl.when(z == zi)
            def _():
                for _, _, event in events:
                    if event[0] == "W":
                        weight_forward(event[1])
                    elif event[0] == "N":
                        normalize(gather_layer, event[1])
                    else:
                        run_event(zi, l, event, gather_layer)

    def normalize(l, tile):
        for src in range(NZ):
            twin_copy(l, tile, src, True).wait_recv()
        step = min(RT, 16)

        def body(i, _):
            rows = pl.ds(pl.multiple_of(tile * RT + i * step, step), step)
            acc = jnp.zeros((step, F), f32)
            for b in range(T):
                value = stream[l - 1, b, rows].astype(f32)
                acc = acc + value * value
            scale = lax.rsqrt(jnp.sum(acc, axis=1, keepdims=True) / D + NORM_FLOOR)
            for b in range(T):
                value = stream[l - 1, b, rows].astype(f32)
                columns = slice(b * F, (b + 1) * F)
                normed[rows, columns] = (value * scale * gain[l:l + 1, columns]).astype(bf16)
            return 0

        lax.fori_loop(0, RT // step, body, 0)

    def project(l, k, into):
        step = min(R, 256)

        def body(i, _):
            rows = pl.ds(pl.multiple_of(i * step, step), step)
            value = jnp.dot(
                normed[rows, :], weights[l - 1, k].reshape(D, C), preferred_element_type=f32
            )
            into[rows, :] = value.astype(bf16)
            return 0

        lax.fori_loop(0, R // step, body, 0)

    def edge_copy(l):
        return remote(
            edge_send.at[l], edge_recv.at[l], edge_send_sem.at[l], edge_recv_sem.at[l],
            ((s + 1) % S, t),
        )

    def mix(l):
        if l == 0:
            first_scale()
            for m, into in enumerate((filter_rows, signal_rows)):
                def join(tile):
                    into[tile_rows(tile)] = joined(m, tile)

                loop(TILES, join)
        else:
            weight_ready(4 * l)
            project(l, 0, filter_rows)
            weight_ready(4 * l + 1)
            project(l, 1, signal_rows)
        value = (filter_rows[...].astype(f32) * signal_rows[...].astype(f32)).astype(bf16)
        product[8:8 + R, :] = value.astype(f32)
        edge_send[l] = value[R - 16:, :]

        @pl.when(s < S - 1)
        def _():
            edge_copy(l).start()

        if l == 0:
            weight_arrival(3, 0, 0).wait_recv()
            weight_copy(3, 1, 1).start()
            weight_first(4)
            weight_first(5)
        else:
            weight_ready(4 * l + 2)

        @pl.when(s > 0)
        def _():
            edge_copy(l).wait_recv()
            product[0:8, :] = edge_recv[l].astype(f32)[8:, :]

        @pl.when(s == 0)
        def _():
            product[0:8, :] = jnp.zeros((8, C), f32)

    order = sorted(range(NZ), key=lambda d: (min(d, NZ - 1 - d), -d))

    def gates(l):
        step = RT if l == 0 else min(R, 256)

        def body(i):
            first = pl.multiple_of(i * step, step)
            rows = pl.ds(first, step)
            if l == 0:
                gate = joined(2, i)
            else:
                gate = jnp.dot(
                    normed[rows, :], weights[l - 1, 2].reshape(D, C), preferred_element_type=f32
                ).astype(bf16)
            window = product[pl.ds(first, step + 8), :]
            filtered = jnp.zeros((step, C), f32)
            for k in range(TAPS):
                begin = 8 - (TAPS - 1) + k
                filtered = filtered + taps[k, l:l + 1, :] * window[begin:begin + step]
            mixed[rows, :] = (gate.astype(f32) * filtered).astype(bf16)

        loop(R // step, body)

    def partials(l, tile):
        rows = tile_rows(tile)
        for own in (False, True):
            for d in order:
                block = 2 * d + (core if own else 1 - core)
                columns = pl.ds(pl.multiple_of((block % TB) * F, F), F)
                value = jnp.dot(
                    mixed[rows, :], outs[l, block // TB, :, columns], preferred_element_type=f32
                ).astype(bf16)
                if own:
                    own_part[l, d, rows] = value
                else:
                    pair_send[l, d, rows] = value
                    pair_copy(l, tile, d).start()

    def launch(l, tile, near=0, far=NZ):
        @pl.when(z == 0)
        def _():
            for d in range(NZ - 1, 0, -1):
                if near <= d < far:
                    run_event(0, l, ("R", tile, d), None)

        @pl.when(z == NZ - 1)
        def _():
            for d in range(NZ - 1):
                if near <= NZ - 1 - d < far:
                    run_event(NZ - 1, l, ("L", tile, d), None)

    def drain_first():
        drained(acts.at[pl.ds(0, 4), 0], act_twin_send.at[0], partner)
        drained(acts.at[0, 0], cross_send.at[0], y_peer)
        for zi in range(NZ):
            @pl.when(zz == zi)
            def _():
                for n, way in enumerate("ud"):
                    count = sum(way in ways for ways in LINK_SENDS[zi].values())
                    if count:
                        drained(acts.at[pl.ds(0, count), 0], line_send.at[n], partner)
        drained(part_send, part_send_sem.at[0], y_peer)
        block = first_squares.at[pl.ds(0, T - 1)]
        drained(block, square_send.at[1], partner)
        drained(first_w.at[pl.ds(0, 3), pl.ds(0, 2)], first_send.at[0], x_peer)

    def drain_gather(l):
        drained(stream.at[l - 1, pl.ds(0, NZ)], twin_send.at[l - 1], partner)
        for zi in range(NZ):
            @pl.when(z == zi)
            def _():
                for direction, count in enumerate((zi + 1 if zi < NZ - 1 else 0, NZ - zi if zi > 0 else 0)):
                    if count:
                        drained(
                            stream.at[l - 1, pl.ds(0, count)], gather_send.at[l - 1, direction], partner
                        )

    def drain_reduce(l):
        @pl.when(s < S - 1)
        def _():
            edge_copy(l).wait_send()

        drained(pair_send.at[l], pair_send_sem.at[l], partner)
        for zi in range(NZ):
            @pl.when(z == zi)
            def _():
                for direction, count in enumerate((NZ - 1 - zi, zi)):
                    if count:
                        drained(
                            own_part.at[l, pl.ds(0, count)], reduce_send.at[l, direction], partner
                        )

    for k in range(3):
        first_copy(k).start()
    weight_copy(3, 0, 0).start()
    for copy in locals_[:3]:
        copy.wait()
    stages = first_plan(TILES)
    for tile in range(TILES):
        for zi in range(NZ):
            @pl.when(zz == zi)
            def _():
                for event in stages[tile][zi]:
                    first_event(zi, event)
        for kind in NEEDED:
            act_twin(kind, tile, True).wait_recv()
        scale_tile(tile)
        if tile == 0:
            first_weight(0)
            first_weight(1)
        loop(2, lambda m: first_product(tile, m))
    first_weight(2)
    loop(TILES, lambda tile: first_product(tile, 2))
    for copy in locals_[6:]:
        copy.wait()
    for l in range(L):
        mix(l)
        if l > 0:
            if l == 1:
                drain_first()
                weight_drain(3)
            else:
                for i in range(4 * l - 4, 4 * l):
                    weight_drain(i)
            drain_gather(l)
            drain_reduce(l - 1)
        gates(l)
        weight_ready(4 * l + 3)
        nearest = 0 if l < last else NZ - 1

        def step(tile):
            partials(l, tile)

            @pl.when(tile > 0)
            def _():
                launch(l, tile - 1, nearest)

        loop(TILES, step)
        launch(l, TILES - 1, nearest)
        if l < last:
            run_phase(l, l + 1, ((12.0, 4 * l + 4), (24.0, 4 * l + 5), (40.0, 4 * l + 6), (57.0, 4 * l + 7)))
        else:
            for distance in range(NZ - 2, 0, -1):
                loop(TILES, lambda tile: launch(l, tile, distance, distance + 1))
            run_phase(l, None, ())

    drain_reduce(last)
    for i in range(4 * last, 4 * L):
        weight_drain(i)
    for tile in range(TILES):
        block = squares.at[tile, pl.ds(0, T - 1)]
        remote(block, block, square_send.at[0], square_recv.at[tile], partner).wait_recv()
        total = squares[tile, 0]
        for k in range(1, T):
            total = total + squares[tile, k]
        scale = lax.rsqrt(total / D + NORM_FLOOR)
        scale_rows[tile * RT:(tile + 1) * RT, :] = jnp.broadcast_to(scale, (128, RT)).T
    outgoing = [
        pltpu.make_async_copy(closing, result, local_sem.at[0]),
        pltpu.make_async_copy(scale_rows, scales, local_sem.at[1]),
    ]
    for copy in outgoing:
        copy.start()
    drained(squares.at[pl.ds(0, TILES), pl.ds(0, T - 1)], square_send.at[0], partner)
    for copy in outgoing:
        copy.wait()


def finish(pieces, closing, scale, gain, result, rows_in, scale_in, gain_in, rows_out, sems, gain_sem):
    R, F = rows_in.shape
    step = R // pieces
    gains = pltpu.make_async_copy(gain, gain_in, gain_sem)
    gains.start()

    def copies(i):
        rows = pl.ds(i * step, step)
        return (
            pltpu.make_async_copy(closing.at[rows], rows_in.at[rows], sems.at[i, 0]),
            pltpu.make_async_copy(scale.at[rows], scale_in.at[rows], sems.at[i, 1]),
            pltpu.make_async_copy(rows_out.at[rows], result.at[rows], sems.at[i, 2]),
        )

    for i in range(pieces):
        copies(i)[0].start()
        copies(i)[1].start()
    gains.wait()
    for i in range(pieces):
        copies(i)[0].wait()
        copies(i)[1].wait()
        rows = slice(i * step, (i + 1) * step)
        for b in range(F // 128):
            columns = slice(b * 128, (b + 1) * 128)
            rows_out[rows, columns] = (
                rows_in[rows, columns].astype(f32) * scale_in[rows, :] * gain_in[:, columns]
            )
        copies(i)[2].start()
    for i in range(pieces):
        copies(i)[2].wait()


def paired_call(S, T, L, R, F, C, DS, TAPS):
    NZ, TB = T // 2, T // S
    dma = pltpu.SemaphoreType.DMA
    any_space = pl.BlockSpec(memory_space=pl.ANY)
    return pl.pallas_call(
        functools.partial(paired_kernel, (S, T, L, R, F, C, DS, TAPS)),
        out_shape=(jax.ShapeDtypeStruct((R, F), bf16), jax.ShapeDtypeStruct((R, 128), f32)),
        in_specs=[any_space] * 7,
        out_specs=(any_space, any_space),
        scratch_shapes=[
            pltpu.VMEM((6, 2, R, F), bf16),
            pltpu.VMEM((L - 1, T, R, F), bf16),
            pltpu.VMEM((R, T * F), bf16),
            pltpu.VMEM((TILES, 2 * R // TILES, T // 2 * F), bf16),
            pltpu.VMEM((3, T // 2, F, C), bf16),
            pltpu.VMEM((L - 1, 3, T, F, C), bf16),
            pltpu.VMEM((L, S, C, DS), bf16),
            pltpu.VMEM((L, NZ, R, F), bf16),
            pltpu.VMEM((L, NZ, R, F), bf16),
            pltpu.VMEM((L, NZ, R, F), bf16),
            pltpu.VMEM((L, 2, NZ, R, F), bf16),
            pltpu.VMEM((3, R, C), bf16),
            pltpu.VMEM((3, R, C), bf16),
            pltpu.VMEM((3, R, C), f32),
            pltpu.VMEM((R + 8, C), f32),
            pltpu.VMEM((L, 16, C), bf16),
            pltpu.VMEM((L, 16, C), bf16),
            pltpu.VMEM((R, C), bf16),
            pltpu.VMEM((R, C), bf16),
            pltpu.VMEM((R, C), bf16),
            pltpu.VMEM((R, F), bf16),
            pltpu.VMEM((TILES, T, 1, R // TILES), f32),
            pltpu.VMEM((T, 1, R), f32),
            pltpu.VMEM((R, 128), f32),
            pltpu.VMEM((L, T * F), f32),
            pltpu.VMEM((TAPS, L, C), f32),
            pltpu.VMEM((R, 128), f32),
            dma((6, TILES)), dma((2,)), dma((1,)), dma((6, TILES)), dma((1,)), dma((3,)), dma((1,)),
            dma((3, TILES)), dma((1,)), dma((4 * L - 3, 2, 2)), dma((4 * L - 3,)),
            dma((L - 1, TILES, NZ)), dma((L - 1, 2)), dma((L - 1, TILES, NZ)), dma((L - 1,)),
            dma((L, TILES, NZ + 1)), dma((L, 2)),
            dma((L, TILES, NZ)), dma((L,)), dma((L,)), dma((L,)),
            dma((TILES + 1,)), dma((2,)), dma((4 * L + 6,)),
        ],
        compiler_params=pltpu.CompilerParams(
            collective_id=0, has_side_effects=True, vmem_limit_bytes=60 * 2**20
        ),
        name="mixers",
    )


def per_device(
    S, T, residual_in, norm_gain, gate_proj, filter_proj, signal_proj, conv_taps, out_proj, final_gain
):
    R, F = residual_in.shape
    L, DS, C = gate_proj.shape
    TAPS = conv_taps.shape[1]
    NZ, TB, H = T // 2, T // S, S // 2
    dma = pltpu.SemaphoreType.DMA
    cut = lambda w: w.reshape(L, TB, F, C)
    any_space = pl.BlockSpec(memory_space=pl.ANY)
    paired = S == 4 and NZ == 4 and L > 1
    if paired:
        closing, scale = paired_call(S, T, L, R, F, C, DS, TAPS)(
            residual_in, norm_gain, cut(filter_proj), cut(signal_proj),
            cut(gate_proj), out_proj, conv_taps.transpose(1, 0, 2),
        )
    else:
        closing, scale = pl.pallas_call(
            functools.partial(kernel, (S, T, L, R, F, C, DS, TAPS)),
            out_shape=(jax.ShapeDtypeStruct((R, F), bf16), jax.ShapeDtypeStruct((R, 128), f32)),
            in_specs=[any_space] * 7,
            out_specs=(any_space, any_space),
            scratch_shapes=[
                pltpu.VMEM((L, T, R, F), bf16),
                pltpu.VMEM((R, T * F), bf16),
                pltpu.VMEM((L, 3, T, F, C), bf16),
                pltpu.VMEM((L, S, C, DS), bf16),
                pltpu.VMEM((L, NZ, R, F), bf16),
                pltpu.VMEM((L, NZ, R, F), bf16),
                pltpu.VMEM((L, NZ, R, F), bf16),
                pltpu.VMEM((L, 2, NZ, R, F), bf16),
                pltpu.VMEM((R, C), bf16),
                pltpu.VMEM((R, C), bf16),
                pltpu.VMEM((R + 8, C), f32),
                pltpu.VMEM((L, 16, C), bf16),
                pltpu.VMEM((L, 16, C), bf16),
                pltpu.VMEM((R, C), bf16),
                pltpu.VMEM((R, F), bf16),
                pltpu.VMEM((TILES, T, 1, R // TILES), f32),
                pltpu.VMEM((L, T * F), f32),
                pltpu.VMEM((TAPS, L, C), f32),
                pltpu.VMEM((R, 128), f32),
                dma((4 * L, 2, H)), dma((4 * L, 2, H)),
                dma((L, TILES, 2, NZ)), dma((L, TILES, 2, NZ)),
                dma((L, TILES, NZ)), dma((L, TILES, NZ)),
                dma((L, TILES, 2, NZ)), dma((L, TILES, 2, NZ)),
                dma((L, TILES, NZ)), dma((L, TILES, NZ)),
                dma((L,)), dma((L,)),
                dma((TILES, T)), dma((TILES, T)),
                dma((4 * L + 3,)),
            ],
            compiler_params=pltpu.CompilerParams(
                collective_id=0, has_side_effects=True, vmem_limit_bytes=60 * 2**20
            ),
            name="mixers",
        )(
            residual_in, norm_gain, cut(filter_proj), cut(signal_proj),
            cut(gate_proj), out_proj, conv_taps.transpose(1, 0, 2),
        )
    return pl.pallas_call(
        functools.partial(finish, 4),
        out_shape=jax.ShapeDtypeStruct((R, F), f32),
        in_specs=[any_space] * 3,
        out_specs=any_space,
        scratch_shapes=[
            pltpu.VMEM((R, F), bf16), pltpu.VMEM((R, 128), f32), pltpu.VMEM((1, F), f32),
            pltpu.VMEM((R, F), f32), dma((4, 3)), dma,
        ],
        name="finish",
    )(closing, scale, final_gain.reshape(1, F))


def solution(mesh):
    return jax.shard_map(
        functools.partial(per_device, mesh.shape["sp"], mesh.shape["tp"]),
        mesh=mesh,
        in_specs=(
            P("sp", "tp"),
            P(),
            P(None, "sp", "tp"),
            P(None, "sp", "tp"),
            P(None, "sp", "tp"),
            P(None, None, "tp"),
            P(None, "tp", "sp"),
            P("tp"),
        ),
        out_specs=P("sp", "tp"),
        check_vma=False,
    )
```

```python
import functools
import heapq

import jax
import jax.numpy as jnp
from jax import lax
from jax.experimental import pallas as pl
from jax.experimental.pallas import tpu as pltpu
from jax.sharding import PartitionSpec as P

MESH = pl.DeviceIdType.MESH
NORM_FLOOR = 1e-06
TILES = 4
FINE = 8
CHUNK_US = 11.2
HOP_US = 2.0
f32 = jnp.float32
bf16 = jnp.bfloat16


def grid_width(count):
    height = max(h for h in range(1, count + 1) if count % h == 0 and h * h <= count)
    return count // height


def snake(index, width):
    y, x = index // width, index % width
    return y * width + x + (y % 2) * (width - 1 - 2 * x)


def line_plan(count, tiles, reduce, gather):
    unit = CHUNK_US / tiles
    heap, left, ready = [], {}, {}
    for z in range(count):
        for tile in range(tiles):
            if not reduce:
                heap.append((0.0, tile, 0, z, ("F", tile, z)))
                continue
            left[z, ("F", tile, z)] = (z > 0) + (z < count - 1)
            if left[z, ("F", tile, z)] == 0:
                heap.append((0.0, tile, 0, z, ("F", tile, z)))
            if z == 0:
                for d in range(1, count):
                    order = (tile, count - d) if gather else (count - d, tile)
                    heap.append((0.0, *order, z, ("R", tile, d)))
            if z == count - 1:
                for d in range(count - 1):
                    order = (tile, d) if gather else (d, tile)
                    heap.append((0.0, *order, z, ("L", tile, d)))
    heapq.heapify(heap)
    free = {}
    out = [[] for _ in range(count)]

    def send(now, z, step, event):
        begin = max(now, free.get((z, step), 0.0))
        free[z, step] = begin + unit
        key = (z + step, event)
        ready[key] = max(ready.get(key, 0.0), begin + unit + HOP_US)
        left[key] = left.get(key, 1) - 1
        if left[key] == 0:
            heapq.heappush(heap, (ready[key], event[1], 0, z + step, event))

    while heap:
        now, _, _, z, event = heapq.heappop(heap)
        kind, tile, which = event
        out[z].append((now, event))
        if kind in "RL":
            step = 1 if kind == "R" else -1
            send(now, z, step, ("F", tile, which) if which == z + step else event)
        elif kind == "F" and gather:
            if z + 1 < count:
                send(now, z, 1, ("GR", tile, z))
            if z > 0:
                send(now, z, -1, ("GL", tile, z))
        elif kind == "GR" and z + 1 < count:
            send(now, z, 1, event)
        elif kind == "GL" and z > 0:
            send(now, z, -1, event)
    return out


def kernel(
    sizes,
    residual, gain_in, filter_w, signal_w, gate_w, out_w, taps_in,
    result, scales,
    stream, normed, weights, outs, own_part, pair_send, pair_recv, line_recv,
    filter_rows, signal_rows, product, edge_send, edge_recv, mixed, closing, squares, gain, taps, scale_rows,
    weight_send, weight_recv, gather_send, gather_recv, twin_send, twin_recv,
    reduce_send, reduce_recv, pair_send_sem, pair_recv_sem,
    edge_send_sem, edge_recv_sem, square_send, square_recv, local_sem,
):
    S, T, L, R, F, C, DS, TAPS = sizes
    NZ, TB, RT, H, D = T // 2, T // S, R // TILES, S // 2, T * F
    width = grid_width(S)
    s, t = lax.axis_index("sp"), lax.axis_index("tp")
    z, core = t // 2, t % 2
    partner = (s, t + 1 - 2 * core)
    position = snake(s, width)

    def at_position(p):
        return snake((p + 2 * S) % S, width)

    ring = [(at_position(position + 1), t), (at_position(position - 1), t)]
    last = L - 1

    barrier = pltpu.get_barrier_semaphore()
    for k in range(1, T):
        pl.semaphore_signal(barrier, inc=1, device_id=(s, (t + k) % T), device_id_type=MESH)
    for other in range(1, S):
        pl.semaphore_signal(barrier, inc=1, device_id=((s + other) % S, t), device_id_type=MESH)

    locals_ = []

    def local(src, dst):
        copy = pltpu.make_async_copy(src, dst, local_sem.at[len(locals_)])
        copy.start()
        locals_.append(copy)

    local(residual, stream.at[0, t])
    local(gain_in, gain)
    local(taps_in, taps)
    for l in range(L):
        for k, w in enumerate((filter_w, signal_w, gate_w)):
            local(w.at[l], weights.at[l, k, pl.ds(s * TB, TB)])
        local(out_w.at[l], outs.at[l, s])
    pl.semaphore_wait(barrier, T - 1 + S - 1)

    def weight_ref(i, slot, half):
        l, k = divmod(i, 4)
        if k < 3:
            if half is None:
                return weights.at[l, k, pl.ds(slot * TB, TB)]
            return weights.at[l, k, pl.ds(slot * TB, TB), pl.ds(half * (F // 2), F // 2)]
        if half is None:
            return outs.at[l, slot]
        return outs.at[l, slot, pl.ds(half * (C // 2), C // 2)]

    def weight_source(i, half):
        l, k = divmod(i, 4)
        ref = (filter_w, signal_w, gate_w, out_w)[k]
        if half is None:
            return ref.at[l]
        if k < 3:
            return ref.at[l, pl.ds(0, TB), pl.ds(half * (F // 2), F // 2)]
        return ref.at[l, pl.ds(half * (C // 2), C // 2)]

    def weight_copy(i, direction, hop, receive=False):
        sign = 1 if direction == 0 else -1
        half = direction if hop == H else None
        slot = at_position(position - sign * (hop if receive else hop - 1))
        dst = weight_ref(i, slot, half)
        src = weight_source(i, half) if hop == 1 and not receive else dst
        return pltpu.make_async_remote_copy(
            src_ref=src, dst_ref=dst,
            send_sem=weight_send.at[i, direction, hop - 1],
            recv_sem=weight_recv.at[i, direction, hop - 1],
            device_id=ring[direction], device_id_type=MESH,
        )

    def weight_first(i):
        if i < 4 * L:
            for direction in range(2):
                weight_copy(i, direction, 1).start()

    def weight_forward(i):
        for hop in range(1, H):
            for direction in range(2):
                weight_copy(i, direction, hop, True).wait_recv()
                weight_copy(i, direction, hop + 1).start()
        for step in ((2,), (2,), (), (1, 2))[i % 4]:
            weight_first(i + step)

    def weight_ready(i):
        for direction in range(2):
            weight_copy(i, direction, H, True).wait_recv()

    def rows_of(tile):
        return pl.ds(tile * RT, RT)

    def gather_copy(l, tile, src, direction):
        ref = stream.at[l, 2 * src + core, rows_of(tile)]
        return pltpu.make_async_remote_copy(
            src_ref=ref, dst_ref=ref,
            send_sem=gather_send.at[l, tile, direction, src],
            recv_sem=gather_recv.at[l, tile, direction, src],
            device_id=(s, (t + (2 if direction == 0 else T - 2)) % T), device_id_type=MESH,
        )

    def twin_copy(l, tile, src, receive=False):
        block = 2 * src + (1 - core if receive else core)
        ref = stream.at[l, block, rows_of(tile)]
        return pltpu.make_async_remote_copy(
            src_ref=ref, dst_ref=ref,
            send_sem=twin_send.at[l, tile, src], recv_sem=twin_recv.at[l, tile, src],
            device_id=partner, device_id_type=MESH,
        )

    def reduce_copy(l, tile, d, direction):
        return pltpu.make_async_remote_copy(
            src_ref=own_part.at[l, d, rows_of(tile)],
            dst_ref=line_recv.at[l, direction, d, rows_of(tile)],
            send_sem=reduce_send.at[l, tile, direction, d],
            recv_sem=reduce_recv.at[l, tile, direction, d],
            device_id=(s, (t + (2 if direction == 0 else T - 2)) % T), device_id_type=MESH,
        )

    def pair_copy(l, tile, d):
        return pltpu.make_async_remote_copy(
            src_ref=pair_send.at[l, d, rows_of(tile)], dst_ref=pair_recv.at[l, d, rows_of(tile)],
            send_sem=pair_send_sem.at[l, tile, d], recv_sem=pair_recv_sem.at[l, tile, d],
            device_id=partner, device_id_type=MESH,
        )

    def total_into(l, tile, d, incoming, base, store):
        step = min(RT, 32)

        def body(i, _):
            rows = pl.ds(pl.multiple_of(tile * RT + i * step, step), step)
            value = own_part[l, d, rows].astype(f32) + pair_recv[l, d, rows].astype(f32)
            for direction in incoming:
                value = value + line_recv[l, direction, d, rows].astype(f32)
            if base:
                value = stream[l, t, rows].astype(f32) + value
            store(rows, value.astype(bf16))
            return 0

        lax.fori_loop(0, RT // step, body, 0)

    def square_copy(tile, k, receive=False):
        block = (t + T - k) % T if receive else t
        return pltpu.make_async_remote_copy(
            src_ref=squares.at[tile, block], dst_ref=squares.at[tile, block],
            send_sem=square_send.at[tile, k], recv_sem=square_recv.at[tile, k],
            device_id=(s, (t + k) % T), device_id_type=MESH,
        )

    def close(tile):
        acc = jnp.zeros((RT, 128), f32)
        for b in range(F // 128):
            value = closing[tile * RT:(tile + 1) * RT, b * 128:(b + 1) * 128].astype(f32)
            acc = acc + value * value
        squares[tile, t] = jnp.sum(acc.T, axis=0, keepdims=True)
        for k in range(1, T):
            square_copy(tile, k).start()

    def run_event(zi, l, event, gather_layer):
        kind, tile, which = event
        if kind in "RL":
            direction = 0 if kind == "R" else 1
            pair_copy(l, tile, which).wait_recv()
            incoming = [direction] if (zi > 0 if direction == 0 else zi < NZ - 1) else []
            for d in incoming:
                reduce_copy(l, tile, which, d).wait_recv()

            def store(rows, value):
                own_part[l, which, rows] = value

            total_into(l, tile, which, incoming, False, store)
            reduce_copy(l, tile, which, direction).start()
        elif kind == "F":
            if l is not None:
                pair_copy(l, tile, zi).wait_recv()
                incoming = ([0] if zi > 0 else []) + ([1] if zi < NZ - 1 else [])
                for d in incoming:
                    reduce_copy(l, tile, zi, d).wait_recv()

                def store(rows, value):
                    if l < last:
                        stream[l + 1, t, rows] = value
                    else:
                        closing[rows] = value

                total_into(l, tile, zi, incoming, True, store)
                if l == last:
                    close(tile)
            if gather_layer is not None:
                if zi + 1 < NZ:
                    gather_copy(gather_layer, tile, zi, 0).start()
                if zi > 0:
                    gather_copy(gather_layer, tile, zi, 1).start()
                twin_copy(gather_layer, tile, zi).start()
        else:
            direction = 0 if kind == "GR" else 1
            gather_copy(gather_layer, tile, which, direction).wait_recv()
            if (zi + 1 < NZ) if direction == 0 else (zi > 0):
                gather_copy(gather_layer, tile, which, direction).start()
            twin_copy(gather_layer, tile, which).start()

    def run_phase(l, gather_layer, weight_events):
        plan = line_plan(NZ, TILES, l is not None, gather_layer is not None)
        for zi in range(NZ):
            events = [
                (now, n, e) for n, (now, e) in enumerate(plan[zi])
                if (e[0], zi) not in (("R", 0), ("L", NZ - 1))
            ]
            events += [(now, -1, ("W", i, 0)) for now, i in weight_events if i < 4 * L]
            if gather_layer is not None:
                for tile in range(TILES):
                    arrived = max(now for now, e in plan[zi] if e[1] == tile)
                    events.append((arrived + HOP_US, TILES * T * T, ("N", tile, 0)))
            events.sort(key=lambda e: (e[0], e[1]))

            @pl.when(z == zi)
            def _():
                for _, _, event in events:
                    if event[0] == "W":
                        weight_forward(event[1])
                    elif event[0] == "N":
                        normalize(gather_layer, event[1])
                    else:
                        run_event(zi, l, event, gather_layer)

    def normalize(l, tile):
        for src in range(NZ):
            twin_copy(l, tile, src, True).wait_recv()
        step = min(RT, 16)

        def body(i, _):
            rows = pl.ds(pl.multiple_of(tile * RT + i * step, step), step)
            acc = jnp.zeros((step, F), f32)
            for b in range(T):
                value = stream[l, b, rows].astype(f32)
                acc = acc + value * value
            scale = lax.rsqrt(jnp.sum(acc, axis=1, keepdims=True) / D + NORM_FLOOR)
            for b in range(T):
                value = stream[l, b, rows].astype(f32)
                normed[rows, b * F:(b + 1) * F] = (value * scale * gain[l:l + 1, b * F:(b + 1) * F]).astype(bf16)
            return 0

        lax.fori_loop(0, RT // step, body, 0)

    def project(l, k, into):
        step = min(R, 256)

        def body(i, _):
            rows = pl.ds(pl.multiple_of(i * step, step), step)
            value = jnp.dot(
                normed[rows, :], weights[l, k].reshape(D, C), preferred_element_type=f32
            )
            into[rows, :] = value.astype(bf16)
            return 0

        lax.fori_loop(0, R // step, body, 0)

    def edge_copy(l):
        return pltpu.make_async_remote_copy(
            src_ref=edge_send.at[l], dst_ref=edge_recv.at[l],
            send_sem=edge_send_sem.at[l], recv_sem=edge_recv_sem.at[l],
            device_id=((s + 1) % S, t), device_id_type=MESH,
        )

    def mix(l):
        weight_ready(4 * l)
        project(l, 0, filter_rows)
        weight_ready(4 * l + 1)
        project(l, 1, signal_rows)
        value = (filter_rows[...].astype(f32) * signal_rows[...].astype(f32)).astype(bf16)
        product[8:8 + R, :] = value.astype(f32)
        edge_send[l] = value[R - 16:, :]

        @pl.when(s < S - 1)
        def _():
            edge_copy(l).start()

        if l == 0:
            weight_forward(4 * l + 3)
        weight_ready(4 * l + 2)

        @pl.when(s > 0)
        def _():
            edge_copy(l).wait_recv()
            product[0:8, :] = edge_recv[l].astype(f32)[8:, :]

        @pl.when(s == 0)
        def _():
            product[0:8, :] = jnp.zeros((8, C), f32)

    order = sorted(range(NZ), key=lambda d: (min(d, NZ - 1 - d), -d))

    def partials(l, tile):
        first, rows = tile * RT, slice(tile * RT, (tile + 1) * RT)
        gate = jnp.dot(
            normed[rows, :], weights[l, 2].reshape(D, C), preferred_element_type=f32
        ).astype(bf16)
        filtered = jnp.zeros((RT, C), f32)
        for k in range(TAPS):
            begin = 8 - (TAPS - 1) + k + first
            filtered = filtered + taps[k, l:l + 1, :] * product[begin:begin + RT, :]
        mixed[rows, :] = (gate.astype(f32) * filtered).astype(bf16)
        if tile == 0:
            weight_ready(4 * l + 3)
        for own in (False, True):
            for d in order:
                block = 2 * d + (core if own else 1 - core)
                columns = pl.ds(pl.multiple_of((block % TB) * F, F), F)
                value = jnp.dot(
                    mixed[rows, :], outs[l, block // TB, :, columns], preferred_element_type=f32
                ).astype(bf16)
                if own:
                    own_part[l, d, rows] = value
                else:
                    pair_send[l, d, rows] = value
                    pair_copy(l, tile, d).start()

    def launch(l, tile, near=0, far=NZ):
        @pl.when(z == 0)
        def _():
            for d in range(NZ - 1, 0, -1):
                if near <= d < far:
                    run_event(0, l, ("R", tile, d), None)

        @pl.when(z == NZ - 1)
        def _():
            for d in range(NZ - 1):
                if near <= NZ - 1 - d < far:
                    run_event(NZ - 1, l, ("L", tile, d), None)

    def drain_gather(l):
        for tile in range(TILES):
            for d in range(NZ):
                twin_copy(l, tile, d).wait_send()

                @pl.when((z < NZ - 1) & (d <= z))
                def _():
                    gather_copy(l, tile, d, 0).wait_send()

                @pl.when((z > 0) & (d >= z))
                def _():
                    gather_copy(l, tile, d, 1).wait_send()

    def drain_reduce(l):
        @pl.when(s < S - 1)
        def _():
            edge_copy(l).wait_send()

        for tile in range(TILES):
            for d in range(NZ):
                pair_copy(l, tile, d).wait_send()

                @pl.when((z < NZ - 1) & (d > z))
                def _():
                    reduce_copy(l, tile, d, 0).wait_send()

                @pl.when((z > 0) & (d < z))
                def _():
                    reduce_copy(l, tile, d, 1).wait_send()

    def drain_weights(first, end):
        for i in range(first, end):
            for direction in range(2):
                for hop in range(1, H + 1):
                    weight_copy(i, direction, hop).wait_send()

    weight_first(0)
    weight_first(1)
    for copy in locals_[:3]:
        copy.wait()
    run_phase(None, 0, ((13.0, 0), (24.0, 1)))
    for copy in locals_[3:]:
        copy.wait()
    weight_forward(2)
    for l in range(L):
        mix(l)
        if l == 1:
            drain_gather(0)
        if l > 0:
            drain_gather(l)
            drain_reduce(l - 1)
            drain_weights(4 * l - 4, 4 * l)
        for tile in range(TILES):
            partials(l, tile)
            if tile > 0:
                launch(l, tile - 1, 0 if l < last else NZ - 1)
        launch(l, TILES - 1, 0 if l < last else NZ - 1)
        if l < last:
            run_phase(l, l + 1, ((8.0, 4 * l + 4), (20.0, 4 * l + 5), (36.0, 4 * l + 6), (52.0, 4 * l + 7)))
        else:
            for distance in range(NZ - 2, 0, -1):
                for tile in range(TILES):
                    launch(l, tile, distance, distance + 1)
            run_phase(l, None, ())

    drain_reduce(last)
    drain_weights(4 * last, 4 * L)
    for tile in range(TILES):
        for k in range(1, T):
            square_copy(tile, k, True).wait_recv()
        total = squares[tile, 0]
        for k in range(1, T):
            total = total + squares[tile, k]
        scale = lax.rsqrt(total / D + NORM_FLOOR)
        scale_rows[tile * RT:(tile + 1) * RT, :] = jnp.broadcast_to(scale, (128, RT)).T
    outgoing = [
        pltpu.make_async_copy(closing, result, local_sem.at[0]),
        pltpu.make_async_copy(scale_rows, scales, local_sem.at[1]),
    ]
    for copy in outgoing:
        copy.start()
    for copy in outgoing:
        copy.wait()

    for tile in range(TILES):
        for k in range(1, T):
            square_copy(tile, k).wait_send()


LINK_SENDS = (
    {0: "u", 4: "u", 2: "c"},
    {1: "ud", 0: "u", 4: "u", 2: "dc", 5: "d"},
    {2: "cd", 1: "u", 0: "u", 4: "u"},
    {3: "c"},
)
NEEDED = (0, 1, 4, 5)


def first_plan(tiles):
    unit = CHUNK_US / tiles
    heap, free = [], {}
    out = [[] for _ in range(4)]
    complete = [{tile: 0.0 for tile in range(tiles)} for _ in range(4)]
    for zz in range(4):
        for tile in range(tiles):
            heapq.heappush(heap, (0.0, tile, zz, zz))
    while heap:
        now, tile, zz, kind = heapq.heappop(heap)
        out[zz].append((now, tile, ("S" if kind == zz else "G", tile, kind)))
        if kind in NEEDED:
            complete[zz][tile] = max(complete[zz][tile], now)
        for way in LINK_SENDS[zz].get(kind, ""):
            begin = max(now, free.get((zz, way), 0.0))
            free[zz, way] = begin + unit
            target, there = {"u": (zz + 1, kind), "d": (zz - 1, kind), "c": (3 - zz, 7 - kind)}[way]
            heapq.heappush(heap, (begin + unit + HOP_US, tile, target, there))
    limits = [max(complete[zz][tile] for zz in range(4)) for tile in range(tiles)]
    for zz in range(4):
        out[zz].append((0.0, tiles, ("Q", 0, 0)))
        out[zz].append((16.0 if zz == 1 else 0.0, tiles + 1, ("Y", 0, 0)))
        out[zz].append((CHUNK_US + 7.0, tiles, ("WX", 0, 0)))
        out[zz].append((2 * CHUNK_US + 7.0, tiles, ("WY", 0, 0)))
        out[zz].sort(key=lambda e: (e[0], e[1]))
    stages = []
    for tile in range(tiles):
        low = limits[tile - 1] if tile > 0 else -1.0
        high = limits[tile] if tile < tiles - 1 else float("inf")
        stages.append([[e for now, _, e in events if low < now <= high] for events in out])
    return stages


def paired_kernel(
    sizes,
    residual, gain_in, filter_w, signal_w, gate_w, out_w, taps_in,
    result, scales,
    acts, stream, normed, first_rows, first_w, weights, outs, own_part, pair_send, pair_recv, line_recv,
    part_send, part_recv, own_sum, product, edge_send, edge_recv, inner_rows,
    mixed, closing, squares, first_squares, row_scale, gain, taps, scale_rows,
    act_recv, line_send, cross_send, act_twin_recv, act_twin_send, first_recv, first_send,
    part_recv_sem, part_send_sem, weight_recv, weight_send, piece_recv,
    gather_recv, gather_send, twin_recv, twin_send, reduce_recv, reduce_send,
    pair_recv_sem, pair_send_sem, edge_recv_sem, edge_send_sem, square_recv, square_send, local_sem,
):
    S, T, L, R, F, C, DS, TAPS = sizes
    NZ, TB, RT, D = T // 2, T // S, R // TILES, T * F
    last = L - 1
    s, t = lax.axis_index("sp"), lax.axis_index("tp")
    z, core = t // 2, t % 2
    y, x = s // 2, s % 2
    zz = z + y * (NZ - 1 - 2 * z)
    local_kind = x + y * (1 - 2 * x)
    partner = (s, t + 1 - 2 * core)
    x_peer, y_peer = (s + 1 - 2 * x, t), (s + 2 - 4 * y, t)
    x_slot, y_slot = s + 1 - 2 * x, s + 2 - 4 * y
    diagonal = S - 1 - s
    own_w = (filter_w, signal_w, gate_w, out_w)

    barrier = pltpu.get_barrier_semaphore()
    for k in range(1, T):
        pl.semaphore_signal(barrier, inc=1, device_id=(s, (t + k) % T), device_id_type=MESH)
    for other in range(1, S):
        pl.semaphore_signal(barrier, inc=1, device_id=((s + other) % S, t), device_id_type=MESH)

    locals_ = []

    def local(src, dst):
        copy = pltpu.make_async_copy(src, dst, local_sem.at[len(locals_)])
        copy.start()
        locals_.append(copy)

    def remote(src, dst, send_sem, recv_sem, device):
        return pltpu.make_async_remote_copy(
            src_ref=src, dst_ref=dst, send_sem=send_sem, recv_sem=recv_sem,
            device_id=device, device_id_type=MESH,
        )

    local(residual, acts.at[zz, core])
    local(gain_in, gain)
    local(taps_in, taps)
    for k in range(3):
        local(own_w[k].at[0], first_w.at[k, pl.ds(local_kind * 2, 2)])
    for l in range(L):
        if l > 0:
            for k in range(3):
                local(own_w[k].at[l], weights.at[l - 1, k, pl.ds(s * TB, TB)])
        local(out_w.at[l], outs.at[l, s])
    pl.semaphore_wait(barrier, T - 1 + S - 1)

    share = FINE // TILES

    def first_of(tile, size):
        return R - size - tile * size

    def rows_of(tile):
        return pl.ds(first_of(tile, RT), RT)

    def layer_rows(l, tile):
        size = R // FINE
        return pl.ds(pl.multiple_of(first_of(tile, size), size), size)

    def tile_rows(tile):
        return pl.ds(pl.multiple_of(first_of(tile, RT), RT), RT)

    def drained(ref, sem, device):
        remote(ref, ref, sem, sem, device).wait_send()


    def first_copy(k):
        block = first_w.at[k, pl.ds(local_kind * 2, 2)]
        return remote(own_w[k].at[0], block, first_send.at[0], first_recv.at[k], x_peer)

    def first_arrival(k):
        block = first_w.at[k, pl.ds(2 - local_kind * 2, 2)]
        return remote(block, block, first_send.at[0], first_recv.at[k], x_peer)

    def act_copy(kind, tile, way):
        ref = acts.at[kind, core, rows_of(tile)]
        if way == "c":
            there = 7 - kind
            return remote(
                ref, acts.at[there, core, rows_of(tile)],
                cross_send.at[0], act_recv.at[there, tile], y_peer,
            )
        step = 2 - 4 * y if way == "u" else 4 * y - 2
        return remote(
            ref, ref, line_send.at["ud".index(way)], act_recv.at[kind, tile], (s, (t + step + T) % T)
        )

    def act_arrival(kind, tile):
        ref = acts.at[kind, core, rows_of(tile)]
        return remote(ref, ref, cross_send.at[0], act_recv.at[kind, tile], y_peer)

    def act_twin(kind, tile):
        ref = acts.at[kind, core, rows_of(tile)]
        return remote(ref, ref, act_twin_send.at[0], act_twin_recv.at[tile], partner)

    def part_copy(m, tile, receive=False):
        return remote(
            part_send.at[m, rows_of(tile)], part_recv.at[m, rows_of(tile)],
            part_send_sem.at[0], part_recv_sem.at[m, tile], y_peer,
        )

    def first_square_copy(k):
        return remote(
            first_squares.at[t], first_squares.at[t],
            square_send.at[1], square_recv.at[TILES], (s, (t + k) % T),
        )

    def row_squares(ref, tile):
        acc = jnp.zeros((RT, 128), f32)
        for b in range(F // 128):
            value = ref[rows_of(tile), b * 128:(b + 1) * 128].astype(f32)
            acc = acc + value * value
        return jnp.sum(acc.T, axis=0, keepdims=True)

    def first_event(zi, event):
        what, tile, kind = event
        if what in "SG":
            if what == "G":
                act_arrival(kind, tile).wait_recv()
            for way in LINK_SENDS[zi].get(kind, ""):
                act_copy(kind, tile, way).start()
            if kind in NEEDED:
                act_twin(kind, tile).start()
        elif what == "Q":
            for i in range(TILES):
                first_squares[t, :, i * RT:(i + 1) * RT] = row_squares(acts.at[zi, core], i)
            for k in range(1, T):
                first_square_copy(k).start()
        elif what == "Y":
            weight_copy(3, 1, 0).start()
        else:
            axis = "XY".index(what[1])
            weight_arrival(3, axis, 0).wait_recv()
            weight_copy(3, 1 - axis, 1).start()

    def scale_tile(tile):
        step = min(RT, 32)

        def body(i, _):
            rows = pl.ds(pl.multiple_of(first_of(tile, RT) + i * step, step), step)
            for kind in NEEDED:
                j, below = (kind, RT) if kind < 2 else (kind - 4, 0)
                block = j + y * (NZ - 1 - 2 * j)
                into = pl.ds(pl.multiple_of(below + i * step, step), step)
                for c in range(2):
                    columns = pl.ds(pl.multiple_of((2 * block + c) * F, F), F)
                    value = acts[kind, c, rows].astype(f32) * gain[0:1, columns]
                    begin = (2 * j + c) * F
                    first_rows[tile, into, begin:begin + F] = value.astype(bf16)
            return 0

        lax.fori_loop(0, RT // step, body, 0)

    def first_product(tile, m):
        value = jnp.dot(
            first_rows[tile], first_w[m].reshape(D // 2, C), preferred_element_type=f32
        )
        rows = tile_rows(tile)
        part_send[m, rows] = value[:RT].astype(bf16)
        part_copy(m, tile).start()
        own_sum[m, rows] = value[RT:]

    def first_weight(m):
        locals_[3 + m].wait()
        first_arrival(m).wait_recv()

    def loop(count, body):
        def step(i, _):
            body(i)
            return 0

        lax.fori_loop(0, count, step, 0)

    def joined(m, rows):
        scale = row_scale[rows, :]
        total = own_sum[m, rows] + part_recv[m, rows].astype(f32)
        return jnp.concatenate(
            [total[:, b * 128:(b + 1) * 128] * scale for b in range(C // 128)], axis=1
        ).astype(bf16)

    def first_scale():
        block = first_squares.at[pl.ds(0, T - 1)]
        remote(block, block, square_send.at[1], square_recv.at[TILES], partner).wait_recv()
        total = first_squares[0]
        for k in range(1, T):
            total = total + first_squares[k]
        scale = lax.rsqrt(total / D + NORM_FLOOR)
        for i in range(TILES):
            row_scale[rows_of(i), :] = jnp.broadcast_to(
                scale[:, i * RT:(i + 1) * RT], (128, RT)
            ).T


    def weight_ref(i, slot, half=None):
        l, k = divmod(i, 4)
        if k < 3:
            if half is None:
                return weights.at[l - 1, k, pl.ds(slot * TB, TB)]
            cut = F * 9 // 16
            return weights.at[l - 1, k, pl.ds(slot * TB, TB), pl.ds(cut * half, F - cut if half else cut)]
        if half is None:
            return outs.at[l, slot]
        cut = C // 4 if l == 0 else C // 2
        return outs.at[l, slot, pl.ds(cut * half, C - cut if half else cut)]

    def weight_copy(i, axis, hop):
        l, k = divmod(i, 4)
        if hop == 0:
            src, dst = own_w[k].at[l], weight_ref(i, s)
        else:
            src = dst = weight_ref(i, (y_slot, x_slot)[axis], axis)
        return remote(
            src, dst, weight_send.at[i - 3], weight_recv.at[i - 3, axis, hop], (x_peer, y_peer)[axis]
        )

    def piece_copy(axis, piece, receive=False):
        rows = pl.ds(piece * (C // 2), C // 2)
        dst = outs.at[last, (x_slot, y_slot)[axis] if receive else s, rows]
        return remote(
            dst if receive else out_w.at[last, rows], dst, weight_send.at[4 * last],
            weight_recv.at[4 * last, axis, 0] if piece else piece_recv.at[axis], (x_peer, y_peer)[axis],
        )

    def weight_arrival(i, axis, hop):
        ref = weight_ref(i, (x_slot, y_slot)[axis]) if hop == 0 else weight_ref(i, diagonal, axis)
        return remote(
            ref, ref, weight_send.at[i - 3], weight_recv.at[i - 3, axis, hop], (x_peer, y_peer)[axis]
        )

    def weight_first(i):
        if i < 4 * L:
            for axis in range(2):
                weight_copy(i, axis, 0).start()

    def weight_forward(i):
        for axis in range(2):
            weight_arrival(i, 1 - axis, 0).wait_recv()
            weight_copy(i, axis, 1).start()
        if i == 4 * last + 2:
            for axis in range(2):
                piece_copy(axis, 0).start()
        elif i != 4 * last + 1:
            for step in ((2,), (2,), (), (1, 2))[i % 4]:
                weight_first(i + step)

    def weight_ready(i):
        for axis in range(2):
            weight_arrival(i, axis, 1).wait_recv()

    def weight_drain(i):
        l, k = divmod(i, 4)
        ref = weights.at[l - 1, k, pl.ds(0, 3 * TB)] if k < 3 else outs.at[l, pl.ds(0, 3)]
        drained(ref, weight_send.at[i - 3], x_peer)

    def line_peer(direction):
        return (s, (t + (2 if direction == 0 else T - 2)) % T)

    def gather_copy(l, tile, src, direction):
        ref = stream.at[l - 1, 2 * src + core, layer_rows(l - 1, tile)]
        return remote(
            ref, ref, gather_send.at[l - 1, direction], gather_recv.at[l - 1, tile, src],
            line_peer(direction),
        )

    def twin_copy(l, tile, src):
        ref = stream.at[l - 1, 2 * src + core, layer_rows(l - 1, tile)]
        group = tile // share
        return remote(ref, ref, twin_send.at[l - 1], twin_recv.at[l - 1, group], partner)

    def reduce_copy(l, tile, d, direction):
        return remote(
            own_part.at[l, d, layer_rows(l, tile)], line_recv.at[l, direction, d, layer_rows(l, tile)],
            reduce_send.at[l, direction], reduce_recv.at[tile, d + 1 - direction],
            line_peer(direction),
        )

    def pair_copy(l, tile, d):
        return remote(
            pair_send.at[l, d, tile_rows(tile)], pair_recv.at[l, d, tile_rows(tile)],
            pair_send_sem.at[l], pair_recv_sem.at[tile, d], partner,
        )

    def total_into(l, tile, d, incoming, base, store):
        size = R // FINE
        step = min(size, 32)

        def body(i, _):
            rows = pl.ds(pl.multiple_of(first_of(tile, size) + i * step, step), step)
            value = own_part[l, d, rows].astype(f32) + pair_recv[l, d, rows].astype(f32)
            for direction in incoming:
                value = value + line_recv[l, direction, d, rows].astype(f32)
            if base:
                before = acts[zz, core, rows] if l == 0 else stream[l - 1, t, rows]
                value = before.astype(f32) + value
            store(rows, value.astype(bf16))
            return 0

        lax.fori_loop(0, size // step, body, 0)

    def square_copy(tile, k):
        return remote(
            squares.at[tile, t], squares.at[tile, t],
            square_send.at[0], square_recv.at[tile], (s, (t + k) % T),
        )

    def close(tile):
        squares[tile, t] = row_squares(closing, tile)
        for k in range(1, T):
            square_copy(tile, k).start()
        closing_copy(tile).start()

    def closing_copy(tile):
        return pltpu.make_async_copy(
            closing.at[rows_of(tile)], result.at[rows_of(tile)], local_sem.at[1 + tile]
        )

    def pair_arrival(l, tile, d, i):
        if i is None:
            i = tile % share
        if i == 0:
            pair_copy(l, tile // share, d).wait_recv()

    def run_event(zi, l, event, gather_layer, i=None):
        kind, tile, which = event
        if kind in "RL":
            direction = 0 if kind == "R" else 1
            pair_arrival(l, tile, which, i)
            incoming = [direction] if (zi > 0 if direction == 0 else zi < NZ - 1) else []
            for d in incoming:
                reduce_copy(l, tile, which, d).wait_recv()

            def store(rows, value):
                own_part[l, which, rows] = value

            total_into(l, tile, which, incoming, False, store)
            reduce_copy(l, tile, which, direction).start()
        elif kind == "F":
            pair_arrival(l, tile, zi, i)
            incoming = ([0] if zi > 0 else []) + ([1] if zi < NZ - 1 else [])
            for d in incoming:
                reduce_copy(l, tile, zi, d).wait_recv()

            def store(rows, value):
                if l < last:
                    stream[l, t, rows] = value
                else:
                    closing[rows] = value

            total_into(l, tile, zi, incoming, True, store)
            if l == last:
                if tile % share == share - 1:
                    close(tile // share)
            else:
                if zi + 1 < NZ:
                    gather_copy(gather_layer, tile, zi, 0).start()
                if zi > 0:
                    gather_copy(gather_layer, tile, zi, 1).start()
                twin_copy(gather_layer, tile, zi).start()
        else:
            direction = 0 if kind == "GR" else 1
            gather_copy(gather_layer, tile, which, direction).wait_recv()
            if (zi + 1 < NZ) if direction == 0 else (zi > 0):
                gather_copy(gather_layer, tile, which, direction).start()
            twin_copy(gather_layer, tile, which).start()

    def run_phase(l, gather_layer, weight_events):
        tiles = FINE
        plan = line_plan(NZ, tiles, True, gather_layer is not None)
        groups = TILES if gather_layer is not None else 1
        ends = [
            max(now for z_events in plan for now, e in z_events if e[1] * groups // tiles <= g)
            for g in range(groups)
        ]
        for g in range(groups):
            low = ends[g - 1] if g > 0 else -1.0
            high = ends[g] if g < groups - 1 else float("inf")
            for zi in range(NZ):
                events = [
                    (now, n, e) for n, (now, e) in enumerate(plan[zi])
                    if (e[0], zi) not in (("R", 0), ("L", NZ - 1))
                ]
                events += [(now, -1, ("W", i, 0)) for now, i in weight_events if i < 4 * L]
                events = sorted((e for e in events if low < e[0] <= high), key=lambda e: (e[0], e[1]))

                @pl.when(z == zi)
                def _():
                    for _, _, event in events:
                        if event[0] == "W":
                            weight_forward(event[1])
                        else:
                            run_event(zi, l, event, gather_layer)

            if gather_layer is not None:
                normalize(gather_layer, g)
                if g == 0:
                    weight_ready(4 * gather_layer)
                    weight_ready(4 * gather_layer + 1)
                    loop(2, lambda k: project(gather_layer, k, R - RT, RT))
                    send_edge(gather_layer)
                    if gather_layer == last:
                        for axis in range(2):
                            piece_copy(axis, 1).start()
                elif g == groups - 1:
                    loop(2, lambda k: project(gather_layer, k, 0, R - RT))

    def normalize(l, tile):
        block = stream.at[l - 1, pl.ds(0, NZ), rows_of(tile)]
        remote(block, block, twin_send.at[l - 1], twin_recv.at[l - 1, tile], partner).wait_recv()
        step = min(RT, 16)

        def body(i, _):
            rows = pl.ds(pl.multiple_of(first_of(tile, RT) + i * step, step), step)
            acc = jnp.zeros((step, F), f32)
            for b in range(T):
                value = stream[l - 1, b, rows].astype(f32)
                acc = acc + value * value
            scale = lax.rsqrt(jnp.sum(acc, axis=1, keepdims=True) / D + NORM_FLOOR)
            for b in range(T):
                value = stream[l - 1, b, rows].astype(f32)
                columns = slice(b * F, (b + 1) * F)
                normed[rows, columns] = (value * scale * gain[l:l + 1, columns]).astype(bf16)
            return 0

        lax.fori_loop(0, RT // step, body, 0)

    def project(l, k, first, size):
        rows = pl.ds(first, size)
        value = jnp.dot(
            normed[rows, :], weights[l - 1, k].reshape(D, C), preferred_element_type=f32
        )
        inner_rows[k, rows] = value.astype(bf16)

    def edge_copy(l):
        return remote(
            edge_send.at[l], edge_recv.at[l], edge_send_sem.at[l], edge_recv_sem.at[l],
            ((s + 1) % S, t),
        )

    def send_edge(l):
        rows = slice(R - 16, R)
        edge_send[l] = (
            inner_rows[0, rows].astype(f32) * inner_rows[1, rows].astype(f32)
        ).astype(bf16)

        @pl.when(s < S - 1)
        def _():
            edge_copy(l).start()

    def mix(l):
        if l == 0:
            first_scale()
            for m in range(2):
                def join(tile):
                    inner_rows[m, tile_rows(tile)] = joined(m, tile_rows(tile))

                def arrive(tile):
                    part_copy(m, tile, True).wait_recv()
                    join(tile)

                arrive(0)
                if m == 1:
                    send_edge(l)
                loop(TILES - 1, lambda i: arrive(i + 1))
        value = (inner_rows[0].astype(f32) * inner_rows[1].astype(f32)).astype(bf16)
        product[8:8 + R, :] = value.astype(f32)
        if l == 0:
            first_weight(2)
            loop(TILES, lambda tile: first_product(tile, 2))
            weight_first(4)
            weight_first(5)

        @pl.when(s > 0)
        def _():
            edge_copy(l).wait_recv()
            product[0:8, :] = edge_recv[l].astype(f32)[8:, :]

        @pl.when(s == 0)
        def _():
            product[0:8, :] = jnp.zeros((8, C), f32)

    def gates(l, tile):
        size = RT
        first = pl.multiple_of(first_of(tile, size), size)
        rows = pl.ds(first, size)
        if l == 0:
            part_copy(2, tile, True).wait_recv()
            gate = joined(2, rows)
        else:
            gate = jnp.dot(
                normed[rows, :], weights[l - 1, 2].reshape(D, C), preferred_element_type=f32
            ).astype(bf16)
        window = product[pl.ds(first, size + 8), :]
        filtered = jnp.zeros((size, C), f32)
        for k in range(TAPS):
            begin = 8 - (TAPS - 1) + k
            filtered = filtered + taps[k, l:l + 1, :] * window[begin:begin + size]
        mixed[rows, :] = (gate.astype(f32) * filtered).astype(bf16)

    def partials(l, tile, dests):
        rows = tile_rows(tile)
        for own in (False, True):
            for d in dests:
                part = core if own else 1 - core
                columns = pl.ds(pl.multiple_of(part * F, F), F)
                value = jnp.dot(
                    mixed[rows, :], outs[l, d, :, columns], preferred_element_type=f32
                ).astype(bf16)
                if own:
                    own_part[l, d, rows] = value
                else:
                    pair_send[l, d, rows] = value
                    pair_copy(l, tile, d).start()

    def launch_tile(l, tile, ranks):
        for i in range(share):
            launch(l, tile * share + i, ranks, i)

    def launch(l, tile, ranks, i):
        @pl.when(z == 0)
        def _():
            swap = 1 - x if l == last else 0
            for rank in ranks:
                d = NZ - 1 - rank
                if rank < 2:
                    d = d + swap * (2 * rank - 1)
                run_event(0, l, ("R", tile, d), None, i)

        @pl.when(z == NZ - 1)
        def _():
            swap = x if l == last else 0
            for rank in ranks:
                d = rank
                if rank < 2:
                    d = d + swap * (1 - 2 * rank)
                run_event(NZ - 1, l, ("L", tile, d), None, i)

    def drain_first():
        drained(acts.at[pl.ds(0, 4), 0], act_twin_send.at[0], partner)
        drained(acts.at[0, 0], cross_send.at[0], y_peer)
        for zi in range(NZ):
            @pl.when(zz == zi)
            def _():
                for n, way in enumerate("ud"):
                    count = sum(way in ways for ways in LINK_SENDS[zi].values())
                    if count:
                        drained(acts.at[pl.ds(0, count), 0], line_send.at[n], partner)
        drained(part_send, part_send_sem.at[0], y_peer)
        block = first_squares.at[pl.ds(0, T - 1)]
        drained(block, square_send.at[1], partner)
        drained(first_w.at[pl.ds(0, 3), pl.ds(0, 2)], first_send.at[0], x_peer)

    def drain_gather(l):
        drained(stream.at[l - 1, pl.ds(0, NZ)], twin_send.at[l - 1], partner)
        for zi in range(NZ):
            @pl.when(z == zi)
            def _():
                for direction, count in enumerate((zi + 1 if zi < NZ - 1 else 0, NZ - zi if zi > 0 else 0)):
                    if count:
                        drained(
                            stream.at[l - 1, pl.ds(0, count)], gather_send.at[l - 1, direction], partner
                        )

    def drain_reduce(l):
        @pl.when(s < S - 1)
        def _():
            edge_copy(l).wait_send()

        drained(pair_send.at[l], pair_send_sem.at[l], partner)
        for zi in range(NZ):
            @pl.when(z == zi)
            def _():
                for direction, count in enumerate((NZ - 1 - zi, zi)):
                    if count:
                        drained(
                            own_part.at[l, pl.ds(0, count)], reduce_send.at[l, direction], partner
                        )

    weight_copy(3, 0, 0).start()
    for k in range(3):
        first_copy(k).start()
    for copy in locals_[:3]:
        copy.wait()
    stages = first_plan(TILES)
    for tile in range(TILES):
        for zi in range(NZ):
            @pl.when(zz == zi)
            def _():
                for event in stages[tile][zi]:
                    first_event(zi, event)
        block = acts.at[pl.ds(0, 4), 0, rows_of(tile)]
        remote(block, block, act_twin_send.at[0], act_twin_recv.at[tile], partner).wait_recv()
        scale_tile(tile)
        if tile == 0:
            first_weight(0)
        first_product(tile, 0)
    first_weight(1)
    loop(TILES, lambda tile: first_product(tile, 1))
    for copy in locals_[6:]:
        copy.wait()
    for l in range(L):
        mix(l)
        if l > 0:
            if l == 1:
                drain_first()
                weight_drain(3)
            else:
                for i in range(4 * l - 4, 4 * l):
                    weight_drain(i)
            drain_gather(l)
            drain_reduce(l - 1)
            weight_ready(4 * l + 2)
        if l < last:
            weight_ready(4 * l + 3)
            ranks, dests = range(NZ - 1), range(NZ)
        else:
            for axis in (1, 0):
                for piece in range(2):
                    piece_copy(axis, piece, True).wait_recv()
                weight_copy(4 * l + 3, 1 - axis, 1).start()
            turn = (x + jnp.where(z < NZ // 2, NZ - 2, 0) - diagonal + NZ) % NZ
            ranks, dests = (0,), ((diagonal + turn) % NZ,)

        def step(tile):
            gates(l, tile)
            partials(l, tile, dests)

            @pl.when(tile > 0)
            def _():
                launch_tile(l, tile - 1, ranks)

        loop(TILES, step)
        if l < last:
            launch_tile(l, TILES - 1, ranks)
            run_phase(l, l + 1, ((12.0, 4 * l + 4), (24.0, 4 * l + 5), (40.0, 4 * l + 6)) + (((57.0, 4 * l + 7),) if l + 1 < last else ()))
        else:
            others = [(diagonal + 1 + (turn + n) % (NZ - 1)) % NZ for n in range(NZ - 2)]

            def rest(tile):
                partials(l, tile, others)

                @pl.when(tile == 0)
                def _():
                    launch_tile(l, TILES - 1, ranks)

            loop(TILES, rest)
            weight_ready(4 * l + 3)
            loop(TILES, lambda tile: partials(l, tile, (diagonal,)))
            for rank in range(1, NZ - 1):
                loop(TILES, lambda tile: launch_tile(l, tile, (rank,)))
            run_phase(l, None, ())

    drain_reduce(last)
    for i in range(4 * last, 4 * L):
        weight_drain(i)
    for tile in range(TILES):
        block = squares.at[tile, pl.ds(0, T - 1)]
        remote(block, block, square_send.at[0], square_recv.at[tile], partner).wait_recv()
        total = squares[tile, 0]
        for k in range(1, T):
            total = total + squares[tile, k]
        scale_rows[:, rows_of(tile)] = lax.rsqrt(total / D + NORM_FLOOR)
    outgoing = pltpu.make_async_copy(scale_rows, scales, local_sem.at[0])
    outgoing.start()
    drained(squares.at[pl.ds(0, TILES), pl.ds(0, T - 1)], square_send.at[0], partner)
    for tile in range(TILES):
        closing_copy(tile).wait()
    outgoing.wait()


def finish(pieces, closing, scale, gain, result, rows_in, scale_in, gain_in, rows_out, sems):
    R, F = rows_in.shape
    step = R // pieces

    def copies(i):
        rows = pl.ds(i * step, step)
        return (
            pltpu.make_async_copy(closing.at[rows], rows_in.at[rows], sems.at[i]),
            pltpu.make_async_copy(rows_out.at[rows], result.at[rows], sems.at[i]),
        )

    small = [
        pltpu.make_async_copy(scale, scale_in, sems.at[pieces]),
        pltpu.make_async_copy(gain, gain_in, sems.at[pieces + 1]),
    ]
    for copy in small:
        copy.start()
    for i in range(pieces):
        copies(i)[0].start()
    for copy in small:
        copy.wait()
    for i in range(pieces):
        rows = slice(i * step, (i + 1) * step)
        factor = jnp.broadcast_to(scale_in[:, rows], (128, step)).T
        copies(i)[0].wait()
        for b in range(F // 128):
            columns = slice(b * 128, (b + 1) * 128)
            rows_out[rows, columns] = (
                rows_in[rows, columns].astype(f32) * factor * gain_in[:, columns]
            )
        copies(i)[1].start()
    for i in range(pieces):
        copies(i)[1].wait()


def paired_call(S, T, L, R, F, C, DS, TAPS):
    NZ, TB = T // 2, T // S
    dma = pltpu.SemaphoreType.DMA
    any_space = pl.BlockSpec(memory_space=pl.ANY)
    return pl.pallas_call(
        functools.partial(paired_kernel, (S, T, L, R, F, C, DS, TAPS)),
        out_shape=(jax.ShapeDtypeStruct((R, F), bf16), jax.ShapeDtypeStruct((1, R), f32)),
        in_specs=[any_space] * 7,
        out_specs=(any_space, any_space),
        scratch_shapes=[
            pltpu.VMEM((6, 2, R, F), bf16),
            pltpu.VMEM((L - 1, T, R, F), bf16),
            pltpu.VMEM((R, T * F), bf16),
            pltpu.VMEM((TILES, 2 * R // TILES, T // 2 * F), bf16),
            pltpu.VMEM((3, T // 2, F, C), bf16),
            pltpu.VMEM((L - 1, 3, T, F, C), bf16),
            pltpu.VMEM((L, S, C, DS), bf16),
            pltpu.VMEM((L, NZ, R, F), bf16),
            pltpu.VMEM((L, NZ, R, F), bf16),
            pltpu.VMEM((L, NZ, R, F), bf16),
            pltpu.VMEM((L, 2, NZ, R, F), bf16),
            pltpu.VMEM((3, R, C), bf16),
            pltpu.VMEM((3, R, C), bf16),
            pltpu.VMEM((3, R, C), f32),
            pltpu.VMEM((R + 8, C), f32),
            pltpu.VMEM((L, 16, C), bf16),
            pltpu.VMEM((L, 16, C), bf16),
            pltpu.VMEM((2, R, C), bf16),
            pltpu.VMEM((R, C), bf16),
            pltpu.VMEM((R, F), bf16),
            pltpu.VMEM((TILES, T, 1, R // TILES), f32),
            pltpu.VMEM((T, 1, R), f32),
            pltpu.VMEM((R, 128), f32),
            pltpu.VMEM((L, T * F), f32),
            pltpu.VMEM((TAPS, L, C), f32),
            pltpu.VMEM((1, R), f32),
            dma((6, TILES)), dma((2,)), dma((1,)), dma((TILES,)), dma((1,)), dma((3,)), dma((1,)),
            dma((3, TILES)), dma((1,)), dma((4 * L - 3, 2, 2)), dma((4 * L - 3,)), dma((2,)),
            dma((L - 1, FINE, NZ)), dma((L - 1, 2)), dma((L - 1, TILES)), dma((L - 1,)),
            dma((FINE, NZ + 1)), dma((L, 2)),
            dma((TILES, NZ)), dma((L,)), dma((L,)), dma((L,)),
            dma((TILES + 1,)), dma((2,)), dma((4 * L + 6,)),
        ],
        compiler_params=pltpu.CompilerParams(
            collective_id=0, has_side_effects=True, vmem_limit_bytes=60 * 2**20
        ),
        name="mixers",
    )


def per_device(
    S, T, residual_in, norm_gain, gate_proj, filter_proj, signal_proj, conv_taps, out_proj, final_gain
):
    R, F = residual_in.shape
    L, DS, C = gate_proj.shape
    TAPS = conv_taps.shape[1]
    NZ, TB, H = T // 2, T // S, S // 2
    dma = pltpu.SemaphoreType.DMA
    cut = lambda w: w.reshape(L, TB, F, C)
    any_space = pl.BlockSpec(memory_space=pl.ANY)
    paired = S == 4 and NZ == 4 and L > 1
    if paired:
        closing, scale = paired_call(S, T, L, R, F, C, DS, TAPS)(
            residual_in, norm_gain, cut(filter_proj), cut(signal_proj),
            cut(gate_proj), out_proj, conv_taps.transpose(1, 0, 2),
        )
    else:
        closing, scale = pl.pallas_call(
            functools.partial(kernel, (S, T, L, R, F, C, DS, TAPS)),
            out_shape=(jax.ShapeDtypeStruct((R, F), bf16), jax.ShapeDtypeStruct((R, 128), f32)),
            in_specs=[any_space] * 7,
            out_specs=(any_space, any_space),
            scratch_shapes=[
                pltpu.VMEM((L, T, R, F), bf16),
                pltpu.VMEM((R, T * F), bf16),
                pltpu.VMEM((L, 3, T, F, C), bf16),
                pltpu.VMEM((L, S, C, DS), bf16),
                pltpu.VMEM((L, NZ, R, F), bf16),
                pltpu.VMEM((L, NZ, R, F), bf16),
                pltpu.VMEM((L, NZ, R, F), bf16),
                pltpu.VMEM((L, 2, NZ, R, F), bf16),
                pltpu.VMEM((R, C), bf16),
                pltpu.VMEM((R, C), bf16),
                pltpu.VMEM((R + 8, C), f32),
                pltpu.VMEM((L, 16, C), bf16),
                pltpu.VMEM((L, 16, C), bf16),
                pltpu.VMEM((R, C), bf16),
                pltpu.VMEM((R, F), bf16),
                pltpu.VMEM((TILES, T, 1, R // TILES), f32),
                pltpu.VMEM((L, T * F), f32),
                pltpu.VMEM((TAPS, L, C), f32),
                pltpu.VMEM((R, 128), f32),
                dma((4 * L, 2, H)), dma((4 * L, 2, H)),
                dma((L, TILES, 2, NZ)), dma((L, TILES, 2, NZ)),
                dma((L, TILES, NZ)), dma((L, TILES, NZ)),
                dma((L, TILES, 2, NZ)), dma((L, TILES, 2, NZ)),
                dma((L, TILES, NZ)), dma((L, TILES, NZ)),
                dma((L,)), dma((L,)),
                dma((TILES, T)), dma((TILES, T)),
                dma((4 * L + 3,)),
            ],
            compiler_params=pltpu.CompilerParams(
                collective_id=0, has_side_effects=True, vmem_limit_bytes=60 * 2**20
            ),
            name="mixers",
        )(
            residual_in, norm_gain, cut(filter_proj), cut(signal_proj),
            cut(gate_proj), out_proj, conv_taps.transpose(1, 0, 2),
        )
        scale = scale[:, 0].reshape(1, R)
    return pl.pallas_call(
        functools.partial(finish, 4),
        out_shape=jax.ShapeDtypeStruct((R, F), f32),
        in_specs=[any_space] * 3,
        out_specs=any_space,
        scratch_shapes=[
            pltpu.VMEM((R, F), bf16), pltpu.VMEM((1, R), f32), pltpu.VMEM((1, F), f32),
            pltpu.VMEM((R, F), f32), dma((6,)),
        ],
        name="finish",
    )(closing, scale, final_gain.reshape(1, F))


def solution(mesh):
    return jax.shard_map(
        functools.partial(per_device, mesh.shape["sp"], mesh.shape["tp"]),
        mesh=mesh,
        in_specs=(
            P("sp", "tp"),
            P(),
            P(None, "sp", "tp"),
            P(None, "sp", "tp"),
            P(None, "sp", "tp"),
            P(None, None, "tp"),
            P(None, "tp", "sp"),
            P("tp"),
        ),
        out_specs=P("sp", "tp"),
        check_vma=False,
    )
```

```python
import functools
import heapq

import jax
import jax.numpy as jnp
from jax import lax
from jax.experimental import pallas as pl
from jax.experimental.pallas import tpu as pltpu
from jax.sharding import PartitionSpec as P

MESH = pl.DeviceIdType.MESH
NORM_FLOOR = 1e-06
TILES = 4
FINE = 8
CHUNK_US = 11.2
HOP_US = 2.0
f32 = jnp.float32
bf16 = jnp.bfloat16


def grid_width(count):
    height = max(h for h in range(1, count + 1) if count % h == 0 and h * h <= count)
    return count // height


def snake(index, width):
    y, x = index // width, index % width
    return y * width + x + (y % 2) * (width - 1 - 2 * x)


def line_plan(count, tiles, reduce, gather):
    unit = CHUNK_US / tiles
    heap, left, ready = [], {}, {}
    for z in range(count):
        for tile in range(tiles):
            if not reduce:
                heap.append((0.0, tile, 0, z, ("F", tile, z)))
                continue
            left[z, ("F", tile, z)] = (z > 0) + (z < count - 1)
            if left[z, ("F", tile, z)] == 0:
                heap.append((0.0, tile, 0, z, ("F", tile, z)))
            if z == 0:
                for d in range(1, count):
                    order = (tile, count - d) if gather else (count - d, tile)
                    heap.append((0.0, *order, z, ("R", tile, d)))
            if z == count - 1:
                for d in range(count - 1):
                    order = (tile, d) if gather else (d, tile)
                    heap.append((0.0, *order, z, ("L", tile, d)))
    heapq.heapify(heap)
    free = {}
    out = [[] for _ in range(count)]

    def send(now, z, step, event):
        begin = max(now, free.get((z, step), 0.0))
        free[z, step] = begin + unit
        key = (z + step, event)
        ready[key] = max(ready.get(key, 0.0), begin + unit + HOP_US)
        left[key] = left.get(key, 1) - 1
        if left[key] == 0:
            heapq.heappush(heap, (ready[key], event[1], 0, z + step, event))

    while heap:
        now, _, _, z, event = heapq.heappop(heap)
        kind, tile, which = event
        out[z].append((now, event))
        if kind in "RL":
            step = 1 if kind == "R" else -1
            send(now, z, step, ("F", tile, which) if which == z + step else event)
        elif kind == "F" and gather:
            if z + 1 < count:
                send(now, z, 1, ("GR", tile, z))
            if z > 0:
                send(now, z, -1, ("GL", tile, z))
        elif kind == "GR" and z + 1 < count:
            send(now, z, 1, event)
        elif kind == "GL" and z > 0:
            send(now, z, -1, event)
    return out


def kernel(
    sizes,
    residual, gain_in, filter_w, signal_w, gate_w, out_w, taps_in,
    result, scales,
    stream, normed, weights, outs, own_part, pair_send, pair_recv, line_recv,
    filter_rows, signal_rows, product, edge_send, edge_recv, mixed, closing, squares, gain, taps, scale_rows,
    weight_send, weight_recv, gather_send, gather_recv, twin_send, twin_recv,
    reduce_send, reduce_recv, pair_send_sem, pair_recv_sem,
    edge_send_sem, edge_recv_sem, square_send, square_recv, local_sem,
):
    S, T, L, R, F, C, DS, TAPS = sizes
    NZ, TB, RT, H, D = T // 2, T // S, R // TILES, S // 2, T * F
    width = grid_width(S)
    s, t = lax.axis_index("sp"), lax.axis_index("tp")
    z, core = t // 2, t % 2
    partner = (s, t + 1 - 2 * core)
    position = snake(s, width)

    def at_position(p):
        return snake((p + 2 * S) % S, width)

    ring = [(at_position(position + 1), t), (at_position(position - 1), t)]
    last = L - 1

    barrier = pltpu.get_barrier_semaphore()
    for k in range(1, T):
        pl.semaphore_signal(barrier, inc=1, device_id=(s, (t + k) % T), device_id_type=MESH)
    for other in range(1, S):
        pl.semaphore_signal(barrier, inc=1, device_id=((s + other) % S, t), device_id_type=MESH)

    locals_ = []

    def local(src, dst):
        copy = pltpu.make_async_copy(src, dst, local_sem.at[len(locals_)])
        copy.start()
        locals_.append(copy)

    local(residual, stream.at[0, t])
    local(gain_in, gain)
    local(taps_in, taps)
    for l in range(L):
        for k, w in enumerate((filter_w, signal_w, gate_w)):
            local(w.at[l], weights.at[l, k, pl.ds(s * TB, TB)])
        local(out_w.at[l], outs.at[l, s])
    pl.semaphore_wait(barrier, T - 1 + S - 1)

    def weight_ref(i, slot, half):
        l, k = divmod(i, 4)
        if k < 3:
            if half is None:
                return weights.at[l, k, pl.ds(slot * TB, TB)]
            return weights.at[l, k, pl.ds(slot * TB, TB), pl.ds(half * (F // 2), F // 2)]
        if half is None:
            return outs.at[l, slot]
        return outs.at[l, slot, pl.ds(half * (C // 2), C // 2)]

    def weight_source(i, half):
        l, k = divmod(i, 4)
        ref = (filter_w, signal_w, gate_w, out_w)[k]
        if half is None:
            return ref.at[l]
        if k < 3:
            return ref.at[l, pl.ds(0, TB), pl.ds(half * (F // 2), F // 2)]
        return ref.at[l, pl.ds(half * (C // 2), C // 2)]

    def weight_copy(i, direction, hop, receive=False):
        sign = 1 if direction == 0 else -1
        half = direction if hop == H else None
        slot = at_position(position - sign * (hop if receive else hop - 1))
        dst = weight_ref(i, slot, half)
        src = weight_source(i, half) if hop == 1 and not receive else dst
        return pltpu.make_async_remote_copy(
            src_ref=src, dst_ref=dst,
            send_sem=weight_send.at[i, direction, hop - 1],
            recv_sem=weight_recv.at[i, direction, hop - 1],
            device_id=ring[direction], device_id_type=MESH,
        )

    def weight_first(i):
        if i < 4 * L:
            for direction in range(2):
                weight_copy(i, direction, 1).start()

    def weight_forward(i):
        for hop in range(1, H):
            for direction in range(2):
                weight_copy(i, direction, hop, True).wait_recv()
                weight_copy(i, direction, hop + 1).start()
        for step in ((2,), (2,), (), (1, 2))[i % 4]:
            weight_first(i + step)

    def weight_ready(i):
        for direction in range(2):
            weight_copy(i, direction, H, True).wait_recv()

    def rows_of(tile):
        return pl.ds(tile * RT, RT)

    def gather_copy(l, tile, src, direction):
        ref = stream.at[l, 2 * src + core, rows_of(tile)]
        return pltpu.make_async_remote_copy(
            src_ref=ref, dst_ref=ref,
            send_sem=gather_send.at[l, tile, direction, src],
            recv_sem=gather_recv.at[l, tile, direction, src],
            device_id=(s, (t + (2 if direction == 0 else T - 2)) % T), device_id_type=MESH,
        )

    def twin_copy(l, tile, src, receive=False):
        block = 2 * src + (1 - core if receive else core)
        ref = stream.at[l, block, rows_of(tile)]
        return pltpu.make_async_remote_copy(
            src_ref=ref, dst_ref=ref,
            send_sem=twin_send.at[l, tile, src], recv_sem=twin_recv.at[l, tile, src],
            device_id=partner, device_id_type=MESH,
        )

    def reduce_copy(l, tile, d, direction):
        return pltpu.make_async_remote_copy(
            src_ref=own_part.at[l, d, rows_of(tile)],
            dst_ref=line_recv.at[l, direction, d, rows_of(tile)],
            send_sem=reduce_send.at[l, tile, direction, d],
            recv_sem=reduce_recv.at[l, tile, direction, d],
            device_id=(s, (t + (2 if direction == 0 else T - 2)) % T), device_id_type=MESH,
        )

    def pair_copy(l, tile, d):
        return pltpu.make_async_remote_copy(
            src_ref=pair_send.at[l, d, rows_of(tile)], dst_ref=pair_recv.at[l, d, rows_of(tile)],
            send_sem=pair_send_sem.at[l, tile, d], recv_sem=pair_recv_sem.at[l, tile, d],
            device_id=partner, device_id_type=MESH,
        )

    def total_into(l, tile, d, incoming, base, store):
        step = min(RT, 32)

        def body(i, _):
            rows = pl.ds(pl.multiple_of(tile * RT + i * step, step), step)
            value = own_part[l, d, rows].astype(f32) + pair_recv[l, d, rows].astype(f32)
            for direction in incoming:
                value = value + line_recv[l, direction, d, rows].astype(f32)
            if base:
                value = stream[l, t, rows].astype(f32) + value
            store(rows, value.astype(bf16))
            return 0

        lax.fori_loop(0, RT // step, body, 0)

    def square_copy(tile, k, receive=False):
        block = (t + T - k) % T if receive else t
        return pltpu.make_async_remote_copy(
            src_ref=squares.at[tile, block], dst_ref=squares.at[tile, block],
            send_sem=square_send.at[tile, k], recv_sem=square_recv.at[tile, k],
            device_id=(s, (t + k) % T), device_id_type=MESH,
        )

    def close(tile):
        acc = jnp.zeros((RT, 128), f32)
        for b in range(F // 128):
            value = closing[tile * RT:(tile + 1) * RT, b * 128:(b + 1) * 128].astype(f32)
            acc = acc + value * value
        squares[tile, t] = jnp.sum(acc.T, axis=0, keepdims=True)
        for k in range(1, T):
            square_copy(tile, k).start()

    def run_event(zi, l, event, gather_layer):
        kind, tile, which = event
        if kind in "RL":
            direction = 0 if kind == "R" else 1
            pair_copy(l, tile, which).wait_recv()
            incoming = [direction] if (zi > 0 if direction == 0 else zi < NZ - 1) else []
            for d in incoming:
                reduce_copy(l, tile, which, d).wait_recv()

            def store(rows, value):
                own_part[l, which, rows] = value

            total_into(l, tile, which, incoming, False, store)
            reduce_copy(l, tile, which, direction).start()
        elif kind == "F":
            if l is not None:
                pair_copy(l, tile, zi).wait_recv()
                incoming = ([0] if zi > 0 else []) + ([1] if zi < NZ - 1 else [])
                for d in incoming:
                    reduce_copy(l, tile, zi, d).wait_recv()

                def store(rows, value):
                    if l < last:
                        stream[l + 1, t, rows] = value
                    else:
                        closing[rows] = value

                total_into(l, tile, zi, incoming, True, store)
                if l == last:
                    close(tile)
            if gather_layer is not None:
                if zi + 1 < NZ:
                    gather_copy(gather_layer, tile, zi, 0).start()
                if zi > 0:
                    gather_copy(gather_layer, tile, zi, 1).start()
                twin_copy(gather_layer, tile, zi).start()
        else:
            direction = 0 if kind == "GR" else 1
            gather_copy(gather_layer, tile, which, direction).wait_recv()
            if (zi + 1 < NZ) if direction == 0 else (zi > 0):
                gather_copy(gather_layer, tile, which, direction).start()
            twin_copy(gather_layer, tile, which).start()

    def run_phase(l, gather_layer, weight_events):
        plan = line_plan(NZ, TILES, l is not None, gather_layer is not None)
        for zi in range(NZ):
            events = [
                (now, n, e) for n, (now, e) in enumerate(plan[zi])
                if (e[0], zi) not in (("R", 0), ("L", NZ - 1))
            ]
            events += [(now, -1, ("W", i, 0)) for now, i in weight_events if i < 4 * L]
            if gather_layer is not None:
                for tile in range(TILES):
                    arrived = max(now for now, e in plan[zi] if e[1] == tile)
                    events.append((arrived + HOP_US, TILES * T * T, ("N", tile, 0)))
            events.sort(key=lambda e: (e[0], e[1]))

            @pl.when(z == zi)
            def _():
                for _, _, event in events:
                    if event[0] == "W":
                        weight_forward(event[1])
                    elif event[0] == "N":
                        normalize(gather_layer, event[1])
                    else:
                        run_event(zi, l, event, gather_layer)

    def normalize(l, tile):
        for src in range(NZ):
            twin_copy(l, tile, src, True).wait_recv()
        step = min(RT, 16)

        def body(i, _):
            rows = pl.ds(pl.multiple_of(tile * RT + i * step, step), step)
            acc = jnp.zeros((step, F), f32)
            for b in range(T):
                value = stream[l, b, rows].astype(f32)
                acc = acc + value * value
            scale = lax.rsqrt(jnp.sum(acc, axis=1, keepdims=True) / D + NORM_FLOOR)
            for b in range(T):
                value = stream[l, b, rows].astype(f32)
                normed[rows, b * F:(b + 1) * F] = (value * scale * gain[l:l + 1, b * F:(b + 1) * F]).astype(bf16)
            return 0

        lax.fori_loop(0, RT // step, body, 0)

    def project(l, k, into):
        step = min(R, 256)

        def body(i, _):
            rows = pl.ds(pl.multiple_of(i * step, step), step)
            value = jnp.dot(
                normed[rows, :], weights[l, k].reshape(D, C), preferred_element_type=f32
            )
            into[rows, :] = value.astype(bf16)
            return 0

        lax.fori_loop(0, R // step, body, 0)

    def edge_copy(l):
        return pltpu.make_async_remote_copy(
            src_ref=edge_send.at[l], dst_ref=edge_recv.at[l],
            send_sem=edge_send_sem.at[l], recv_sem=edge_recv_sem.at[l],
            device_id=((s + 1) % S, t), device_id_type=MESH,
        )

    def mix(l):
        weight_ready(4 * l)
        project(l, 0, filter_rows)
        weight_ready(4 * l + 1)
        project(l, 1, signal_rows)
        value = (filter_rows[...].astype(f32) * signal_rows[...].astype(f32)).astype(bf16)
        product[8:8 + R, :] = value.astype(f32)
        edge_send[l] = value[R - 16:, :]

        @pl.when(s < S - 1)
        def _():
            edge_copy(l).start()

        if l == 0:
            weight_forward(4 * l + 3)
        weight_ready(4 * l + 2)

        @pl.when(s > 0)
        def _():
            edge_copy(l).wait_recv()
            product[0:8, :] = edge_recv[l].astype(f32)[8:, :]

        @pl.when(s == 0)
        def _():
            product[0:8, :] = jnp.zeros((8, C), f32)

    order = sorted(range(NZ), key=lambda d: (min(d, NZ - 1 - d), -d))

    def partials(l, tile):
        first, rows = tile * RT, slice(tile * RT, (tile + 1) * RT)
        gate = jnp.dot(
            normed[rows, :], weights[l, 2].reshape(D, C), preferred_element_type=f32
        ).astype(bf16)
        filtered = jnp.zeros((RT, C), f32)
        for k in range(TAPS):
            begin = 8 - (TAPS - 1) + k + first
            filtered = filtered + taps[k, l:l + 1, :] * product[begin:begin + RT, :]
        mixed[rows, :] = (gate.astype(f32) * filtered).astype(bf16)
        if tile == 0:
            weight_ready(4 * l + 3)
        for own in (False, True):
            for d in order:
                block = 2 * d + (core if own else 1 - core)
                columns = pl.ds(pl.multiple_of((block % TB) * F, F), F)
                value = jnp.dot(
                    mixed[rows, :], outs[l, block // TB, :, columns], preferred_element_type=f32
                ).astype(bf16)
                if own:
                    own_part[l, d, rows] = value
                else:
                    pair_send[l, d, rows] = value
                    pair_copy(l, tile, d).start()

    def launch(l, tile, near=0, far=NZ):
        @pl.when(z == 0)
        def _():
            for d in range(NZ - 1, 0, -1):
                if near <= d < far:
                    run_event(0, l, ("R", tile, d), None)

        @pl.when(z == NZ - 1)
        def _():
            for d in range(NZ - 1):
                if near <= NZ - 1 - d < far:
                    run_event(NZ - 1, l, ("L", tile, d), None)

    def drain_gather(l):
        for tile in range(TILES):
            for d in range(NZ):
                twin_copy(l, tile, d).wait_send()

                @pl.when((z < NZ - 1) & (d <= z))
                def _():
                    gather_copy(l, tile, d, 0).wait_send()

                @pl.when((z > 0) & (d >= z))
                def _():
                    gather_copy(l, tile, d, 1).wait_send()

    def drain_reduce(l):
        @pl.when(s < S - 1)
        def _():
            edge_copy(l).wait_send()

        for tile in range(TILES):
            for d in range(NZ):
                pair_copy(l, tile, d).wait_send()

                @pl.when((z < NZ - 1) & (d > z))
                def _():
                    reduce_copy(l, tile, d, 0).wait_send()

                @pl.when((z > 0) & (d < z))
                def _():
                    reduce_copy(l, tile, d, 1).wait_send()

    def drain_weights(first, end):
        for i in range(first, end):
            for direction in range(2):
                for hop in range(1, H + 1):
                    weight_copy(i, direction, hop).wait_send()

    weight_first(0)
    weight_first(1)
    for copy in locals_[:3]:
        copy.wait()
    run_phase(None, 0, ((13.0, 0), (24.0, 1)))
    for copy in locals_[3:]:
        copy.wait()
    weight_forward(2)
    for l in range(L):
        mix(l)
        if l == 1:
            drain_gather(0)
        if l > 0:
            drain_gather(l)
            drain_reduce(l - 1)
            drain_weights(4 * l - 4, 4 * l)
        for tile in range(TILES):
            partials(l, tile)
            if tile > 0:
                launch(l, tile - 1, 0 if l < last else NZ - 1)
        launch(l, TILES - 1, 0 if l < last else NZ - 1)
        if l < last:
            run_phase(l, l + 1, ((8.0, 4 * l + 4), (20.0, 4 * l + 5), (36.0, 4 * l + 6), (52.0, 4 * l + 7)))
        else:
            for distance in range(NZ - 2, 0, -1):
                for tile in range(TILES):
                    launch(l, tile, distance, distance + 1)
            run_phase(l, None, ())

    drain_reduce(last)
    drain_weights(4 * last, 4 * L)
    for tile in range(TILES):
        for k in range(1, T):
            square_copy(tile, k, True).wait_recv()
        total = squares[tile, 0]
        for k in range(1, T):
            total = total + squares[tile, k]
        scale = lax.rsqrt(total / D + NORM_FLOOR)
        scale_rows[tile * RT:(tile + 1) * RT, :] = jnp.broadcast_to(scale, (128, RT)).T
    outgoing = [
        pltpu.make_async_copy(closing, result, local_sem.at[0]),
        pltpu.make_async_copy(scale_rows, scales, local_sem.at[1]),
    ]
    for copy in outgoing:
        copy.start()
    for copy in outgoing:
        copy.wait()

    for tile in range(TILES):
        for k in range(1, T):
            square_copy(tile, k).wait_send()


LINK_SENDS = (
    {0: "u", 4: "u", 2: "c"},
    {1: "ud", 0: "u", 4: "u", 2: "dc", 5: "d"},
    {2: "cd", 1: "u", 0: "u", 4: "u"},
    {3: "c"},
)
NEEDED = (0, 1, 4, 5)


def first_plan(tiles):
    unit = CHUNK_US / tiles
    heap, free = [], {}
    out = [[] for _ in range(4)]
    complete = [{tile: 0.0 for tile in range(tiles)} for _ in range(4)]
    for zz in range(4):
        for tile in range(tiles):
            heapq.heappush(heap, (0.0, tile, zz, zz))
    while heap:
        now, tile, zz, kind = heapq.heappop(heap)
        out[zz].append((now, tile, ("S" if kind == zz else "G", tile, kind)))
        if kind in NEEDED:
            complete[zz][tile] = max(complete[zz][tile], now)
        for way in LINK_SENDS[zz].get(kind, ""):
            begin = max(now, free.get((zz, way), 0.0))
            free[zz, way] = begin + unit
            target, there = {"u": (zz + 1, kind), "d": (zz - 1, kind), "c": (3 - zz, 7 - kind)}[way]
            heapq.heappush(heap, (begin + unit + HOP_US, tile, target, there))
    limits = [max(complete[zz][tile] for zz in range(4)) for tile in range(tiles)]
    for zz in range(4):
        out[zz].append((0.0, tiles, ("Q", 0, 0)))
        out[zz].append((16.0 if zz == 1 else 0.0, tiles + 1, ("Y", 0, 0)))
        out[zz].append((CHUNK_US + 7.0, tiles, ("WX", 0, 0)))
        out[zz].append((2 * CHUNK_US + 7.0, tiles, ("WY", 0, 0)))
        out[zz].sort(key=lambda e: (e[0], e[1]))
    stages = []
    for tile in range(tiles):
        low = limits[tile - 1] if tile > 0 else -1.0
        high = limits[tile] if tile < tiles - 1 else float("inf")
        stages.append([[e for now, _, e in events if low < now <= high] for events in out])
    return stages


def paired_kernel(
    sizes,
    residual, gain_in, filter_w, signal_w, gate_w, out_w, taps_in,
    result, scales,
    acts, stream, normed, first_rows, first_w, weights, outs, own_part, pair_send, pair_recv, line_recv,
    part_send, part_recv, own_sum, product, edge_send, edge_recv, inner_rows,
    mixed, closing, squares, first_squares, row_scale, gain, taps, scale_rows,
    act_recv, line_send, cross_send, act_twin_recv, act_twin_send, first_recv, first_send,
    part_recv_sem, part_send_sem, weight_recv, weight_send, piece_recv,
    gather_recv, gather_send, twin_recv, twin_send, reduce_recv, reduce_send,
    pair_recv_sem, pair_send_sem, edge_recv_sem, edge_send_sem, square_recv, square_send, local_sem,
):
    S, T, L, R, F, C, DS, TAPS = sizes
    NZ, TB, RT, D = T // 2, T // S, R // TILES, T * F
    last = L - 1
    s, t = lax.axis_index("sp"), lax.axis_index("tp")
    z, core = t // 2, t % 2
    y, x = s // 2, s % 2
    zz = z + y * (NZ - 1 - 2 * z)
    local_kind = x + y * (1 - 2 * x)
    partner = (s, t + 1 - 2 * core)
    x_peer, y_peer = (s + 1 - 2 * x, t), (s + 2 - 4 * y, t)
    x_slot, y_slot = s + 1 - 2 * x, s + 2 - 4 * y
    diagonal = S - 1 - s
    own_w = (filter_w, signal_w, gate_w, out_w)

    barrier = pltpu.get_barrier_semaphore()
    for k in range(1, T):
        pl.semaphore_signal(barrier, inc=1, device_id=(s, (t + k) % T), device_id_type=MESH)
    for other in range(1, S):
        pl.semaphore_signal(barrier, inc=1, device_id=((s + other) % S, t), device_id_type=MESH)

    locals_ = []

    def local(src, dst):
        copy = pltpu.make_async_copy(src, dst, local_sem.at[len(locals_)])
        copy.start()
        locals_.append(copy)

    def remote(src, dst, send_sem, recv_sem, device):
        return pltpu.make_async_remote_copy(
            src_ref=src, dst_ref=dst, send_sem=send_sem, recv_sem=recv_sem,
            device_id=device, device_id_type=MESH,
        )

    local(residual, acts.at[zz, core])
    local(gain_in, gain)
    local(taps_in, taps)
    for k in range(3):
        local(own_w[k].at[0], first_w.at[k, pl.ds(local_kind * 2, 2)])
    for l in range(L):
        if l > 0:
            for k in range(3):
                local(own_w[k].at[l], weights.at[l - 1, k, pl.ds(s * TB, TB)])
        local(out_w.at[l], outs.at[l, s])
    pl.semaphore_wait(barrier, T - 1 + S - 1)

    share = FINE // TILES

    def first_of(tile, size):
        return R - size - tile * size

    def rows_of(tile):
        return pl.ds(first_of(tile, RT), RT)

    def layer_rows(l, tile):
        size = R // FINE
        return pl.ds(pl.multiple_of(first_of(tile, size), size), size)

    def tile_rows(tile):
        return pl.ds(pl.multiple_of(first_of(tile, RT), RT), RT)

    def drained(ref, sem, device):
        remote(ref, ref, sem, sem, device).wait_send()


    def first_copy(k):
        block = first_w.at[k, pl.ds(local_kind * 2, 2)]
        return remote(own_w[k].at[0], block, first_send.at[0], first_recv.at[k], x_peer)

    def first_arrival(k):
        block = first_w.at[k, pl.ds(2 - local_kind * 2, 2)]
        return remote(block, block, first_send.at[0], first_recv.at[k], x_peer)

    def act_copy(kind, tile, way):
        ref = acts.at[kind, core, rows_of(tile)]
        if way == "c":
            there = 7 - kind
            return remote(
                ref, acts.at[there, core, rows_of(tile)],
                cross_send.at[0], act_recv.at[there, tile], y_peer,
            )
        step = 2 - 4 * y if way == "u" else 4 * y - 2
        return remote(
            ref, ref, line_send.at["ud".index(way)], act_recv.at[kind, tile], (s, (t + step + T) % T)
        )

    def act_arrival(kind, tile):
        ref = acts.at[kind, core, rows_of(tile)]
        return remote(ref, ref, cross_send.at[0], act_recv.at[kind, tile], y_peer)

    def act_twin(kind, tile):
        ref = acts.at[kind, core, rows_of(tile)]
        return remote(ref, ref, act_twin_send.at[0], act_twin_recv.at[tile], partner)

    def part_copy(m, tile, receive=False):
        return remote(
            part_send.at[m, rows_of(tile)], part_recv.at[m, rows_of(tile)],
            part_send_sem.at[0], part_recv_sem.at[m, tile], y_peer,
        )

    def first_square_copy(k):
        return remote(
            first_squares.at[t], first_squares.at[t],
            square_send.at[1], square_recv.at[TILES], (s, (t + k) % T),
        )

    def row_squares(ref, tile):
        acc = jnp.zeros((RT, 128), f32)
        for b in range(F // 128):
            value = ref[rows_of(tile), b * 128:(b + 1) * 128].astype(f32)
            acc = acc + value * value
        return jnp.sum(acc.T, axis=0, keepdims=True)

    def first_event(zi, event):
        what, tile, kind = event
        if what in "SG":
            if what == "G":
                act_arrival(kind, tile).wait_recv()
            for way in LINK_SENDS[zi].get(kind, ""):
                act_copy(kind, tile, way).start()
            if kind in NEEDED:
                act_twin(kind, tile).start()
        elif what == "Q":
            for i in range(TILES):
                first_squares[t, :, i * RT:(i + 1) * RT] = row_squares(acts.at[zi, core], i)
            for k in range(1, T):
                first_square_copy(k).start()
        elif what == "Y":
            weight_copy(3, 1, 0).start()
        else:
            axis = "XY".index(what[1])
            weight_arrival(3, axis, 0).wait_recv()
            weight_copy(3, 1 - axis, 1).start()

    def scale_tile(tile):
        step = min(RT, 32)

        def body(i, _):
            rows = pl.ds(pl.multiple_of(first_of(tile, RT) + i * step, step), step)
            for kind in NEEDED:
                j, below = (kind, RT) if kind < 2 else (kind - 4, 0)
                block = j + y * (NZ - 1 - 2 * j)
                into = pl.ds(pl.multiple_of(below + i * step, step), step)
                for c in range(2):
                    columns = pl.ds(pl.multiple_of((2 * block + c) * F, F), F)
                    value = acts[kind, c, rows].astype(f32) * gain[0:1, columns]
                    begin = (2 * j + c) * F
                    first_rows[tile, into, begin:begin + F] = value.astype(bf16)
            return 0

        lax.fori_loop(0, RT // step, body, 0)

    def first_product(tile, m):
        value = jnp.dot(
            first_rows[tile], first_w[m].reshape(D // 2, C), preferred_element_type=f32
        )
        rows = tile_rows(tile)
        part_send[m, rows] = value[:RT].astype(bf16)
        part_copy(m, tile).start()
        own_sum[m, rows] = value[RT:]

    def first_weight(m):
        locals_[3 + m].wait()
        first_arrival(m).wait_recv()

    def loop(count, body):
        def step(i, _):
            body(i)
            return 0

        lax.fori_loop(0, count, step, 0)

    def joined(m, rows):
        scale = row_scale[rows, :]
        total = own_sum[m, rows] + part_recv[m, rows].astype(f32)
        return jnp.concatenate(
            [total[:, b * 128:(b + 1) * 128] * scale for b in range(C // 128)], axis=1
        ).astype(bf16)

    def first_scale():
        block = first_squares.at[pl.ds(0, T - 1)]
        remote(block, block, square_send.at[1], square_recv.at[TILES], partner).wait_recv()
        total = first_squares[0]
        for k in range(1, T):
            total = total + first_squares[k]
        scale = lax.rsqrt(total / D + NORM_FLOOR)
        for i in range(TILES):
            row_scale[rows_of(i), :] = jnp.broadcast_to(
                scale[:, i * RT:(i + 1) * RT], (128, RT)
            ).T


    def weight_ref(i, slot, half=None):
        l, k = divmod(i, 4)
        if k < 3:
            if half is None:
                return weights.at[l - 1, k, pl.ds(slot * TB, TB)]
            cut = F * 9 // 16
            return weights.at[l - 1, k, pl.ds(slot * TB, TB), pl.ds(cut * half, F - cut if half else cut)]
        if half is None:
            return outs.at[l, slot]
        cut = C // 4 if l == 0 else C // 2
        return outs.at[l, slot, pl.ds(cut * half, C - cut if half else cut)]

    def weight_copy(i, axis, hop):
        l, k = divmod(i, 4)
        if hop == 0:
            src, dst = own_w[k].at[l], weight_ref(i, s)
        else:
            src = dst = weight_ref(i, (y_slot, x_slot)[axis], axis)
        return remote(
            src, dst, weight_send.at[i - 3], weight_recv.at[i - 3, axis, hop], (x_peer, y_peer)[axis]
        )

    def piece_copy(axis, piece, receive=False):
        rows = pl.ds(piece * (C // 2), C // 2)
        dst = outs.at[last, (x_slot, y_slot)[axis] if receive else s, rows]
        return remote(
            dst if receive else out_w.at[last, rows], dst, weight_send.at[4 * last],
            weight_recv.at[4 * last, axis, 0] if piece else piece_recv.at[axis], (x_peer, y_peer)[axis],
        )

    def weight_arrival(i, axis, hop):
        ref = weight_ref(i, (x_slot, y_slot)[axis]) if hop == 0 else weight_ref(i, diagonal, axis)
        return remote(
            ref, ref, weight_send.at[i - 3], weight_recv.at[i - 3, axis, hop], (x_peer, y_peer)[axis]
        )

    def weight_first(i):
        if i < 4 * L:
            for axis in range(2):
                weight_copy(i, axis, 0).start()

    def weight_forward(i):
        for axis in range(2):
            weight_arrival(i, 1 - axis, 0).wait_recv()
            weight_copy(i, axis, 1).start()
        if i == 4 * last + 2:
            for axis in range(2):
                piece_copy(axis, 0).start()
        elif i != 4 * last + 1:
            for step in ((2,), (2,), (), (1, 2))[i % 4]:
                weight_first(i + step)

    def weight_ready(i):
        for axis in range(2):
            weight_arrival(i, axis, 1).wait_recv()

    def weight_drain(i):
        l, k = divmod(i, 4)
        ref = weights.at[l - 1, k, pl.ds(0, 3 * TB)] if k < 3 else outs.at[l, pl.ds(0, 3)]
        drained(ref, weight_send.at[i - 3], x_peer)

    def line_peer(direction):
        return (s, (t + (2 if direction == 0 else T - 2)) % T)

    def gather_copy(l, tile, src, direction):
        ref = stream.at[l - 1, 2 * src + core, layer_rows(l - 1, tile)]
        return remote(
            ref, ref, gather_send.at[l - 1, direction], gather_recv.at[l - 1, tile, src],
            line_peer(direction),
        )

    def twin_copy(l, tile, src):
        ref = stream.at[l - 1, 2 * src + core, layer_rows(l - 1, tile)]
        group = tile // share
        return remote(ref, ref, twin_send.at[l - 1], twin_recv.at[l - 1, group], partner)

    def reduce_copy(l, tile, d, direction):
        return remote(
            own_part.at[l, d, layer_rows(l, tile)], line_recv.at[l, direction, d, layer_rows(l, tile)],
            reduce_send.at[l, direction], reduce_recv.at[tile, d + 1 - direction],
            line_peer(direction),
        )

    def pair_copy(l, tile, d):
        return remote(
            pair_send.at[l, d, tile_rows(tile)], pair_recv.at[l, d, tile_rows(tile)],
            pair_send_sem.at[l], pair_recv_sem.at[tile, d], partner,
        )

    def total_into(l, tile, d, incoming, base, store):
        size = R // FINE
        step = min(size, 32)

        def body(i, _):
            rows = pl.ds(pl.multiple_of(first_of(tile, size) + i * step, step), step)
            value = own_part[l, d, rows].astype(f32) + pair_recv[l, d, rows].astype(f32)
            for direction in incoming:
                value = value + line_recv[l, direction, d, rows].astype(f32)
            if base:
                before = acts[zz, core, rows] if l == 0 else stream[l - 1, t, rows]
                value = before.astype(f32) + value
            store(rows, value.astype(bf16))
            return 0

        lax.fori_loop(0, size // step, body, 0)

    def square_copy(tile, k):
        return remote(
            squares.at[tile, t], squares.at[tile, t],
            square_send.at[0], square_recv.at[tile], (s, (t + k) % T),
        )

    def close(tile):
        squares[tile, t] = row_squares(closing, tile)
        for k in range(1, T):
            square_copy(tile, k).start()
        closing_copy(tile).start()

    def closing_copy(tile):
        return pltpu.make_async_copy(
            closing.at[rows_of(tile)], result.at[rows_of(tile)], local_sem.at[1 + tile]
        )

    def pair_arrival(l, tile, d, i):
        if i is None:
            i = tile % share
        if i == 0:
            pair_copy(l, tile // share, d).wait_recv()

    def run_event(zi, l, event, gather_layer, i=None):
        kind, tile, which = event
        if kind in "RL":
            direction = 0 if kind == "R" else 1
            pair_arrival(l, tile, which, i)
            incoming = [direction] if (zi > 0 if direction == 0 else zi < NZ - 1) else []
            for d in incoming:
                reduce_copy(l, tile, which, d).wait_recv()

            def store(rows, value):
                own_part[l, which, rows] = value

            total_into(l, tile, which, incoming, False, store)
            reduce_copy(l, tile, which, direction).start()
        elif kind == "F":
            pair_arrival(l, tile, zi, i)
            incoming = ([0] if zi > 0 else []) + ([1] if zi < NZ - 1 else [])
            for d in incoming:
                reduce_copy(l, tile, zi, d).wait_recv()

            def store(rows, value):
                if l < last:
                    stream[l, t, rows] = value
                else:
                    closing[rows] = value

            total_into(l, tile, zi, incoming, True, store)
            if l == last:
                if tile % share == share - 1:
                    close(tile // share)
            else:
                if zi + 1 < NZ:
                    gather_copy(gather_layer, tile, zi, 0).start()
                if zi > 0:
                    gather_copy(gather_layer, tile, zi, 1).start()
                twin_copy(gather_layer, tile, zi).start()
        else:
            direction = 0 if kind == "GR" else 1
            gather_copy(gather_layer, tile, which, direction).wait_recv()
            if (zi + 1 < NZ) if direction == 0 else (zi > 0):
                gather_copy(gather_layer, tile, which, direction).start()
            twin_copy(gather_layer, tile, which).start()

    def run_phase(l, gather_layer, weight_events):
        tiles = FINE
        plan = line_plan(NZ, tiles, True, gather_layer is not None)
        groups = TILES if gather_layer is not None else 1
        ends = [
            max(now for z_events in plan for now, e in z_events if e[1] * groups // tiles <= g)
            for g in range(groups)
        ]
        for g in range(groups):
            low = ends[g - 1] if g > 0 else -1.0
            high = ends[g] if g < groups - 1 else float("inf")
            for zi in range(NZ):
                events = [
                    (now, n, e) for n, (now, e) in enumerate(plan[zi])
                    if (e[0], zi) not in (("R", 0), ("L", NZ - 1))
                ]
                events += [(now, -1, ("W", i, 0)) for now, i in weight_events if i < 4 * L]
                events = sorted((e for e in events if low < e[0] <= high), key=lambda e: (e[0], e[1]))

                @pl.when(z == zi)
                def _():
                    for _, _, event in events:
                        if event[0] == "W":
                            weight_forward(event[1])
                        else:
                            run_event(zi, l, event, gather_layer)

            if gather_layer is not None:
                normalize(gather_layer, g)
                if g == 0:
                    weight_ready(4 * gather_layer)
                    weight_ready(4 * gather_layer + 1)
                    loop(2, lambda k: project(gather_layer, k, R - RT, RT))
                    send_edge(gather_layer)
                    if gather_layer == last:
                        for axis in range(2):
                            piece_copy(axis, 1).start()
                elif g >= groups - 2:
                    size = R - 2 * RT if g < groups - 1 else RT
                    loop(2, lambda k: project(gather_layer, k, R - RT - size if g < groups - 1 else 0, size))

    def normalize(l, tile):
        block = stream.at[l - 1, pl.ds(0, NZ), rows_of(tile)]
        remote(block, block, twin_send.at[l - 1], twin_recv.at[l - 1, tile], partner).wait_recv()
        step = min(RT, 16)

        def body(i, _):
            rows = pl.ds(pl.multiple_of(first_of(tile, RT) + i * step, step), step)
            acc = jnp.zeros((step, F), f32)
            for b in range(T):
                value = stream[l - 1, b, rows].astype(f32)
                acc = acc + value * value
            scale = lax.rsqrt(jnp.sum(acc, axis=1, keepdims=True) / D + NORM_FLOOR)
            for b in range(T):
                value = stream[l - 1, b, rows].astype(f32)
                columns = slice(b * F, (b + 1) * F)
                normed[rows, columns] = (value * scale * gain[l:l + 1, columns]).astype(bf16)
            return 0

        lax.fori_loop(0, RT // step, body, 0)

    def project(l, k, first, size):
        rows = pl.ds(first, size)
        value = jnp.dot(
            normed[rows, :], weights[l - 1, k].reshape(D, C), preferred_element_type=f32
        )
        inner_rows[k, rows] = value.astype(bf16)

    def edge_copy(l):
        return remote(
            edge_send.at[l], edge_recv.at[l], edge_send_sem.at[l], edge_recv_sem.at[l],
            ((s + 1) % S, t),
        )

    def send_edge(l):
        rows = slice(R - 16, R)
        edge_send[l] = (
            inner_rows[0, rows].astype(f32) * inner_rows[1, rows].astype(f32)
        ).astype(bf16)

        @pl.when(s < S - 1)
        def _():
            edge_copy(l).start()

    def mix(l):
        if l == 0:
            first_scale()

            def arrive(m, tile):
                part_copy(m, tile, True).wait_recv()
                inner_rows[m, tile_rows(tile)] = joined(m, tile_rows(tile))

            arrive(0, 0)
            arrive(1, 0)
            send_edge(l)
            for i in (4, 5):
                weight_copy(i, 0, 0).start()
            loop(TILES - 1, lambda i: arrive(0, i + 1))
            first_weight(2)
            loop(TILES, lambda tile: first_product(tile, 2))
            for i in (4, 5):
                weight_copy(i, 1, 0).start()
            loop(TILES - 1, lambda i: arrive(1, i + 1))
        value = (inner_rows[0].astype(f32) * inner_rows[1].astype(f32)).astype(bf16)
        product[8:8 + R, :] = value.astype(f32)
        @pl.when(s > 0)
        def _():
            edge_copy(l).wait_recv()
            product[0:8, :] = edge_recv[l].astype(f32)[8:, :]

        @pl.when(s == 0)
        def _():
            product[0:8, :] = jnp.zeros((8, C), f32)

    def gates(l, tile):
        size = RT
        first = pl.multiple_of(first_of(tile, size), size)
        rows = pl.ds(first, size)
        if l == 0:
            part_copy(2, tile, True).wait_recv()
            gate = joined(2, rows)
        else:
            gate = jnp.dot(
                normed[rows, :], weights[l - 1, 2].reshape(D, C), preferred_element_type=f32
            ).astype(bf16)
        window = product[pl.ds(first, size + 8), :]
        filtered = jnp.zeros((size, C), f32)
        for k in range(TAPS):
            begin = 8 - (TAPS - 1) + k
            filtered = filtered + taps[k, l:l + 1, :] * window[begin:begin + size]
        mixed[rows, :] = (gate.astype(f32) * filtered).astype(bf16)

    def partials(l, tile, dests):
        rows = tile_rows(tile)
        for own in (False, True):
            for d in dests:
                part = core if own else 1 - core
                columns = pl.ds(pl.multiple_of(part * F, F), F)
                value = jnp.dot(
                    mixed[rows, :], outs[l, d, :, columns], preferred_element_type=f32
                ).astype(bf16)
                if own:
                    own_part[l, d, rows] = value
                else:
                    pair_send[l, d, rows] = value
                    pair_copy(l, tile, d).start()

    def launch_tile(l, tile, ranks):
        for i in range(share):
            launch(l, tile * share + i, ranks, i)

    def launch(l, tile, ranks, i):
        @pl.when(z == 0)
        def _():
            swap = 1 - x if l == last else 0
            for rank in ranks:
                d = NZ - 1 - rank
                if rank < 2:
                    d = d + swap * (2 * rank - 1)
                run_event(0, l, ("R", tile, d), None, i)

        @pl.when(z == NZ - 1)
        def _():
            swap = x if l == last else 0
            for rank in ranks:
                d = rank
                if rank < 2:
                    d = d + swap * (1 - 2 * rank)
                run_event(NZ - 1, l, ("L", tile, d), None, i)

    def drain_first():
        drained(acts.at[pl.ds(0, 4), 0], act_twin_send.at[0], partner)
        drained(acts.at[0, 0], cross_send.at[0], y_peer)
        for zi in range(NZ):
            @pl.when(zz == zi)
            def _():
                for n, way in enumerate("ud"):
                    count = sum(way in ways for ways in LINK_SENDS[zi].values())
                    if count:
                        drained(acts.at[pl.ds(0, count), 0], line_send.at[n], partner)
        drained(part_send, part_send_sem.at[0], y_peer)
        block = first_squares.at[pl.ds(0, T - 1)]
        drained(block, square_send.at[1], partner)
        drained(first_w.at[pl.ds(0, 3), pl.ds(0, 2)], first_send.at[0], x_peer)

    def drain_gather(l):
        drained(stream.at[l - 1, pl.ds(0, NZ)], twin_send.at[l - 1], partner)
        for zi in range(NZ):
            @pl.when(z == zi)
            def _():
                for direction, count in enumerate((zi + 1 if zi < NZ - 1 else 0, NZ - zi if zi > 0 else 0)):
                    if count:
                        drained(
                            stream.at[l - 1, pl.ds(0, count)], gather_send.at[l - 1, direction], partner
                        )

    def drain_reduce(l):
        @pl.when(s < S - 1)
        def _():
            edge_copy(l).wait_send()

        drained(pair_send.at[l], pair_send_sem.at[l], partner)
        for zi in range(NZ):
            @pl.when(z == zi)
            def _():
                for direction, count in enumerate((NZ - 1 - zi, zi)):
                    if count:
                        drained(
                            own_part.at[l, pl.ds(0, count)], reduce_send.at[l, direction], partner
                        )

    weight_copy(3, 0, 0).start()
    for k in range(3):
        first_copy(k).start()
    for copy in locals_[:3]:
        copy.wait()
    stages = first_plan(TILES)
    for tile in range(TILES):
        for zi in range(NZ):
            @pl.when(zz == zi)
            def _():
                for event in stages[tile][zi]:
                    first_event(zi, event)
        block = acts.at[pl.ds(0, 4), 0, rows_of(tile)]
        remote(block, block, act_twin_send.at[0], act_twin_recv.at[tile], partner).wait_recv()
        scale_tile(tile)
        if tile == 0:
            first_weight(0)
        first_product(tile, 0)
    first_weight(1)
    loop(TILES, lambda tile: first_product(tile, 1))
    for copy in locals_[6:]:
        copy.wait()
    for l in range(L):
        mix(l)
        if l > 0:
            if l == 1:
                drain_first()
                weight_drain(3)
            else:
                for i in range(4 * l - 4, 4 * l):
                    weight_drain(i)
            drain_gather(l)
            drain_reduce(l - 1)
            weight_ready(4 * l + 2)
        if l < last:
            weight_ready(4 * l + 3)
            ranks, dests = range(NZ - 1), range(NZ)
        else:
            for axis in (1, 0):
                for piece in range(2):
                    piece_copy(axis, piece, True).wait_recv()
                weight_copy(4 * l + 3, 1 - axis, 1).start()
            turn = (x + jnp.where(z < NZ // 2, NZ - 2, 0) - diagonal + NZ) % NZ
            ranks, dests = (0,), ((diagonal + turn) % NZ,)

        def step(tile):
            gates(l, tile)
            partials(l, tile, dests)

            @pl.when(tile > 0)
            def _():
                launch_tile(l, tile - 1, ranks)

        loop(TILES, step)
        if l < last:
            launch_tile(l, TILES - 1, ranks)
            run_phase(l, l + 1, ((12.0, 4 * l + 4), (24.0, 4 * l + 5), (40.0, 4 * l + 6)) + (((57.0, 4 * l + 7),) if l + 1 < last else ()))
        else:
            others = [(diagonal + 1 + (turn + n) % (NZ - 1)) % NZ for n in range(NZ - 2)]

            def rest(tile):
                partials(l, tile, others)

                @pl.when(tile == 0)
                def _():
                    launch_tile(l, TILES - 1, ranks)

            loop(TILES, rest)
            weight_ready(4 * l + 3)
            loop(TILES, lambda tile: partials(l, tile, (diagonal,)))
            for rank in range(1, NZ - 1):
                loop(TILES, lambda tile: launch_tile(l, tile, (rank,)))
            run_phase(l, None, ())

    drain_reduce(last)
    for i in range(4 * last, 4 * L):
        weight_drain(i)
    for tile in range(TILES):
        block = squares.at[tile, pl.ds(0, T - 1)]
        remote(block, block, square_send.at[0], square_recv.at[tile], partner).wait_recv()
        total = squares[tile, 0]
        for k in range(1, T):
            total = total + squares[tile, k]
        scale_rows[:, rows_of(tile)] = lax.rsqrt(total / D + NORM_FLOOR)
    outgoing = pltpu.make_async_copy(scale_rows, scales, local_sem.at[0])
    outgoing.start()
    drained(squares.at[pl.ds(0, TILES), pl.ds(0, T - 1)], square_send.at[0], partner)
    for tile in range(TILES):
        closing_copy(tile).wait()
    outgoing.wait()


def finish(pieces, closing, scale, gain, result, rows_in, scale_in, gain_in, rows_out, sems):
    R, F = rows_in.shape
    step = R // pieces

    def copies(i):
        rows = pl.ds(i * step, step)
        return (
            pltpu.make_async_copy(closing.at[rows], rows_in.at[rows], sems.at[i]),
            pltpu.make_async_copy(rows_out.at[rows], result.at[rows], sems.at[i]),
        )

    small = [
        pltpu.make_async_copy(scale, scale_in, sems.at[pieces]),
        pltpu.make_async_copy(gain, gain_in, sems.at[pieces + 1]),
    ]
    for copy in small:
        copy.start()
    for i in range(pieces):
        copies(i)[0].start()
    for copy in small:
        copy.wait()
    for i in range(pieces):
        rows = slice(i * step, (i + 1) * step)
        factor = jnp.broadcast_to(scale_in[:, rows], (128, step)).T
        copies(i)[0].wait()
        for b in range(F // 128):
            columns = slice(b * 128, (b + 1) * 128)
            rows_out[rows, columns] = (
                rows_in[rows, columns].astype(f32) * factor * gain_in[:, columns]
            )
        copies(i)[1].start()
    for i in range(pieces):
        copies(i)[1].wait()


def paired_call(S, T, L, R, F, C, DS, TAPS):
    NZ, TB = T // 2, T // S
    dma = pltpu.SemaphoreType.DMA
    any_space = pl.BlockSpec(memory_space=pl.ANY)
    return pl.pallas_call(
        functools.partial(paired_kernel, (S, T, L, R, F, C, DS, TAPS)),
        out_shape=(jax.ShapeDtypeStruct((R, F), bf16), jax.ShapeDtypeStruct((1, R), f32)),
        in_specs=[any_space] * 7,
        out_specs=(any_space, any_space),
        scratch_shapes=[
            pltpu.VMEM((6, 2, R, F), bf16),
            pltpu.VMEM((L - 1, T, R, F), bf16),
            pltpu.VMEM((R, T * F), bf16),
            pltpu.VMEM((TILES, 2 * R // TILES, T // 2 * F), bf16),
            pltpu.VMEM((3, T // 2, F, C), bf16),
            pltpu.VMEM((L - 1, 3, T, F, C), bf16),
            pltpu.VMEM((L, S, C, DS), bf16),
            pltpu.VMEM((L, NZ, R, F), bf16),
            pltpu.VMEM((L, NZ, R, F), bf16),
            pltpu.VMEM((L, NZ, R, F), bf16),
            pltpu.VMEM((L, 2, NZ, R, F), bf16),
            pltpu.VMEM((3, R, C), bf16),
            pltpu.VMEM((3, R, C), bf16),
            pltpu.VMEM((3, R, C), f32),
            pltpu.VMEM((R + 8, C), f32),
            pltpu.VMEM((L, 16, C), bf16),
            pltpu.VMEM((L, 16, C), bf16),
            pltpu.VMEM((2, R, C), bf16),
            pltpu.VMEM((R, C), bf16),
            pltpu.VMEM((R, F), bf16),
            pltpu.VMEM((TILES, T, 1, R // TILES), f32),
            pltpu.VMEM((T, 1, R), f32),
            pltpu.VMEM((R, 128), f32),
            pltpu.VMEM((L, T * F), f32),
            pltpu.VMEM((TAPS, L, C), f32),
            pltpu.VMEM((1, R), f32),
            dma((6, TILES)), dma((2,)), dma((1,)), dma((TILES,)), dma((1,)), dma((3,)), dma((1,)),
            dma((3, TILES)), dma((1,)), dma((4 * L - 3, 2, 2)), dma((4 * L - 3,)), dma((2,)),
            dma((L - 1, FINE, NZ)), dma((L - 1, 2)), dma((L - 1, TILES)), dma((L - 1,)),
            dma((FINE, NZ + 1)), dma((L, 2)),
            dma((TILES, NZ)), dma((L,)), dma((L,)), dma((L,)),
            dma((TILES + 1,)), dma((2,)), dma((4 * L + 6,)),
        ],
        compiler_params=pltpu.CompilerParams(
            collective_id=0, has_side_effects=True, vmem_limit_bytes=60 * 2**20
        ),
        name="mixers",
    )


def per_device(
    S, T, residual_in, norm_gain, gate_proj, filter_proj, signal_proj, conv_taps, out_proj, final_gain
):
    R, F = residual_in.shape
    L, DS, C = gate_proj.shape
    TAPS = conv_taps.shape[1]
    NZ, TB, H = T // 2, T // S, S // 2
    dma = pltpu.SemaphoreType.DMA
    cut = lambda w: w.reshape(L, TB, F, C)
    any_space = pl.BlockSpec(memory_space=pl.ANY)
    paired = S == 4 and NZ == 4 and L > 1
    if paired:
        closing, scale = paired_call(S, T, L, R, F, C, DS, TAPS)(
            residual_in, norm_gain, cut(filter_proj), cut(signal_proj),
            cut(gate_proj), out_proj, conv_taps.transpose(1, 0, 2),
        )
    else:
        closing, scale = pl.pallas_call(
            functools.partial(kernel, (S, T, L, R, F, C, DS, TAPS)),
            out_shape=(jax.ShapeDtypeStruct((R, F), bf16), jax.ShapeDtypeStruct((R, 128), f32)),
            in_specs=[any_space] * 7,
            out_specs=(any_space, any_space),
            scratch_shapes=[
                pltpu.VMEM((L, T, R, F), bf16),
                pltpu.VMEM((R, T * F), bf16),
                pltpu.VMEM((L, 3, T, F, C), bf16),
                pltpu.VMEM((L, S, C, DS), bf16),
                pltpu.VMEM((L, NZ, R, F), bf16),
                pltpu.VMEM((L, NZ, R, F), bf16),
                pltpu.VMEM((L, NZ, R, F), bf16),
                pltpu.VMEM((L, 2, NZ, R, F), bf16),
                pltpu.VMEM((R, C), bf16),
                pltpu.VMEM((R, C), bf16),
                pltpu.VMEM((R + 8, C), f32),
                pltpu.VMEM((L, 16, C), bf16),
                pltpu.VMEM((L, 16, C), bf16),
                pltpu.VMEM((R, C), bf16),
                pltpu.VMEM((R, F), bf16),
                pltpu.VMEM((TILES, T, 1, R // TILES), f32),
                pltpu.VMEM((L, T * F), f32),
                pltpu.VMEM((TAPS, L, C), f32),
                pltpu.VMEM((R, 128), f32),
                dma((4 * L, 2, H)), dma((4 * L, 2, H)),
                dma((L, TILES, 2, NZ)), dma((L, TILES, 2, NZ)),
                dma((L, TILES, NZ)), dma((L, TILES, NZ)),
                dma((L, TILES, 2, NZ)), dma((L, TILES, 2, NZ)),
                dma((L, TILES, NZ)), dma((L, TILES, NZ)),
                dma((L,)), dma((L,)),
                dma((TILES, T)), dma((TILES, T)),
                dma((4 * L + 3,)),
            ],
            compiler_params=pltpu.CompilerParams(
                collective_id=0, has_side_effects=True, vmem_limit_bytes=60 * 2**20
            ),
            name="mixers",
        )(
            residual_in, norm_gain, cut(filter_proj), cut(signal_proj),
            cut(gate_proj), out_proj, conv_taps.transpose(1, 0, 2),
        )
        scale = scale[:, 0].reshape(1, R)
    return pl.pallas_call(
        functools.partial(finish, 4),
        out_shape=jax.ShapeDtypeStruct((R, F), f32),
        in_specs=[any_space] * 3,
        out_specs=any_space,
        scratch_shapes=[
            pltpu.VMEM((R, F), bf16), pltpu.VMEM((1, R), f32), pltpu.VMEM((1, F), f32),
            pltpu.VMEM((R, F), f32), dma((6,)),
        ],
        name="finish",
    )(closing, scale, final_gain.reshape(1, F))


def solution(mesh):
    return jax.shard_map(
        functools.partial(per_device, mesh.shape["sp"], mesh.shape["tp"]),
        mesh=mesh,
        in_specs=(
            P("sp", "tp"),
            P(),
            P(None, "sp", "tp"),
            P(None, "sp", "tp"),
            P(None, "sp", "tp"),
            P(None, None, "tp"),
            P(None, "tp", "sp"),
            P("tp"),
        ),
        out_specs=P("sp", "tp"),
        check_vma=False,
    )
```

```python
import functools
import heapq

import jax
import jax.numpy as jnp
from jax import lax
from jax.experimental import pallas as pl
from jax.experimental.pallas import tpu as pltpu
from jax.sharding import PartitionSpec as P

MESH = pl.DeviceIdType.MESH
NORM_FLOOR = 1e-06
TILES = 4
FINE = 8
CHUNK_US = 11.2
HOP_US = 2.0
f32 = jnp.float32
bf16 = jnp.bfloat16


def grid_width(count):
    height = max(h for h in range(1, count + 1) if count % h == 0 and h * h <= count)
    return count // height


def snake(index, width):
    y, x = index // width, index % width
    return y * width + x + (y % 2) * (width - 1 - 2 * x)


def line_plan(count, tiles, reduce, gather):
    unit = CHUNK_US / tiles
    heap, left, ready = [], {}, {}
    for z in range(count):
        for tile in range(tiles):
            if not reduce:
                heap.append((0.0, tile, 0, z, ("F", tile, z)))
                continue
            left[z, ("F", tile, z)] = (z > 0) + (z < count - 1)
            if left[z, ("F", tile, z)] == 0:
                heap.append((0.0, tile, 0, z, ("F", tile, z)))
            if z == 0:
                for d in range(1, count):
                    order = (tile, count - d) if gather else (count - d, tile)
                    heap.append((0.0, *order, z, ("R", tile, d)))
            if z == count - 1:
                for d in range(count - 1):
                    order = (tile, d) if gather else (d, tile)
                    heap.append((0.0, *order, z, ("L", tile, d)))
    heapq.heapify(heap)
    free = {}
    out = [[] for _ in range(count)]

    def send(now, z, step, event):
        begin = max(now, free.get((z, step), 0.0))
        free[z, step] = begin + unit
        key = (z + step, event)
        ready[key] = max(ready.get(key, 0.0), begin + unit + HOP_US)
        left[key] = left.get(key, 1) - 1
        if left[key] == 0:
            heapq.heappush(heap, (ready[key], event[1], 0, z + step, event))

    while heap:
        now, _, _, z, event = heapq.heappop(heap)
        kind, tile, which = event
        out[z].append((now, event))
        if kind in "RL":
            step = 1 if kind == "R" else -1
            send(now, z, step, ("F", tile, which) if which == z + step else event)
        elif kind == "F" and gather:
            if z + 1 < count:
                send(now, z, 1, ("GR", tile, z))
            if z > 0:
                send(now, z, -1, ("GL", tile, z))
        elif kind == "GR" and z + 1 < count:
            send(now, z, 1, event)
        elif kind == "GL" and z > 0:
            send(now, z, -1, event)
    return out


def kernel(
    sizes,
    residual, gain_in, filter_w, signal_w, gate_w, out_w, taps_in,
    result, scales,
    stream, normed, weights, outs, own_part, pair_send, pair_recv, line_recv,
    filter_rows, signal_rows, product, edge_send, edge_recv, mixed, closing, squares, gain, taps, scale_rows,
    weight_send, weight_recv, gather_send, gather_recv, twin_send, twin_recv,
    reduce_send, reduce_recv, pair_send_sem, pair_recv_sem,
    edge_send_sem, edge_recv_sem, square_send, square_recv, local_sem,
):
    S, T, L, R, F, C, DS, TAPS = sizes
    NZ, TB, RT, H, D = T // 2, T // S, R // TILES, S // 2, T * F
    width = grid_width(S)
    s, t = lax.axis_index("sp"), lax.axis_index("tp")
    z, core = t // 2, t % 2
    partner = (s, t + 1 - 2 * core)
    position = snake(s, width)

    def at_position(p):
        return snake((p + 2 * S) % S, width)

    ring = [(at_position(position + 1), t), (at_position(position - 1), t)]
    last = L - 1

    barrier = pltpu.get_barrier_semaphore()
    for k in range(1, T):
        pl.semaphore_signal(barrier, inc=1, device_id=(s, (t + k) % T), device_id_type=MESH)
    for other in range(1, S):
        pl.semaphore_signal(barrier, inc=1, device_id=((s + other) % S, t), device_id_type=MESH)

    locals_ = []

    def local(src, dst):
        copy = pltpu.make_async_copy(src, dst, local_sem.at[len(locals_)])
        copy.start()
        locals_.append(copy)

    local(residual, stream.at[0, t])
    local(gain_in, gain)
    local(taps_in, taps)
    for l in range(L):
        for k, w in enumerate((filter_w, signal_w, gate_w)):
            local(w.at[l], weights.at[l, k, pl.ds(s * TB, TB)])
        local(out_w.at[l], outs.at[l, s])
    pl.semaphore_wait(barrier, T - 1 + S - 1)

    def weight_ref(i, slot, half):
        l, k = divmod(i, 4)
        if k < 3:
            if half is None:
                return weights.at[l, k, pl.ds(slot * TB, TB)]
            return weights.at[l, k, pl.ds(slot * TB, TB), pl.ds(half * (F // 2), F // 2)]
        if half is None:
            return outs.at[l, slot]
        return outs.at[l, slot, pl.ds(half * (C // 2), C // 2)]

    def weight_source(i, half):
        l, k = divmod(i, 4)
        ref = (filter_w, signal_w, gate_w, out_w)[k]
        if half is None:
            return ref.at[l]
        if k < 3:
            return ref.at[l, pl.ds(0, TB), pl.ds(half * (F // 2), F // 2)]
        return ref.at[l, pl.ds(half * (C // 2), C // 2)]

    def weight_copy(i, direction, hop, receive=False):
        sign = 1 if direction == 0 else -1
        half = direction if hop == H else None
        slot = at_position(position - sign * (hop if receive else hop - 1))
        dst = weight_ref(i, slot, half)
        src = weight_source(i, half) if hop == 1 and not receive else dst
        return pltpu.make_async_remote_copy(
            src_ref=src, dst_ref=dst,
            send_sem=weight_send.at[i, direction, hop - 1],
            recv_sem=weight_recv.at[i, direction, hop - 1],
            device_id=ring[direction], device_id_type=MESH,
        )

    def weight_first(i):
        if i < 4 * L:
            for direction in range(2):
                weight_copy(i, direction, 1).start()

    def weight_forward(i):
        for hop in range(1, H):
            for direction in range(2):
                weight_copy(i, direction, hop, True).wait_recv()
                weight_copy(i, direction, hop + 1).start()
        for step in ((2,), (2,), (), (1, 2))[i % 4]:
            weight_first(i + step)

    def weight_ready(i):
        for direction in range(2):
            weight_copy(i, direction, H, True).wait_recv()

    def rows_of(tile):
        return pl.ds(tile * RT, RT)

    def gather_copy(l, tile, src, direction):
        ref = stream.at[l, 2 * src + core, rows_of(tile)]
        return pltpu.make_async_remote_copy(
            src_ref=ref, dst_ref=ref,
            send_sem=gather_send.at[l, tile, direction, src],
            recv_sem=gather_recv.at[l, tile, direction, src],
            device_id=(s, (t + (2 if direction == 0 else T - 2)) % T), device_id_type=MESH,
        )

    def twin_copy(l, tile, src, receive=False):
        block = 2 * src + (1 - core if receive else core)
        ref = stream.at[l, block, rows_of(tile)]
        return pltpu.make_async_remote_copy(
            src_ref=ref, dst_ref=ref,
            send_sem=twin_send.at[l, tile, src], recv_sem=twin_recv.at[l, tile, src],
            device_id=partner, device_id_type=MESH,
        )

    def reduce_copy(l, tile, d, direction):
        return pltpu.make_async_remote_copy(
            src_ref=own_part.at[l, d, rows_of(tile)],
            dst_ref=line_recv.at[l, direction, d, rows_of(tile)],
            send_sem=reduce_send.at[l, tile, direction, d],
            recv_sem=reduce_recv.at[l, tile, direction, d],
            device_id=(s, (t + (2 if direction == 0 else T - 2)) % T), device_id_type=MESH,
        )

    def pair_copy(l, tile, d):
        return pltpu.make_async_remote_copy(
            src_ref=pair_send.at[l, d, rows_of(tile)], dst_ref=pair_recv.at[l, d, rows_of(tile)],
            send_sem=pair_send_sem.at[l, tile, d], recv_sem=pair_recv_sem.at[l, tile, d],
            device_id=partner, device_id_type=MESH,
        )

    def total_into(l, tile, d, incoming, base, store):
        step = min(RT, 32)

        def body(i, _):
            rows = pl.ds(pl.multiple_of(tile * RT + i * step, step), step)
            value = own_part[l, d, rows].astype(f32) + pair_recv[l, d, rows].astype(f32)
            for direction in incoming:
                value = value + line_recv[l, direction, d, rows].astype(f32)
            if base:
                value = stream[l, t, rows].astype(f32) + value
            store(rows, value.astype(bf16))
            return 0

        lax.fori_loop(0, RT // step, body, 0)

    def square_copy(tile, k, receive=False):
        block = (t + T - k) % T if receive else t
        return pltpu.make_async_remote_copy(
            src_ref=squares.at[tile, block], dst_ref=squares.at[tile, block],
            send_sem=square_send.at[tile, k], recv_sem=square_recv.at[tile, k],
            device_id=(s, (t + k) % T), device_id_type=MESH,
        )

    def close(tile):
        acc = jnp.zeros((RT, 128), f32)
        for b in range(F // 128):
            value = closing[tile * RT:(tile + 1) * RT, b * 128:(b + 1) * 128].astype(f32)
            acc = acc + value * value
        squares[tile, t] = jnp.sum(acc.T, axis=0, keepdims=True)
        for k in range(1, T):
            square_copy(tile, k).start()

    def run_event(zi, l, event, gather_layer):
        kind, tile, which = event
        if kind in "RL":
            direction = 0 if kind == "R" else 1
            pair_copy(l, tile, which).wait_recv()
            incoming = [direction] if (zi > 0 if direction == 0 else zi < NZ - 1) else []
            for d in incoming:
                reduce_copy(l, tile, which, d).wait_recv()

            def store(rows, value):
                own_part[l, which, rows] = value

            total_into(l, tile, which, incoming, False, store)
            reduce_copy(l, tile, which, direction).start()
        elif kind == "F":
            if l is not None:
                pair_copy(l, tile, zi).wait_recv()
                incoming = ([0] if zi > 0 else []) + ([1] if zi < NZ - 1 else [])
                for d in incoming:
                    reduce_copy(l, tile, zi, d).wait_recv()

                def store(rows, value):
                    if l < last:
                        stream[l + 1, t, rows] = value
                    else:
                        closing[rows] = value

                total_into(l, tile, zi, incoming, True, store)
                if l == last:
                    close(tile)
            if gather_layer is not None:
                if zi + 1 < NZ:
                    gather_copy(gather_layer, tile, zi, 0).start()
                if zi > 0:
                    gather_copy(gather_layer, tile, zi, 1).start()
                twin_copy(gather_layer, tile, zi).start()
        else:
            direction = 0 if kind == "GR" else 1
            gather_copy(gather_layer, tile, which, direction).wait_recv()
            if (zi + 1 < NZ) if direction == 0 else (zi > 0):
                gather_copy(gather_layer, tile, which, direction).start()
            twin_copy(gather_layer, tile, which).start()

    def run_phase(l, gather_layer, weight_events):
        plan = line_plan(NZ, TILES, l is not None, gather_layer is not None)
        for zi in range(NZ):
            events = [
                (now, n, e) for n, (now, e) in enumerate(plan[zi])
                if (e[0], zi) not in (("R", 0), ("L", NZ - 1))
            ]
            events += [(now, -1, ("W", i, 0)) for now, i in weight_events if i < 4 * L]
            if gather_layer is not None:
                for tile in range(TILES):
                    arrived = max(now for now, e in plan[zi] if e[1] == tile)
                    events.append((arrived + HOP_US, TILES * T * T, ("N", tile, 0)))
            events.sort(key=lambda e: (e[0], e[1]))

            @pl.when(z == zi)
            def _():
                for _, _, event in events:
                    if event[0] == "W":
                        weight_forward(event[1])
                    elif event[0] == "N":
                        normalize(gather_layer, event[1])
                    else:
                        run_event(zi, l, event, gather_layer)

    def normalize(l, tile):
        for src in range(NZ):
            twin_copy(l, tile, src, True).wait_recv()
        step = min(RT, 16)

        def body(i, _):
            rows = pl.ds(pl.multiple_of(tile * RT + i * step, step), step)
            acc = jnp.zeros((step, F), f32)
            for b in range(T):
                value = stream[l, b, rows].astype(f32)
                acc = acc + value * value
            scale = lax.rsqrt(jnp.sum(acc, axis=1, keepdims=True) / D + NORM_FLOOR)
            for b in range(T):
                value = stream[l, b, rows].astype(f32)
                normed[rows, b * F:(b + 1) * F] = (value * scale * gain[l:l + 1, b * F:(b + 1) * F]).astype(bf16)
            return 0

        lax.fori_loop(0, RT // step, body, 0)

    def project(l, k, into):
        step = min(R, 256)

        def body(i, _):
            rows = pl.ds(pl.multiple_of(i * step, step), step)
            value = jnp.dot(
                normed[rows, :], weights[l, k].reshape(D, C), preferred_element_type=f32
            )
            into[rows, :] = value.astype(bf16)
            return 0

        lax.fori_loop(0, R // step, body, 0)

    def edge_copy(l):
        return pltpu.make_async_remote_copy(
            src_ref=edge_send.at[l], dst_ref=edge_recv.at[l],
            send_sem=edge_send_sem.at[l], recv_sem=edge_recv_sem.at[l],
            device_id=((s + 1) % S, t), device_id_type=MESH,
        )

    def mix(l):
        weight_ready(4 * l)
        project(l, 0, filter_rows)
        weight_ready(4 * l + 1)
        project(l, 1, signal_rows)
        value = (filter_rows[...].astype(f32) * signal_rows[...].astype(f32)).astype(bf16)
        product[8:8 + R, :] = value.astype(f32)
        edge_send[l] = value[R - 16:, :]

        @pl.when(s < S - 1)
        def _():
            edge_copy(l).start()

        if l == 0:
            weight_forward(4 * l + 3)
        weight_ready(4 * l + 2)

        @pl.when(s > 0)
        def _():
            edge_copy(l).wait_recv()
            product[0:8, :] = edge_recv[l].astype(f32)[8:, :]

        @pl.when(s == 0)
        def _():
            product[0:8, :] = jnp.zeros((8, C), f32)

    order = sorted(range(NZ), key=lambda d: (min(d, NZ - 1 - d), -d))

    def partials(l, tile):
        first, rows = tile * RT, slice(tile * RT, (tile + 1) * RT)
        gate = jnp.dot(
            normed[rows, :], weights[l, 2].reshape(D, C), preferred_element_type=f32
        ).astype(bf16)
        filtered = jnp.zeros((RT, C), f32)
        for k in range(TAPS):
            begin = 8 - (TAPS - 1) + k + first
            filtered = filtered + taps[k, l:l + 1, :] * product[begin:begin + RT, :]
        mixed[rows, :] = (gate.astype(f32) * filtered).astype(bf16)
        if tile == 0:
            weight_ready(4 * l + 3)
        for own in (False, True):
            for d in order:
                block = 2 * d + (core if own else 1 - core)
                columns = pl.ds(pl.multiple_of((block % TB) * F, F), F)
                value = jnp.dot(
                    mixed[rows, :], outs[l, block // TB, :, columns], preferred_element_type=f32
                ).astype(bf16)
                if own:
                    own_part[l, d, rows] = value
                else:
                    pair_send[l, d, rows] = value
                    pair_copy(l, tile, d).start()

    def launch(l, tile, near=0, far=NZ):
        @pl.when(z == 0)
        def _():
            for d in range(NZ - 1, 0, -1):
                if near <= d < far:
                    run_event(0, l, ("R", tile, d), None)

        @pl.when(z == NZ - 1)
        def _():
            for d in range(NZ - 1):
                if near <= NZ - 1 - d < far:
                    run_event(NZ - 1, l, ("L", tile, d), None)

    def drain_gather(l):
        for tile in range(TILES):
            for d in range(NZ):
                twin_copy(l, tile, d).wait_send()

                @pl.when((z < NZ - 1) & (d <= z))
                def _():
                    gather_copy(l, tile, d, 0).wait_send()

                @pl.when((z > 0) & (d >= z))
                def _():
                    gather_copy(l, tile, d, 1).wait_send()

    def drain_reduce(l):
        @pl.when(s < S - 1)
        def _():
            edge_copy(l).wait_send()

        for tile in range(TILES):
            for d in range(NZ):
                pair_copy(l, tile, d).wait_send()

                @pl.when((z < NZ - 1) & (d > z))
                def _():
                    reduce_copy(l, tile, d, 0).wait_send()

                @pl.when((z > 0) & (d < z))
                def _():
                    reduce_copy(l, tile, d, 1).wait_send()

    def drain_weights(first, end):
        for i in range(first, end):
            for direction in range(2):
                for hop in range(1, H + 1):
                    weight_copy(i, direction, hop).wait_send()

    weight_first(0)
    weight_first(1)
    for copy in locals_[:3]:
        copy.wait()
    run_phase(None, 0, ((13.0, 0), (24.0, 1)))
    for copy in locals_[3:]:
        copy.wait()
    weight_forward(2)
    for l in range(L):
        mix(l)
        if l == 1:
            drain_gather(0)
        if l > 0:
            drain_gather(l)
            drain_reduce(l - 1)
            drain_weights(4 * l - 4, 4 * l)
        for tile in range(TILES):
            partials(l, tile)
            if tile > 0:
                launch(l, tile - 1, 0 if l < last else NZ - 1)
        launch(l, TILES - 1, 0 if l < last else NZ - 1)
        if l < last:
            run_phase(l, l + 1, ((8.0, 4 * l + 4), (20.0, 4 * l + 5), (36.0, 4 * l + 6), (52.0, 4 * l + 7)))
        else:
            for distance in range(NZ - 2, 0, -1):
                for tile in range(TILES):
                    launch(l, tile, distance, distance + 1)
            run_phase(l, None, ())

    drain_reduce(last)
    drain_weights(4 * last, 4 * L)
    for tile in range(TILES):
        for k in range(1, T):
            square_copy(tile, k, True).wait_recv()
        total = squares[tile, 0]
        for k in range(1, T):
            total = total + squares[tile, k]
        scale = lax.rsqrt(total / D + NORM_FLOOR)
        scale_rows[tile * RT:(tile + 1) * RT, :] = jnp.broadcast_to(scale, (128, RT)).T
    outgoing = [
        pltpu.make_async_copy(closing, result, local_sem.at[0]),
        pltpu.make_async_copy(scale_rows, scales, local_sem.at[1]),
    ]
    for copy in outgoing:
        copy.start()
    for copy in outgoing:
        copy.wait()

    for tile in range(TILES):
        for k in range(1, T):
            square_copy(tile, k).wait_send()


LINK_SENDS = (
    {0: "u", 4: "u", 2: "c"},
    {1: "ud", 0: "u", 4: "u", 2: "dc", 5: "d"},
    {2: "cd", 1: "u", 0: "u", 4: "u"},
    {3: "c"},
)
NEEDED = (0, 1, 4, 5)


def first_plan(tiles):
    unit = CHUNK_US / tiles
    heap, free = [], {}
    out = [[] for _ in range(4)]
    complete = [{tile: 0.0 for tile in range(tiles)} for _ in range(4)]
    for zz in range(4):
        for tile in range(tiles):
            heapq.heappush(heap, (0.0, tile, zz, zz))
    while heap:
        now, tile, zz, kind = heapq.heappop(heap)
        out[zz].append((now, tile, ("S" if kind == zz else "G", tile, kind)))
        if kind in NEEDED:
            complete[zz][tile] = max(complete[zz][tile], now)
        for way in LINK_SENDS[zz].get(kind, ""):
            begin = max(now, free.get((zz, way), 0.0))
            free[zz, way] = begin + unit
            target, there = {"u": (zz + 1, kind), "d": (zz - 1, kind), "c": (3 - zz, 7 - kind)}[way]
            heapq.heappush(heap, (begin + unit + HOP_US, tile, target, there))
    limits = [max(complete[zz][tile] for zz in range(4)) for tile in range(tiles)]
    for zz in range(4):
        out[zz].append((0.0, tiles, ("Q", 0, 0)))
        out[zz].append((16.0 if zz == 1 else 0.0, tiles + 1, ("Y", 0, 0)))
        out[zz].append((CHUNK_US + 7.0, tiles, ("WX", 0, 0)))
        out[zz].append((2 * CHUNK_US + 7.0, tiles, ("WY", 0, 0)))
        out[zz].sort(key=lambda e: (e[0], e[1]))
    stages = []
    for tile in range(tiles):
        low = limits[tile - 1] if tile > 0 else -1.0
        high = limits[tile] if tile < tiles - 1 else float("inf")
        stages.append([[e for now, _, e in events if low < now <= high] for events in out])
    return stages


def paired_kernel(
    sizes,
    residual, gain_in, filter_w, signal_w, gate_w, out_w, taps_in,
    result, scales,
    acts, stream, normed, first_rows, first_w, weights, outs, own_part, pair_send, pair_recv, line_recv,
    part_send, part_recv, own_sum, product, edge_send, edge_recv, inner_rows,
    mixed, closing, squares, first_squares, row_scale, gain, taps, scale_rows,
    act_recv, line_send, cross_send, act_twin_recv, act_twin_send, first_recv, first_send,
    part_recv_sem, part_send_sem, weight_recv, weight_send, piece_recv,
    gather_recv, gather_send, twin_recv, twin_send, reduce_recv, reduce_send,
    pair_recv_sem, pair_send_sem, edge_recv_sem, edge_send_sem, square_recv, square_send, local_sem,
):
    S, T, L, R, F, C, DS, TAPS = sizes
    NZ, TB, RT, D = T // 2, T // S, R // TILES, T * F
    last = L - 1
    s, t = lax.axis_index("sp"), lax.axis_index("tp")
    z, core = t // 2, t % 2
    y, x = s // 2, s % 2
    zz = z + y * (NZ - 1 - 2 * z)
    local_kind = x + y * (1 - 2 * x)
    partner = (s, t + 1 - 2 * core)
    x_peer, y_peer = (s + 1 - 2 * x, t), (s + 2 - 4 * y, t)
    x_slot, y_slot = s + 1 - 2 * x, s + 2 - 4 * y
    diagonal = S - 1 - s
    own_w = (filter_w, signal_w, gate_w, out_w)

    barrier = pltpu.get_barrier_semaphore()
    for k in range(1, T):
        pl.semaphore_signal(barrier, inc=1, device_id=(s, (t + k) % T), device_id_type=MESH)
    for other in range(1, S):
        pl.semaphore_signal(barrier, inc=1, device_id=((s + other) % S, t), device_id_type=MESH)

    locals_ = []

    def local(src, dst):
        copy = pltpu.make_async_copy(src, dst, local_sem.at[len(locals_)])
        copy.start()
        locals_.append(copy)

    def remote(src, dst, send_sem, recv_sem, device):
        return pltpu.make_async_remote_copy(
            src_ref=src, dst_ref=dst, send_sem=send_sem, recv_sem=recv_sem,
            device_id=device, device_id_type=MESH,
        )

    local(residual, acts.at[zz, core])
    local(gain_in, gain)
    local(taps_in, taps)
    for k in range(3):
        local(own_w[k].at[0], first_w.at[k, pl.ds(local_kind * 2, 2)])
    for l in range(L):
        if l > 0:
            for k in range(3):
                local(own_w[k].at[l], weights.at[l - 1, k, pl.ds(s * TB, TB)])
        local(out_w.at[l], outs.at[l, s])
    pl.semaphore_wait(barrier, T - 1 + S - 1)

    share = FINE // TILES

    def first_of(tile, size):
        return R - size - tile * size

    def rows_of(tile):
        return pl.ds(first_of(tile, RT), RT)

    def layer_rows(l, tile):
        size = R // FINE
        return pl.ds(pl.multiple_of(first_of(tile, size), size), size)

    def tile_rows(tile):
        return pl.ds(pl.multiple_of(first_of(tile, RT), RT), RT)

    def drained(ref, sem, device):
        remote(ref, ref, sem, sem, device).wait_send()


    def first_copy(k):
        block = first_w.at[k, pl.ds(local_kind * 2, 2)]
        return remote(own_w[k].at[0], block, first_send.at[0], first_recv.at[k], x_peer)

    def first_arrival(k):
        block = first_w.at[k, pl.ds(2 - local_kind * 2, 2)]
        return remote(block, block, first_send.at[0], first_recv.at[k], x_peer)

    def act_copy(kind, tile, way):
        ref = acts.at[kind, core, rows_of(tile)]
        if way == "c":
            there = 7 - kind
            return remote(
                ref, acts.at[there, core, rows_of(tile)],
                cross_send.at[0], act_recv.at[there, tile], y_peer,
            )
        step = 2 - 4 * y if way == "u" else 4 * y - 2
        return remote(
            ref, ref, line_send.at["ud".index(way)], act_recv.at[kind, tile], (s, (t + step + T) % T)
        )

    def act_arrival(kind, tile):
        ref = acts.at[kind, core, rows_of(tile)]
        return remote(ref, ref, cross_send.at[0], act_recv.at[kind, tile], y_peer)

    def act_twin(kind, tile):
        ref = acts.at[kind, core, rows_of(tile)]
        return remote(ref, ref, act_twin_send.at[0], act_twin_recv.at[tile], partner)

    def part_copy(m, tile, receive=False):
        return remote(
            part_send.at[m, rows_of(tile)], part_recv.at[m, rows_of(tile)],
            part_send_sem.at[0], part_recv_sem.at[m, tile], y_peer,
        )

    def first_square_copy(k):
        return remote(
            first_squares.at[t], first_squares.at[t],
            square_send.at[1], square_recv.at[TILES], (s, (t + k) % T),
        )

    def row_squares(ref, tile):
        acc = jnp.zeros((RT, 128), f32)
        for b in range(F // 128):
            value = ref[rows_of(tile), b * 128:(b + 1) * 128].astype(f32)
            acc = acc + value * value
        return jnp.sum(acc.T, axis=0, keepdims=True)

    def first_event(zi, event):
        what, tile, kind = event
        if what in "SG":
            if what == "G":
                act_arrival(kind, tile).wait_recv()
            for way in LINK_SENDS[zi].get(kind, ""):
                act_copy(kind, tile, way).start()
            if kind in NEEDED:
                act_twin(kind, tile).start()
        elif what == "Q":
            for i in range(TILES):
                first_squares[t, :, i * RT:(i + 1) * RT] = row_squares(acts.at[zi, core], i)
            for k in range(1, T):
                first_square_copy(k).start()
        elif what == "Y":
            weight_copy(3, 1, 0).start()
        else:
            axis = "XY".index(what[1])
            if axis == 0:
                out_copy(0, True).wait_recv()
            else:
                weight_arrival(3, axis, 0).wait_recv()
            weight_copy(3, 1 - axis, 1).start()

    def scale_tile(tile):
        step = min(RT, 32)

        def body(i, _):
            rows = pl.ds(pl.multiple_of(first_of(tile, RT) + i * step, step), step)
            for kind in NEEDED:
                j, below = (kind, RT) if kind < 2 else (kind - 4, 0)
                block = j + y * (NZ - 1 - 2 * j)
                into = pl.ds(pl.multiple_of(below + i * step, step), step)
                for c in range(2):
                    columns = pl.ds(pl.multiple_of((2 * block + c) * F, F), F)
                    value = acts[kind, c, rows].astype(f32) * gain[0:1, columns]
                    begin = (2 * j + c) * F
                    first_rows[tile, into, begin:begin + F] = value.astype(bf16)
            return 0

        lax.fori_loop(0, RT // step, body, 0)

    def first_product(tile, m):
        value = jnp.dot(
            first_rows[tile], first_w[m].reshape(D // 2, C), preferred_element_type=f32
        )
        rows = tile_rows(tile)
        part_send[m, rows] = value[:RT].astype(bf16)
        part_copy(m, tile).start()
        own_sum[m, rows] = value[RT:]

    def first_weight(m):
        locals_[3 + m].wait()
        first_arrival(m).wait_recv()

    def loop(count, body):
        def step(i, _):
            body(i)
            return 0

        lax.fori_loop(0, count, step, 0)

    def joined(m, rows):
        return scaled(own_sum[m, rows] + part_recv[m, rows].astype(f32), rows)

    def scaled(value, rows):
        scale = row_scale[rows, :]
        return jnp.concatenate(
            [value[:, b * 128:(b + 1) * 128] * scale for b in range(C // 128)], axis=1
        ).astype(bf16)

    def first_scale():
        block = first_squares.at[pl.ds(0, T - 1)]
        remote(block, block, square_send.at[1], square_recv.at[TILES], partner).wait_recv()
        total = first_squares[0]
        for k in range(1, T):
            total = total + first_squares[k]
        scale = lax.rsqrt(total / D + NORM_FLOOR)
        for i in range(TILES):
            row_scale[rows_of(i), :] = jnp.broadcast_to(
                scale[:, i * RT:(i + 1) * RT], (128, RT)
            ).T


    def weight_ref(i, slot, half=None):
        l, k = divmod(i, 4)
        if k < 3:
            if half is None:
                return weights.at[l - 1, k, pl.ds(slot * TB, TB)]
            cut = F * 3 // 4
            return weights.at[l - 1, k, pl.ds(slot * TB, TB), pl.ds(cut * half, F - cut if half else cut)]
        if half is None:
            return outs.at[l, slot]
        cut = C * 3 // 8 if l == 0 else C // 2
        return outs.at[l, slot, pl.ds(cut * half, C - cut if half else cut)]

    def weight_copy(i, axis, hop):
        l, k = divmod(i, 4)
        if hop == 0:
            src, dst = own_w[k].at[l], weight_ref(i, s)
        else:
            src = dst = weight_ref(i, (y_slot, x_slot)[axis], axis)
        return remote(
            src, dst, weight_send.at[i - 3], weight_recv.at[i - 3, axis, hop], (x_peer, y_peer)[axis]
        )

    def out_copy(piece, receive=False):
        cut = C * 3 // 8
        rows = pl.ds(0, cut) if piece else pl.ds(cut, C - cut)
        dst = outs.at[0, x_slot if receive else s, rows]
        return remote(
            dst if receive else out_w.at[0, rows], dst, weight_send.at[0],
            piece_recv.at[2] if piece else weight_recv.at[0, 0, 0], x_peer,
        )

    def piece_copy(axis, piece, receive=False):
        rows = pl.ds(piece * (C // 2), C // 2)
        dst = outs.at[last, (x_slot, y_slot)[axis] if receive else s, rows]
        return remote(
            dst if receive else out_w.at[last, rows], dst, weight_send.at[4 * last],
            weight_recv.at[4 * last, axis, 0] if piece else piece_recv.at[axis], (x_peer, y_peer)[axis],
        )

    def last_copy(part, receive=False):
        low, high, axis, sem = (
            (C * 3 // 4, C, 0, weight_recv.at[4 * last, 0, 1]),
            (0, C // 2, 1, piece_recv.at[3]),
            (C // 2, C * 3 // 4, 1, weight_recv.at[4 * last, 1, 1]),
        )[part]
        slot = diagonal if receive else (y_slot, x_slot)[axis]
        ref = outs.at[last, slot, pl.ds(low, high - low)]
        return remote(ref, ref, weight_send.at[4 * last], sem, (x_peer, y_peer)[axis])

    def weight_arrival(i, axis, hop):
        ref = weight_ref(i, (x_slot, y_slot)[axis]) if hop == 0 else weight_ref(i, diagonal, axis)
        return remote(
            ref, ref, weight_send.at[i - 3], weight_recv.at[i - 3, axis, hop], (x_peer, y_peer)[axis]
        )

    def weight_first(i):
        if i < 4 * L:
            for axis in range(2):
                weight_copy(i, axis, 0).start()

    def weight_forward(i):
        for axis in range(2):
            weight_arrival(i, 1 - axis, 0).wait_recv()
            weight_copy(i, axis, 1).start()
        if i == 4 * last + 2:
            for piece in range(2):
                piece_copy(1, piece).start()
        elif i != 4 * last + 1:
            for step in ((2,), (2,), (), (1, 2))[i % 4]:
                weight_first(i + step)

    def weight_ready(i):
        for axis in range(2):
            weight_arrival(i, axis, 1).wait_recv()

    def weight_drain(i):
        l, k = divmod(i, 4)
        ref = weights.at[l - 1, k, pl.ds(0, 3 * TB)] if k < 3 else outs.at[l, pl.ds(0, 3)]
        drained(ref, weight_send.at[i - 3], x_peer)

    def line_peer(direction):
        return (s, (t + (2 if direction == 0 else T - 2)) % T)

    def gather_copy(l, tile, src, direction):
        ref = stream.at[l - 1, 2 * src + core, layer_rows(l - 1, tile)]
        return remote(
            ref, ref, gather_send.at[l - 1, direction], gather_recv.at[l - 1, tile, src],
            line_peer(direction),
        )

    def twin_copy(l, tile, src):
        ref = stream.at[l - 1, 2 * src + core, layer_rows(l - 1, tile)]
        group = tile // share
        return remote(ref, ref, twin_send.at[l - 1], twin_recv.at[l - 1, group], partner)

    def reduce_copy(l, tile, d, direction):
        return remote(
            own_part.at[l, d, layer_rows(l, tile)], line_recv.at[l, direction, d, layer_rows(l, tile)],
            reduce_send.at[l, direction], reduce_recv.at[tile, d + 1 - direction],
            line_peer(direction),
        )

    def pair_copy(l, tile, d):
        return remote(
            pair_send.at[l, d, tile_rows(tile)], pair_recv.at[l, d, tile_rows(tile)],
            pair_send_sem.at[l], pair_recv_sem.at[tile, d], partner,
        )

    def total_into(l, tile, d, incoming, base, store):
        size = R // FINE
        step = min(size, 32)

        def body(i, _):
            rows = pl.ds(pl.multiple_of(first_of(tile, size) + i * step, step), step)
            value = own_part[l, d, rows].astype(f32) + pair_recv[l, d, rows].astype(f32)
            for direction in incoming:
                value = value + line_recv[l, direction, d, rows].astype(f32)
            if base:
                before = acts[zz, core, rows] if l == 0 else stream[l - 1, t, rows]
                value = before.astype(f32) + value
            store(rows, value.astype(bf16))
            return 0

        lax.fori_loop(0, size // step, body, 0)

    def square_copy(tile, k):
        return remote(
            squares.at[tile, t], squares.at[tile, t],
            square_send.at[0], square_recv.at[tile], (s, (t + k) % T),
        )

    def close(tile):
        squares[tile, t] = row_squares(closing, tile)
        for k in range(1, T):
            square_copy(tile, k).start()
        closing_copy(tile).start()

    def closing_copy(tile):
        return pltpu.make_async_copy(
            closing.at[rows_of(tile)], result.at[rows_of(tile)], local_sem.at[1 + tile]
        )

    def pair_arrival(l, tile, d, i):
        if i is None:
            i = tile % share
        if i == 0:
            pair_copy(l, tile // share, d).wait_recv()

    def run_event(zi, l, event, gather_layer, i=None):
        kind, tile, which = event
        if kind in "RL":
            direction = 0 if kind == "R" else 1
            pair_arrival(l, tile, which, i)
            incoming = [direction] if (zi > 0 if direction == 0 else zi < NZ - 1) else []
            for d in incoming:
                reduce_copy(l, tile, which, d).wait_recv()

            def store(rows, value):
                own_part[l, which, rows] = value

            total_into(l, tile, which, incoming, False, store)
            reduce_copy(l, tile, which, direction).start()
        elif kind == "F":
            pair_arrival(l, tile, zi, i)
            incoming = ([0] if zi > 0 else []) + ([1] if zi < NZ - 1 else [])
            for d in incoming:
                reduce_copy(l, tile, zi, d).wait_recv()

            def store(rows, value):
                if l < last:
                    stream[l, t, rows] = value
                else:
                    closing[rows] = value

            total_into(l, tile, zi, incoming, True, store)
            if l == last:
                if tile % share == share - 1:
                    close(tile // share)
            else:
                if zi + 1 < NZ:
                    gather_copy(gather_layer, tile, zi, 0).start()
                if zi > 0:
                    gather_copy(gather_layer, tile, zi, 1).start()
                twin_copy(gather_layer, tile, zi).start()
        else:
            direction = 0 if kind == "GR" else 1
            gather_copy(gather_layer, tile, which, direction).wait_recv()
            if (zi + 1 < NZ) if direction == 0 else (zi > 0):
                gather_copy(gather_layer, tile, which, direction).start()
            twin_copy(gather_layer, tile, which).start()

    def run_phase(l, gather_layer, weight_events):
        tiles = FINE
        plan = line_plan(NZ, tiles, True, gather_layer is not None)
        groups = TILES if gather_layer is not None else 1
        ends = [
            max(now for z_events in plan for now, e in z_events if e[1] * groups // tiles <= g)
            for g in range(groups)
        ]
        for g in range(groups):
            low = ends[g - 1] if g > 0 else -1.0
            high = ends[g] if g < groups - 1 else float("inf")
            for zi in range(NZ):
                events = [
                    (now, n, e) for n, (now, e) in enumerate(plan[zi])
                    if (e[0], zi) not in (("R", 0), ("L", NZ - 1))
                ]
                events += [(now, -1, ("W", i, 0)) for now, i in weight_events if i < 4 * L]
                events = sorted((e for e in events if low < e[0] <= high), key=lambda e: (e[0], e[1]))

                @pl.when(z == zi)
                def _():
                    for _, _, event in events:
                        if event[0] == "W":
                            weight_forward(event[1])
                        else:
                            run_event(zi, l, event, gather_layer)

            if gather_layer is not None:
                normalize(gather_layer, g)
                if g == 0:
                    weight_ready(4 * gather_layer)
                    weight_ready(4 * gather_layer + 1)
                    loop(2, lambda k: project(gather_layer, k, R - RT, RT))
                    send_edge(gather_layer)
                    if gather_layer == last:
                        for piece in range(2):
                            piece_copy(0, piece).start()
                elif g >= groups - 2:
                    size = R - 2 * RT if g < groups - 1 else RT
                    loop(2, lambda k: project(gather_layer, k, R - RT - size if g < groups - 1 else 0, size))

    def normalize(l, tile):
        block = stream.at[l - 1, pl.ds(0, NZ), rows_of(tile)]
        remote(block, block, twin_send.at[l - 1], twin_recv.at[l - 1, tile], partner).wait_recv()
        step = min(RT, 16)

        def body(i, _):
            rows = pl.ds(pl.multiple_of(first_of(tile, RT) + i * step, step), step)
            acc = jnp.zeros((step, F), f32)
            for b in range(T):
                value = stream[l - 1, b, rows].astype(f32)
                acc = acc + value * value
                columns = slice(b * F, (b + 1) * F)
                normed[rows, columns] = (value * gain[l:l + 1, columns]).astype(bf16)
            scale = lax.rsqrt(jnp.sum(acc, axis=1, keepdims=True) / D + NORM_FLOOR)
            row_scale[rows, :] = jnp.broadcast_to(scale, (step, 128))
            return 0

        lax.fori_loop(0, RT // step, body, 0)

    def project(l, k, first, size):
        rows = pl.ds(first, size)
        value = jnp.dot(
            normed[rows, :], weights[l - 1, k].reshape(D, C), preferred_element_type=f32
        )
        inner_rows[k, rows] = scaled(value, rows)

    def edge_copy(l):
        return remote(
            edge_send.at[l], edge_recv.at[l], edge_send_sem.at[l], edge_recv_sem.at[l],
            ((s + 1) % S, t),
        )

    def send_edge(l):
        rows = slice(R - 16, R)
        edge_send[l] = (
            inner_rows[0, rows].astype(f32) * inner_rows[1, rows].astype(f32)
        ).astype(bf16)

        @pl.when(s < S - 1)
        def _():
            edge_copy(l).start()

    def mix(l):
        if l == 0:
            first_scale()

            def arrive(m, tile):
                part_copy(m, tile, True).wait_recv()
                inner_rows[m, tile_rows(tile)] = joined(m, tile_rows(tile))

            arrive(0, 0)
            first_weight(2)
            loop(TILES, lambda tile: first_product(tile, 2))
            arrive(1, 0)
            send_edge(l)
            for i in (4, 5):
                weight_first(i)
            loop(TILES - 1, lambda i: arrive(0, i + 1))
            loop(TILES - 1, lambda i: arrive(1, i + 1))
        value = (inner_rows[0].astype(f32) * inner_rows[1].astype(f32)).astype(bf16)
        product[8:8 + R, :] = value.astype(f32)
        @pl.when(s > 0)
        def _():
            edge_copy(l).wait_recv()
            product[0:8, :] = edge_recv[l].astype(f32)[8:, :]

        @pl.when(s == 0)
        def _():
            product[0:8, :] = jnp.zeros((8, C), f32)

    def gates(l, tile):
        size = RT
        first = pl.multiple_of(first_of(tile, size), size)
        rows = pl.ds(first, size)
        if l == 0:
            part_copy(2, tile, True).wait_recv()
            gate = joined(2, rows)
        else:
            gate = scaled(
                jnp.dot(
                    normed[rows, :], weights[l - 1, 2].reshape(D, C), preferred_element_type=f32
                ),
                rows,
            )
        window = product[pl.ds(first, size + 8), :]
        filtered = jnp.zeros((size, C), f32)
        for k in range(TAPS):
            begin = 8 - (TAPS - 1) + k
            filtered = filtered + taps[k, l:l + 1, :] * window[begin:begin + size]
        mixed[rows, :] = (gate.astype(f32) * filtered).astype(bf16)

    def partials(l, tile, dests):
        rows = tile_rows(tile)
        for own in (False, True):
            for d in dests:
                part = core if own else 1 - core
                columns = pl.ds(pl.multiple_of(part * F, F), F)
                value = jnp.dot(
                    mixed[rows, :], outs[l, d, :, columns], preferred_element_type=f32
                ).astype(bf16)
                if own:
                    own_part[l, d, rows] = value
                else:
                    pair_send[l, d, rows] = value
                    pair_copy(l, tile, d).start()

    def launch_tile(l, tile, ranks):
        for i in range(share):
            launch(l, tile * share + i, ranks, i)

    def launch(l, tile, ranks, i):
        @pl.when(z == 0)
        def _():
            swap = 1 - x if l == last else 0
            for rank in ranks:
                d = NZ - 1 - rank
                if rank < 2:
                    d = d + swap * (2 * rank - 1)
                run_event(0, l, ("R", tile, d), None, i)

        @pl.when(z == NZ - 1)
        def _():
            swap = x if l == last else 0
            for rank in ranks:
                d = rank
                if rank < 2:
                    d = d + swap * (1 - 2 * rank)
                run_event(NZ - 1, l, ("L", tile, d), None, i)

    def drain_first():
        drained(acts.at[pl.ds(0, 4), 0], act_twin_send.at[0], partner)
        drained(acts.at[0, 0], cross_send.at[0], y_peer)
        for zi in range(NZ):
            @pl.when(zz == zi)
            def _():
                for n, way in enumerate("ud"):
                    count = sum(way in ways for ways in LINK_SENDS[zi].values())
                    if count:
                        drained(acts.at[pl.ds(0, count), 0], line_send.at[n], partner)
        drained(part_send, part_send_sem.at[0], y_peer)
        block = first_squares.at[pl.ds(0, T - 1)]
        drained(block, square_send.at[1], partner)
        drained(first_w.at[pl.ds(0, 3), pl.ds(0, 2)], first_send.at[0], x_peer)

    def drain_gather(l):
        drained(stream.at[l - 1, pl.ds(0, NZ)], twin_send.at[l - 1], partner)
        for zi in range(NZ):
            @pl.when(z == zi)
            def _():
                for direction, count in enumerate((zi + 1 if zi < NZ - 1 else 0, NZ - zi if zi > 0 else 0)):
                    if count:
                        drained(
                            stream.at[l - 1, pl.ds(0, count)], gather_send.at[l - 1, direction], partner
                        )

    def drain_reduce(l):
        @pl.when(s < S - 1)
        def _():
            edge_copy(l).wait_send()

        drained(pair_send.at[l], pair_send_sem.at[l], partner)
        for zi in range(NZ):
            @pl.when(z == zi)
            def _():
                for direction, count in enumerate((NZ - 1 - zi, zi)):
                    if count:
                        drained(
                            own_part.at[l, pl.ds(0, count)], reduce_send.at[l, direction], partner
                        )

    out_copy(0).start()
    for k in range(3):
        first_copy(k).start()
    out_copy(1).start()
    for copy in locals_[:3]:
        copy.wait()
    stages = first_plan(TILES)
    for tile in range(TILES):
        for zi in range(NZ):
            @pl.when(zz == zi)
            def _():
                for event in stages[tile][zi]:
                    first_event(zi, event)
        block = acts.at[pl.ds(0, 4), 0, rows_of(tile)]
        remote(block, block, act_twin_send.at[0], act_twin_recv.at[tile], partner).wait_recv()
        scale_tile(tile)
        if tile == 0:
            first_weight(0)
        first_product(tile, 0)
    first_weight(1)
    loop(TILES, lambda tile: first_product(tile, 1))
    for copy in locals_[6:]:
        copy.wait()
    for l in range(L):
        mix(l)
        if l > 0:
            if l == 1:
                drain_first()
                weight_drain(3)
            else:
                for i in range(4 * l - 4, 4 * l):
                    weight_drain(i)
            drain_gather(l)
            drain_reduce(l - 1)
            weight_ready(4 * l + 2)
        if l < last:
            if l == 0:
                out_copy(1, True).wait_recv()
            weight_ready(4 * l + 3)
            ranks, dests = range(NZ - 1), range(NZ)
        else:
            for piece in range(2):
                piece_copy(1, piece, True).wait_recv()
            last_copy(0).start()
            turn = (x + jnp.where(z < NZ // 2, NZ - 2, 0) - diagonal + NZ) % NZ
            ranks, dests = (0,), ((diagonal + turn) % NZ,)

        def step(tile):
            gates(l, tile)
            partials(l, tile, dests)
            if l == last:
                @pl.when(tile == 1)
                def _():
                    piece_copy(0, 0, True).wait_recv()
                    last_copy(1).start()

            @pl.when(tile > 0)
            def _():
                launch_tile(l, tile - 1, ranks)

        loop(TILES, step)
        if l < last:
            launch_tile(l, TILES - 1, ranks)
            run_phase(l, l + 1, ((12.0, 4 * l + 4), (24.0, 4 * l + 5), (40.0, 4 * l + 6)) + (((57.0, 4 * l + 7),) if l + 1 < last else ()))
        else:
            others = [(diagonal + 1 + (turn + n) % (NZ - 1)) % NZ for n in range(NZ - 2)]

            def rest(tile):
                partials(l, tile, others)

                @pl.when(tile == 0)
                def _():
                    launch_tile(l, TILES - 1, ranks)

            piece_copy(0, 1, True).wait_recv()
            last_copy(2).start()
            loop(TILES, rest)
            for part in range(3):
                last_copy(part, True).wait_recv()
            loop(TILES, lambda tile: partials(l, tile, (diagonal,)))
            for rank in range(1, NZ - 1):
                loop(TILES, lambda tile: launch_tile(l, tile, (rank,)))
            run_phase(l, None, ())

    drain_reduce(last)
    for i in range(4 * last, 4 * L):
        weight_drain(i)
    for tile in range(TILES):
        block = squares.at[tile, pl.ds(0, T - 1)]
        remote(block, block, square_send.at[0], square_recv.at[tile], partner).wait_recv()
        total = squares[tile, 0]
        for k in range(1, T):
            total = total + squares[tile, k]
        scale_rows[:, rows_of(tile)] = lax.rsqrt(total / D + NORM_FLOOR)
    outgoing = pltpu.make_async_copy(scale_rows, scales, local_sem.at[0])
    outgoing.start()
    drained(squares.at[pl.ds(0, TILES), pl.ds(0, T - 1)], square_send.at[0], partner)
    for tile in range(TILES):
        closing_copy(tile).wait()
    outgoing.wait()


def finish(pieces, closing, scale, gain, result, rows_in, scale_in, gain_in, rows_out, sems):
    R, F = rows_in.shape
    step = R // pieces

    def copies(i):
        rows = pl.ds(i * step, step)
        return (
            pltpu.make_async_copy(closing.at[rows], rows_in.at[rows], sems.at[i]),
            pltpu.make_async_copy(rows_out.at[rows], result.at[rows], sems.at[i]),
        )

    small = [
        pltpu.make_async_copy(scale, scale_in, sems.at[pieces]),
        pltpu.make_async_copy(gain, gain_in, sems.at[pieces + 1]),
    ]
    for copy in small:
        copy.start()
    for i in range(pieces):
        copies(i)[0].start()
    for copy in small:
        copy.wait()
    for i in range(pieces):
        rows = slice(i * step, (i + 1) * step)
        factor = jnp.broadcast_to(scale_in[:, rows], (128, step)).T
        copies(i)[0].wait()
        for b in range(F // 128):
            columns = slice(b * 128, (b + 1) * 128)
            rows_out[rows, columns] = (
                rows_in[rows, columns].astype(f32) * factor * gain_in[:, columns]
            )
        copies(i)[1].start()
    for i in range(pieces):
        copies(i)[1].wait()


def paired_call(S, T, L, R, F, C, DS, TAPS):
    NZ, TB = T // 2, T // S
    dma = pltpu.SemaphoreType.DMA
    any_space = pl.BlockSpec(memory_space=pl.ANY)
    return pl.pallas_call(
        functools.partial(paired_kernel, (S, T, L, R, F, C, DS, TAPS)),
        out_shape=(jax.ShapeDtypeStruct((R, F), bf16), jax.ShapeDtypeStruct((1, R), f32)),
        in_specs=[any_space] * 7,
        out_specs=(any_space, any_space),
        scratch_shapes=[
            pltpu.VMEM((6, 2, R, F), bf16),
            pltpu.VMEM((L - 1, T, R, F), bf16),
            pltpu.VMEM((R, T * F), bf16),
            pltpu.VMEM((TILES, 2 * R // TILES, T // 2 * F), bf16),
            pltpu.VMEM((3, T // 2, F, C), bf16),
            pltpu.VMEM((L - 1, 3, T, F, C), bf16),
            pltpu.VMEM((L, S, C, DS), bf16),
            pltpu.VMEM((L, NZ, R, F), bf16),
            pltpu.VMEM((L, NZ, R, F), bf16),
            pltpu.VMEM((L, NZ, R, F), bf16),
            pltpu.VMEM((L, 2, NZ, R, F), bf16),
            pltpu.VMEM((3, R, C), bf16),
            pltpu.VMEM((3, R, C), bf16),
            pltpu.VMEM((3, R, C), f32),
            pltpu.VMEM((R + 8, C), f32),
            pltpu.VMEM((L, 16, C), bf16),
            pltpu.VMEM((L, 16, C), bf16),
            pltpu.VMEM((2, R, C), bf16),
            pltpu.VMEM((R, C), bf16),
            pltpu.VMEM((R, F), bf16),
            pltpu.VMEM((TILES, T, 1, R // TILES), f32),
            pltpu.VMEM((T, 1, R), f32),
            pltpu.VMEM((R, 128), f32),
            pltpu.VMEM((L, T * F), f32),
            pltpu.VMEM((TAPS, L, C), f32),
            pltpu.VMEM((1, R), f32),
            dma((6, TILES)), dma((2,)), dma((1,)), dma((TILES,)), dma((1,)), dma((3,)), dma((1,)),
            dma((3, TILES)), dma((1,)), dma((4 * L - 3, 2, 2)), dma((4 * L - 3,)), dma((4,)),
            dma((L - 1, FINE, NZ)), dma((L - 1, 2)), dma((L - 1, TILES)), dma((L - 1,)),
            dma((FINE, NZ + 1)), dma((L, 2)),
            dma((TILES, NZ)), dma((L,)), dma((L,)), dma((L,)),
            dma((TILES + 1,)), dma((2,)), dma((4 * L + 6,)),
        ],
        compiler_params=pltpu.CompilerParams(
            collective_id=0, has_side_effects=True, vmem_limit_bytes=60 * 2**20
        ),
        name="mixers",
    )


def per_device(
    S, T, residual_in, norm_gain, gate_proj, filter_proj, signal_proj, conv_taps, out_proj, final_gain
):
    R, F = residual_in.shape
    L, DS, C = gate_proj.shape
    TAPS = conv_taps.shape[1]
    NZ, TB, H = T // 2, T // S, S // 2
    dma = pltpu.SemaphoreType.DMA
    cut = lambda w: w.reshape(L, TB, F, C)
    any_space = pl.BlockSpec(memory_space=pl.ANY)
    paired = S == 4 and NZ == 4 and L > 1
    if paired:
        closing, scale = paired_call(S, T, L, R, F, C, DS, TAPS)(
            residual_in, norm_gain, cut(filter_proj), cut(signal_proj),
            cut(gate_proj), out_proj, conv_taps.transpose(1, 0, 2),
        )
    else:
        closing, scale = pl.pallas_call(
            functools.partial(kernel, (S, T, L, R, F, C, DS, TAPS)),
            out_shape=(jax.ShapeDtypeStruct((R, F), bf16), jax.ShapeDtypeStruct((R, 128), f32)),
            in_specs=[any_space] * 7,
            out_specs=(any_space, any_space),
            scratch_shapes=[
                pltpu.VMEM((L, T, R, F), bf16),
                pltpu.VMEM((R, T * F), bf16),
                pltpu.VMEM((L, 3, T, F, C), bf16),
                pltpu.VMEM((L, S, C, DS), bf16),
                pltpu.VMEM((L, NZ, R, F), bf16),
                pltpu.VMEM((L, NZ, R, F), bf16),
                pltpu.VMEM((L, NZ, R, F), bf16),
                pltpu.VMEM((L, 2, NZ, R, F), bf16),
                pltpu.VMEM((R, C), bf16),
                pltpu.VMEM((R, C), bf16),
                pltpu.VMEM((R + 8, C), f32),
                pltpu.VMEM((L, 16, C), bf16),
                pltpu.VMEM((L, 16, C), bf16),
                pltpu.VMEM((R, C), bf16),
                pltpu.VMEM((R, F), bf16),
                pltpu.VMEM((TILES, T, 1, R // TILES), f32),
                pltpu.VMEM((L, T * F), f32),
                pltpu.VMEM((TAPS, L, C), f32),
                pltpu.VMEM((R, 128), f32),
                dma((4 * L, 2, H)), dma((4 * L, 2, H)),
                dma((L, TILES, 2, NZ)), dma((L, TILES, 2, NZ)),
                dma((L, TILES, NZ)), dma((L, TILES, NZ)),
                dma((L, TILES, 2, NZ)), dma((L, TILES, 2, NZ)),
                dma((L, TILES, NZ)), dma((L, TILES, NZ)),
                dma((L,)), dma((L,)),
                dma((TILES, T)), dma((TILES, T)),
                dma((4 * L + 3,)),
            ],
            compiler_params=pltpu.CompilerParams(
                collective_id=0, has_side_effects=True, vmem_limit_bytes=60 * 2**20
            ),
            name="mixers",
        )(
            residual_in, norm_gain, cut(filter_proj), cut(signal_proj),
            cut(gate_proj), out_proj, conv_taps.transpose(1, 0, 2),
        )
        scale = scale[:, 0].reshape(1, R)
    return pl.pallas_call(
        functools.partial(finish, 4),
        out_shape=jax.ShapeDtypeStruct((R, F), f32),
        in_specs=[any_space] * 3,
        out_specs=any_space,
        scratch_shapes=[
            pltpu.VMEM((R, F), bf16), pltpu.VMEM((1, R), f32), pltpu.VMEM((1, F), f32),
            pltpu.VMEM((R, F), f32), dma((6,)),
        ],
        name="finish",
    )(closing, scale, final_gain.reshape(1, F))


def solution(mesh):
    return jax.shard_map(
        functools.partial(per_device, mesh.shape["sp"], mesh.shape["tp"]),
        mesh=mesh,
        in_specs=(
            P("sp", "tp"),
            P(),
            P(None, "sp", "tp"),
            P(None, "sp", "tp"),
            P(None, "sp", "tp"),
            P(None, None, "tp"),
            P(None, "tp", "sp"),
            P("tp"),
        ),
        out_specs=P("sp", "tp"),
        check_vma=False,
    )
```
